128 devices in a mesh: kv: 16 (over z, x), tp: 8 (over y, core).
Axes of the slice: x: 4, y: 4, z: 4, core: 2. Of those that a mesh axis runs over, the one named last changes fastest.
Arguments:
- tokens: bfloat16 [64, 2048], P(None, 'kv'), may hold values from -6 to 6
- token_gain: float32 [2048], P('kv'), may hold values from 0.1 to 1.9
- w_query: bfloat16 [2048, 1536], P('kv', 'tp'), may hold values from -0.125 to 0.125
- w_down_kv: bfloat16 [2048, 512], P('kv'), may hold values from -0.125 to 0.125
- w_rope_key: bfloat16 [2048, 64], P('kv'), may hold values from -0.125 to 0.125
- latent_gain: float32 [512], replicated, may hold values from 0.1 to 1.9
- w_key_up: bfloat16 [8, 512, 128], P('tp'), may hold values from -0.25 to 0.25
- w_value_up: bfloat16 [8, 512, 128], P('tp'), may hold values from -0.25 to 0.25
- w_out: bfloat16 [1024, 2048], P('tp', 'kv'), may hold values from -0.1875 to 0.1875
- out_gain: float32 [2048], P('kv'), may hold values from 0.1 to 1.9
- cache_latent: bfloat16 [64, 8192, 512], P('tp', 'kv'), may hold values from -6 to 6
- cache_rope: bfloat16 [64, 8192, 64], P('tp', 'kv'), may hold values from -6 to 6
- lengths: int32 [64], replicated, may hold values from 1 to 8191, as said below
Outputs:
- mixed: bfloat16 [64, 2048], P(None, 'kv')
The draws below stay inside these ranges and needn't reach their ends.
Inputs may be any that keep to these rules, and one draw needn't show every extreme that they name: `lengths`: each of the 64 sequences has 1 to 8191 cached positions; some sequence has exactly 8191 and some exactly 1.
All inputs are finite; a program needn't handle non-finite values.
Results may differ from the reference program's by a relative error of at most 0.015.
Values may be sent and summed in bfloat16 or wider, within the bound.
A program may use at most 64 MiB of HBM per device.

```python
import jax
import jax.numpy as jnp
from jax import lax

D = 2048
HEADS = 8
LATENT = 512
NOPE = 128
ROPE = 64
VDIM = 128
BATCH = 64
CACHE_LEN = 8192


def draw_lengths(key, part):
    first_key, second_key = jax.random.split(jax.random.fold_in(key, 11))
    first_draw = jax.random.randint(first_key, (BATCH,), 1, CACHE_LEN)
    second_draw = jax.random.randint(second_key, (BATCH,), 1, CACHE_LEN)
    joined = jnp.minimum(first_draw, second_draw)
    joined = joined.at[0].set(CACHE_LEN - 1).at[BATCH - 1].set(1)
    return joined.astype(jnp.int32)


def block_scale(stream_key, extent, shards, least, high):
    def one(axis_at, shards_of):
        heights = jax.random.uniform(jax.random.fold_in(jax.random.fold_in(stream_key, 6), axis_at), (shards_of,), jnp.float32, least / len(shards), high / len(shards))
        return jnp.repeat(jnp.exp(heights), extent[axis_at] // shards_of).reshape((-1,) + (1,) * (len(extent) - axis_at - 1))

    gain = one(*shards[0])
    for cut in shards[1:]:
        gain = gain * one(*cut)
    return gain


def centred(stream_key, shape, spread, limit, pieces=(), kind=jnp.bfloat16):
    values = jax.random.normal(stream_key, shape, jnp.float32) * spread
    if len(pieces) > 0:
        values = block_scale(stream_key, shape, pieces, -0.22, 0.18) * values
    return jnp.clip(values, min=-limit, max=limit).astype(kind)


def setup_inputs(seed: int = 0) -> dict:
    keys = jax.random.split(jax.random.key(seed), 14)
    return {
        "tokens": centred(keys[0], (BATCH, D), 1.0, 6.0, ((1, 16),)),
        "token_gain": jnp.clip(1.0 + 0.18 * jax.random.normal(keys[1], (D,), jnp.float32), 0.1, 1.9),
        "w_query": centred(keys[2], (D, HEADS * (NOPE + ROPE)), D ** -0.5, 0.125, ((0, 16), (1, 8))),
        "w_down_kv": centred(keys[3], (D, LATENT), D ** -0.5, 0.125, ((0, 16),)),
        "w_rope_key": centred(keys[4], (D, ROPE), D ** -0.5, 0.125, ((0, 16),)),
        "latent_gain": jnp.clip(1.0 + 0.18 * jax.random.normal(keys[5], (LATENT,), jnp.float32), 0.1, 1.9),
        "w_key_up": centred(keys[6], (HEADS, LATENT, NOPE), LATENT ** -0.5, 0.25, ((0, 8),)),
        "w_value_up": centred(keys[7], (HEADS, LATENT, VDIM), LATENT ** -0.5, 0.25, ((0, 8),)),
        "w_out": centred(keys[8], (HEADS * VDIM, D), (HEADS * VDIM) ** -0.5, 0.1875, ((0, 8), (1, 16))),
        "out_gain": jnp.clip(1.0 + 0.18 * jax.random.normal(keys[9], (D,), jnp.float32), 0.1, 1.9),
        "cache_latent": centred(keys[10], (BATCH, CACHE_LEN, LATENT), 1.0, 6.0, ((0, 8), (1, 16))),
        "cache_rope": centred(keys[11], (BATCH, CACHE_LEN, ROPE), 1.0, 6.0, ((0, 8), (1, 16))),
        "lengths": draw_lengths(jax.random.fold_in(keys[13], 71), 0),
    }


EPSILON = 1e-06
NEGATIVE = -1e+30

def rotate_half(values, cosine, sine_table):
    half_width = values.shape[-1] // 2
    lower_half = values[..., :half_width]
    upper_half = values[..., half_width:]
    return jnp.concatenate([lower_half * cosine - upper_half * sine_table, upper_half * cosine + lower_half * sine_table], axis=-1)

def angle_tables(lengths, rope_width):
    inverse_freq = 1.0 / 10000.0 ** (jnp.arange(0, rope_width, 2, dtype=jnp.float32) / rope_width)
    angles = lengths.astype(jnp.float32)[:, None] * inverse_freq[None, :]
    return (jnp.cos(angles), jnp.sin(angles))

def attend_one(packed):
    query_lat, query_rot, new_latent, new_key, length, cached_lat, cached_rot = packed
    factor = (NOPE + ROPE) ** (-0.5)
    scores = (jnp.dot(query_lat, cached_lat.T, preferred_element_type=jnp.float32) + jnp.dot(query_rot, cached_rot.T, preferred_element_type=jnp.float32)) * factor
    new_score = (jnp.dot(query_lat, new_latent, preferred_element_type=jnp.float32) + jnp.dot(query_rot, new_key, preferred_element_type=jnp.float32)) * factor
    visible = jnp.arange(CACHE_LEN) < length
    top_score = jnp.maximum(lax.optimization_barrier(jnp.max(jnp.where(visible[None, :], scores, NEGATIVE), axis=1)), new_score)
    weights = jnp.where(visible[None, :], jnp.exp(scores - top_score[:, None]), jnp.float32(0.0))
    new_weight = jnp.exp(new_score - top_score)
    weight_sum = lax.optimization_barrier(jnp.sum(weights, axis=1)) + new_weight
    rounded_new = lax.optimization_barrier(new_weight.astype(jnp.bfloat16)).astype(jnp.float32)
    weighted = jnp.dot(weights.astype(jnp.bfloat16), cached_lat, preferred_element_type=jnp.float32) + rounded_new[:, None] * new_latent.astype(jnp.float32)[None, :]
    return (weighted / weight_sum[:, None]).astype(jnp.bfloat16)

def reference(tokens, token_gain, w_query, w_down_kv, w_rope_key, latent_gain, w_key_up, w_value_up, w_out, out_gain, cache_latent, cache_rope, lengths):
    token_values = tokens.astype(jnp.float32)
    scaled = (token_values * token_gain).astype(jnp.bfloat16)
    query_heads = jnp.dot(scaled, w_query, preferred_element_type=jnp.float32).astype(jnp.bfloat16).reshape(BATCH, HEADS, NOPE + ROPE)
    latent_raw = jnp.dot(scaled, w_down_kv, preferred_element_type=jnp.float32)
    rope_raw = jnp.dot(scaled, w_rope_key, preferred_element_type=jnp.float32)
    latent = (latent_raw * lax.rsqrt(lax.optimization_barrier(jnp.mean(latent_raw * latent_raw, axis=1, keepdims=True)) + EPSILON) * latent_gain).astype(jnp.bfloat16)
    cosine, sine_table = angle_tables(lengths, ROPE)
    new_rope = rotate_half(rope_raw, cosine, sine_table).astype(jnp.bfloat16)
    query_nope = query_heads[..., :NOPE]
    query_rope = rotate_half(query_heads[..., NOPE:].astype(jnp.float32), cosine[:, None, :], sine_table[:, None, :]).astype(jnp.bfloat16)
    query_latent = jnp.einsum('bhn,hcn->bhc', query_nope.astype(jnp.float32), w_key_up.astype(jnp.float32)).astype(jnp.bfloat16)
    head_latent = lax.map(attend_one, (query_latent, query_rope, latent, new_rope, lengths, cache_latent, cache_rope))
    head_out = jnp.einsum('bhc,hcv->bhv', head_latent.astype(jnp.float32), w_value_up.astype(jnp.float32)).astype(jnp.bfloat16).reshape(BATCH, HEADS * VDIM)
    mixed_sum = jnp.dot(head_out, w_out, preferred_element_type=jnp.float32)
    out_inverse = lax.rsqrt(lax.optimization_barrier(jnp.mean(mixed_sum * mixed_sum, axis=1)) + EPSILON)[:, None]
    return (mixed_sum * out_inverse * out_gain).astype(jnp.bfloat16)
```

```python
import functools

import jax
import jax.numpy as jnp
import numpy as np
from jax import lax
from jax.experimental import pallas as pl
from jax.experimental.pallas import tpu as pltpu
from jax.sharding import PartitionSpec as P

MESH = pl.DeviceIdType.MESH
EPSILON = 1e-06
NEGATIVE = -1e30
BF16 = jnp.bfloat16
F32 = jnp.float32


def dot(a, b):
    return jnp.dot(a, b, preferred_element_type=F32)


def dot_nt(a, b):
    return lax.dot_general(a, b, (((1,), (1,)), ((), ())), preferred_element_type=F32)


def iota(shape, axis):
    return lax.broadcasted_iota(jnp.int32, shape, axis)


def to_column(row, rows):
    picked = iota((rows, rows), 0) == iota((rows, rows), 1)
    return jnp.sum(jnp.where(picked, row[:, :rows], 0.0), axis=1, keepdims=True)


def to_row(column, rows):
    picked = iota((rows, 128), 0) == iota((rows, 128), 1)
    return jnp.sum(jnp.where(picked, column, 0.0), axis=0, keepdims=True)


def kernel(
    tok_h, tgain_h, wq_h, wd_h, wr_h, lgain_h, wk_h, wv_h, wo_h, ogain_h, cl_h, cr_h, len_h, freq_h,
    out_ref,
    tok, tgain, wq, wd, wr, lgain, wk, wv, wo, ogain, cl, cr, lens, freq,
    len_tab, cos_tab, sin_tab,
    a1_send, a1_recv, a2_send, a2_recv,
    lat_all, lat_send, lat_recv,
    b_send, b_recv, q_tab, o_tab, d_send, d_recv,
    c1_send, c1_recv, c1_lse, c1_lser, c2_send, c2_recv, c2_lse, c2_lser,
    f_recv, f_send, g_send, g_recv,
    load_sem, cache_sem,
    a1_ss, a1_rs, a2_ss, a2_rs, lat_ss, lat_rs, b_ss, b_rs, d_ss, d_rs,
    c1_ss, c1_rs, c2_ss, c2_rs, cl1_ss, cl1_rs, cl2_ss, cl2_rs, f_ss, f_rs, g_ss, g_rs,
):
    kv = lax.axis_index("kv")
    tp = lax.axis_index("tp")
    z = kv // 4
    x = kv % 4

    barrier = pltpu.get_barrier_semaphore()

    def greet_kv(d, c):
        pl.semaphore_signal(barrier, inc=1, device_id=((kv + d) % 16, tp), device_id_type=MESH)
        return c

    def greet_tp(d, c):
        pl.semaphore_signal(barrier, inc=1, device_id=(kv, (tp + d) % 8), device_id_type=MESH)
        return c

    lax.fori_loop(1, 16, greet_kv, 0)
    lax.fori_loop(1, 8, greet_tp, 0)

    pairs = [
        (tok_h, tok), (tgain_h, tgain), (wq_h, wq), (len_h, lens), (freq_h, freq), (wd_h, wd), (wr_h, wr),
        (wk_h, wk), (lgain_h, lgain), (wv_h, wv), (wo_h, wo), (ogain_h, ogain),
    ]
    loads = [pltpu.make_async_copy(s, d, load_sem.at[i]) for i, (s, d) in enumerate(pairs)]
    for copy in loads:
        copy.start()
    cache_loads = []
    for s in range(8):
        cache_loads.append(pltpu.make_async_copy(cl_h.at[s], cl.at[s], cache_sem.at[s]))
        cache_loads.append(pltpu.make_async_copy(cr_h.at[s], cr.at[s], cache_sem.at[8 + s]))
    for copy in cache_loads:
        copy.start()

    for i in range(3):
        loads[i].wait()
    scaled = (tok[...].astype(F32) * tgain[...]).astype(BF16)
    q_part = dot(scaled, wq[...])
    rope_part = q_part[:, 128:192]
    q_nope_part = q_part[:, :128]
    q_rope_part = jnp.concatenate([rope_part[:32], rope_part[32:]], axis=1)
    a1_send[0:64, :] = q_nope_part.astype(BF16)
    a1_send[64:96, :] = q_rope_part.astype(BF16)

    pl.semaphore_wait(barrier, 22)

    def x_dev(d):
        return (z * 4 + (x + d) % 4, tp)

    def z_dev(d):
        return (((z + d) % 4) * 4 + x, tp)

    def line(src, dst, ss, rs, dev):
        return [
            pltpu.make_async_remote_copy(
                src_ref=src, dst_ref=dst.at[d - 1], send_sem=ss.at[d - 1], recv_sem=rs.at[d - 1],
                device_id=dev(d), device_id_type=MESH,
            )
            for d in (1, 2, 3)
        ]

    a1 = line(a1_send, a1_recv, a1_ss, a1_rs, x_dev)
    for copy in a1:
        copy.start()

    for i in range(3, 7):
        loads[i].wait()
    lat_all[:, 0:512] = dot(scaled, wd[...])
    lat_all[:, 512:576] = dot(scaled, wr[...])
    lat_all[:, 576:640] = jnp.zeros((64, 64), F32)
    mine = lat_all[pl.ds(pl.multiple_of(tp * 8, 8), 8), :]
    for r in range(8):
        lat_send[r] = mine[r : r + 1, :]
    lat_recv[kv] = lat_send[kv // 2]

    def lat_copy(d):
        to = (kv + d) % 16
        return pltpu.make_async_remote_copy(
            src_ref=lat_send.at[to // 2], dst_ref=lat_recv.at[kv], send_sem=lat_ss.at[d], recv_sem=lat_rs.at[kv],
            device_id=(to, tp), device_id_type=MESH,
        )

    def lat_start(d, c):
        lat_copy(d).start()
        return c

    lax.fori_loop(1, 16, lat_start, 0)

    len_col = to_column(lens[...].astype(F32), 64)
    len_tab[...] = jnp.broadcast_to(len_col, (64, 128))
    lane = iota((32, 128), 1)
    packed_len = jnp.where(lane < 64, len_col[:32], len_col[32:])
    angle = packed_len * freq[...]
    cosine = jnp.cos(angle)
    sine = jnp.sin(angle)
    sine = jnp.where(lane % 64 < 32, -sine, sine)
    cos_tab[0:32, :] = cosine[:, :64]
    cos_tab[32:64, :] = cosine[:, 64:]
    sin_tab[0:32, :] = sine[:, :64]
    sin_tab[32:64, :] = sine[:, 64:]

    def added(own, recv, rows):
        total = own
        for d in range(3):
            total = total + recv[d, rows, :].astype(F32)
        return total

    for copy in a1:
        copy.wait_recv()
    q_nope_sum = added(q_nope_part, a1_recv, slice(0, 64))
    q_rope_sum = added(q_rope_part, a1_recv, slice(64, 96))
    a2_send[0:64, :] = q_nope_sum.astype(BF16)
    a2_send[64:96, :] = q_rope_sum.astype(BF16)
    a2 = line(a2_send, a2_recv, a2_ss, a2_rs, z_dev)
    for copy in a2:
        copy.start()
    for copy in a2:
        copy.wait_recv()
    q_nope = added(q_nope_sum, a2_recv, slice(0, 64)).astype(BF16)
    q_rope = added(q_rope_sum, a2_recv, slice(64, 96)).astype(BF16).astype(F32)
    swapped = jnp.where(lane % 64 < 32, pltpu.roll(q_rope, 96, 1), pltpu.roll(q_rope, 32, 1))
    q_rope = q_rope * cosine + swapped * sine
    q_rope = jnp.concatenate([q_rope[:, :64], q_rope[:, 64:]], axis=0)

    loads[7].wait()
    q_lat = dot_nt(q_nope, wk[...])
    pad = jnp.zeros((8, 64), F32)
    for j in range(8):
        block = jnp.concatenate([q_lat[8 * j : 8 * j + 8], q_rope[8 * j : 8 * j + 8], pad], axis=1)
        b_send[j] = block.astype(BF16)

    def tp_copy(d, src, dst, ss, rs):
        to = (tp + d) % 8
        return pltpu.make_async_remote_copy(
            src_ref=src.at[to], dst_ref=dst.at[tp], send_sem=ss.at[d], recv_sem=rs.at[tp],
            device_id=(kv, to), device_id_type=MESH,
        )

    def tp_wait_copy(d, src, dst, ss, rs):
        frm = (tp + d) % 8
        return pltpu.make_async_remote_copy(
            src_ref=src.at[frm], dst_ref=dst.at[frm], send_sem=ss.at[d], recv_sem=rs.at[frm],
            device_id=(kv, frm), device_id_type=MESH,
        )

    def tp_exchange(src, dst, ss, rs):
        for d in range(1, 8):
            tp_copy(d, src, dst, ss, rs).start()
        dst[tp] = src[tp]
        for d in range(1, 8):
            tp_wait_copy(d, src, dst, ss, rs).wait_recv()

    tp_exchange(b_send, b_recv, b_ss, b_rs)

    r64 = iota((64, 64), 0)
    c64 = iota((64, 64), 1)
    swap = (c64 == (r64 % 8) * 8 + r64 // 8).astype(BF16)
    queries = jnp.concatenate([b_recv[h].astype(F32) for h in range(8)], axis=0).astype(BF16)
    queries = dot(swap, queries)
    for s in range(8):
        q_tab[s] = queries[8 * s : 8 * s + 8]

    def lat_wait(d, c):
        frm = (kv + d) % 16
        pltpu.make_async_remote_copy(
            src_ref=lat_send.at[kv // 2], dst_ref=lat_recv.at[frm], send_sem=lat_ss.at[d], recv_sem=lat_rs.at[frm],
            device_id=(frm, tp), device_id_type=MESH,
        ).wait_recv()
        return c

    lax.fori_loop(1, 16, lat_wait, 0)
    lat_sum = lat_recv[0]
    for k in range(1, 16):
        lat_sum = lat_sum + lat_recv[k]
    loads[8].wait()
    lat_raw = lat_sum[:, :512]
    latent = (
        lat_raw * lax.rsqrt(jnp.mean(lat_raw * lat_raw, axis=1, keepdims=True) + EPSILON) * lgain[...]
    ).astype(BF16).astype(F32)
    key_raw = lat_sum[:, 512:576]
    new_seq = kv // 2
    new_row = tp * 8 + new_seq
    key_swapped = jnp.concatenate([key_raw[:, 32:], key_raw[:, :32]], axis=1)
    new_rope = key_raw * cos_tab[pl.ds(new_row, 1), :] + key_swapped * sin_tab[pl.ds(new_row, 1), :]
    new_rope = new_rope.astype(BF16).astype(F32)
    factor = 192.0 ** (-0.5)
    q_new = q_tab[new_seq]
    new_score = (
        jnp.sum(q_new[:, :512] * latent, axis=1, keepdims=True)
        + jnp.sum(q_new[:, 512:576] * new_rope, axis=1, keepdims=True)
    ) * factor

    positions = (kv * 512 + iota((8, 512), 1)).astype(F32)
    lane8 = iota((8, 128), 1)
    for s in range(8):
        cache_loads[2 * s].wait()
        cache_loads[2 * s + 1].wait()
        q = q_tab[s].astype(BF16)
        scores = (dot_nt(q[:, :512], cl[s]) + dot_nt(q[:, 512:576], cr[s])) * factor
        length = len_tab[pl.ds(tp * 8 + s, 1), 0:1]
        visible = positions < length
        is_new = jnp.logical_and(new_seq == s, kv % 2 == 0)
        own_new = jnp.where(is_new, new_score, NEGATIVE)
        top = jnp.maximum(jnp.max(jnp.where(visible, scores, NEGATIVE), axis=1, keepdims=True), own_new)
        weights = jnp.where(visible, jnp.exp(scores - top), 0.0)
        new_weight = jnp.where(is_new, jnp.exp(own_new - top), 0.0)
        total = jnp.sum(weights, axis=1, keepdims=True) + new_weight
        acc = dot(weights.astype(BF16), cl[s]) + new_weight.astype(BF16).astype(F32) * latent
        some = total > 0.0
        safe = jnp.where(some, total, 1.0)
        lse = jnp.where(some, top + jnp.log(safe), NEGATIVE)
        hi = lse.astype(BF16).astype(F32)
        mid = (lse - hi).astype(BF16).astype(F32)
        low = lse - hi - mid
        o_tab[8 * s : 8 * s + 8, 0:512] = acc / safe
        o_tab[8 * s : 8 * s + 8, 512:640] = jnp.where(
            lane8 == 0, hi, jnp.where(lane8 == 1, mid, jnp.where(lane8 == 2, low, 0.0))
        )

    by_head = dot(swap, o_tab[...].astype(BF16))
    for h in range(8):
        d_send[h] = by_head[8 * h : 8 * h + 8].astype(BF16)
    tp_exchange(d_send, d_recv, d_ss, d_rs)

    parts = jnp.concatenate([d_recv[j].astype(F32) for j in range(8)], axis=0)
    lse = jnp.sum(parts[:, 512:640], axis=1, keepdims=True)
    loads[9].wait()
    value = dot(parts[:, :512].astype(BF16), wv[...])

    def combine(value, lse, send, recv, lse_send, lse_recv, sems, dev):
        send[...] = value.astype(BF16)
        lse_send[...] = to_row(lse, 64)
        copies = line(send, recv, sems[0], sems[1], dev)
        lse_copies = line(lse_send, lse_recv, sems[2], sems[3], dev)
        for copy in lse_copies + copies:
            copy.start()
        for copy in lse_copies:
            copy.wait_recv()
        others = [to_column(lse_recv[d], 64) for d in range(3)]
        top = lse
        for other in others:
            top = jnp.maximum(top, other)
        own_scale = jnp.exp(lse - top)
        scales = [jnp.exp(other - top) for other in others]
        total = own_scale + scales[0] + scales[1] + scales[2]
        for copy in copies:
            copy.wait_recv()
        merged = value * (own_scale / total)
        for d in range(3):
            merged = merged + recv[d].astype(F32) * (scales[d] / total)
        return merged, top + jnp.log(total), copies + lse_copies

    value, lse, c1 = combine(
        value, lse, c1_send, c1_recv, c1_lse, c1_lser, (c1_ss, c1_rs, cl1_ss, cl1_rs), x_dev
    )
    value, lse, c2 = combine(
        value, lse, c2_send, c2_recv, c2_lse, c2_lser, (c2_ss, c2_rs, cl2_ss, cl2_rs), z_dev
    )
    head_out = value.astype(BF16)

    loads[10].wait()
    f_send[...] = dot(head_out, wo[...]).astype(BF16)

    def f_copy(d, slot, to):
        return pltpu.make_async_remote_copy(
            src_ref=f_send, dst_ref=f_recv.at[slot], send_sem=f_ss.at[d], recv_sem=f_rs.at[slot],
            device_id=(kv, to), device_id_type=MESH,
        )

    for d in range(1, 8):
        f_copy(d, tp, (tp + d) % 8).start()
    f_recv[tp] = f_send[...]
    for d in range(1, 8):
        frm = (tp + d) % 8
        f_copy(d, frm, frm).wait_recv()
    mixed = f_recv[0].astype(F32)
    for h in range(1, 8):
        mixed = mixed + f_recv[h].astype(F32)

    g_send[...] = to_row(jnp.sum(mixed * mixed, axis=1, keepdims=True), 64)

    def g_copy(d, slot, to):
        return pltpu.make_async_remote_copy(
            src_ref=g_send, dst_ref=g_recv.at[slot], send_sem=g_ss.at[d], recv_sem=g_rs.at[slot],
            device_id=(to, tp), device_id_type=MESH,
        )

    def g_start(d, c):
        g_copy(d, kv, (kv + d) % 16).start()
        return c

    def g_wait(d, c):
        frm = (kv + d) % 16
        g_copy(d, frm, frm).wait_recv()
        return c

    lax.fori_loop(1, 16, g_start, 0)
    g_recv[kv] = g_send[...]
    loads[11].wait()
    lax.fori_loop(1, 16, g_wait, 0)
    squares = g_recv[0]
    for k in range(1, 16):
        squares = squares + g_recv[k]
    inverse = to_column(lax.rsqrt(squares / 2048.0 + EPSILON), 64)
    out_ref[...] = (mixed * inverse * ogain[...]).astype(BF16)

    for copy in a1 + a2 + c1 + c2:
        copy.wait_send()

    def drain_kv(d, c):
        lat_copy(d).wait_send()
        g_copy(d, kv, (kv + d) % 16).wait_send()
        return c

    def drain_tp(d, c):
        tp_copy(d, b_send, b_recv, b_ss, b_rs).wait_send()
        tp_copy(d, d_send, d_recv, d_ss, d_rs).wait_send()
        f_copy(d, tp, (tp + d) % 8).wait_send()
        return c

    lax.fori_loop(1, 16, drain_kv, 0)
    lax.fori_loop(1, 8, drain_tp, 0)


def on_device(
    tokens, token_gain, w_query, w_down_kv, w_rope_key, latent_gain, w_key_up, w_value_up, w_out, out_gain,
    cache_latent, cache_rope, lengths,
):
    freq = 1.0 / 10000.0 ** (np.arange(0, 64, 2, dtype=np.float32) / np.float32(64.0))
    freq = jnp.asarray(np.tile(freq.astype(np.float32), 4)[None, :])
    operands = (
        tokens, token_gain.reshape(1, 128), w_query, w_down_kv, w_rope_key, latent_gain.reshape(1, 512),
        w_key_up.reshape(512, 128), w_value_up.reshape(512, 128), w_out, out_gain.reshape(1, 128),
        cache_latent, cache_rope, lengths.reshape(1, 64), freq,
    )
    order = (0, 1, 2, 3, 4, 5, 6, 7, 8, 9, 10, 11, 12, 13)
    local = [pltpu.VMEM(operands[i].shape, operands[i].dtype) for i in order]
    dma = pltpu.SemaphoreType.DMA
    scratch = local + [
        pltpu.VMEM((64, 128), F32), pltpu.VMEM((64, 64), F32), pltpu.VMEM((64, 64), F32),
        pltpu.VMEM((96, 128), BF16), pltpu.VMEM((3, 96, 128), BF16),
        pltpu.VMEM((96, 128), BF16), pltpu.VMEM((3, 96, 128), BF16),
        pltpu.VMEM((64, 640), F32), pltpu.VMEM((8, 1, 640), F32), pltpu.VMEM((16, 1, 640), F32),
        pltpu.VMEM((8, 8, 640), BF16), pltpu.VMEM((8, 8, 640), BF16),
        pltpu.VMEM((8, 8, 640), F32), pltpu.VMEM((64, 640), F32),
        pltpu.VMEM((8, 8, 640), BF16), pltpu.VMEM((8, 8, 640), BF16),
        pltpu.VMEM((64, 128), BF16), pltpu.VMEM((3, 64, 128), BF16),
        pltpu.VMEM((1, 128), F32), pltpu.VMEM((3, 1, 128), F32),
        pltpu.VMEM((64, 128), BF16), pltpu.VMEM((3, 64, 128), BF16),
        pltpu.VMEM((1, 128), F32), pltpu.VMEM((3, 1, 128), F32),
        pltpu.VMEM((8, 64, 128), BF16), pltpu.VMEM((64, 128), BF16),
        pltpu.VMEM((1, 128), F32), pltpu.VMEM((16, 1, 128), F32),
        dma((12,)), dma((16,)),
        dma((3,)), dma((3,)), dma((3,)), dma((3,)), dma((16,)), dma((16,)),
        dma((8,)), dma((8,)), dma((8,)), dma((8,)),
        dma((3,)), dma((3,)), dma((3,)), dma((3,)), dma((3,)), dma((3,)), dma((3,)), dma((3,)),
        dma((8,)), dma((8,)), dma((16,)), dma((16,)),
    ]
    return pl.pallas_call(
        kernel,
        out_shape=jax.ShapeDtypeStruct((64, 128), BF16),
        in_specs=[pl.BlockSpec(memory_space=pl.ANY)] * len(operands),
        out_specs=pl.BlockSpec(memory_space=pltpu.VMEM),
        scratch_shapes=scratch,
        compiler_params=pltpu.CompilerParams(
            collective_id=0, has_side_effects=True, vmem_limit_bytes=48 * 1024 * 1024
        ),
    )(*operands)


def solution(mesh):
    return jax.shard_map(
        on_device,
        mesh=mesh,
        in_specs=(
            P(None, "kv"), P("kv"), P("kv", "tp"), P("kv", None), P("kv", None), P(),
            P("tp", None, None), P("tp", None, None), P("tp", "kv"), P("kv"),
            P("tp", "kv", None), P("tp", "kv", None), P(),
        ),
        out_specs=P(None, "kv"),
        check_vma=False,
    )
```

```python
import functools

import jax
import jax.numpy as jnp
import numpy as np
from jax import lax
from jax.experimental import pallas as pl
from jax.experimental.pallas import tpu as pltpu
from jax.sharding import PartitionSpec as P

MESH = pl.DeviceIdType.MESH
EPSILON = 1e-06
NEGATIVE = -1e30
BF16 = jnp.bfloat16
F32 = jnp.float32


def dot(a, b):
    return jnp.dot(a, b, preferred_element_type=F32)


def dot_nt(a, b):
    return lax.dot_general(a, b, (((1,), (1,)), ((), ())), preferred_element_type=F32)


def iota(shape, axis):
    return lax.broadcasted_iota(jnp.int32, shape, axis)


def to_column(row, rows):
    picked = iota((rows, rows), 0) == iota((rows, rows), 1)
    return jnp.sum(jnp.where(picked, row[:, :rows], 0.0), axis=1, keepdims=True)


def to_row(column, rows):
    picked = iota((rows, 128), 0) == iota((rows, 128), 1)
    return jnp.sum(jnp.where(picked, column, 0.0), axis=0, keepdims=True)


def kernel(
    tok_h, tgain_h, wq_h, wd_h, wr_h, lgain_h, wk_h, wv_h, wo_h, ogain_h, cl_h, cr_h, len_h, freq_h,
    out_ref,
    tok, tgain, wq, wd, wr, lgain, wk, wv, wo, ogain, cl, cr, lens, freq,
    len_tab, cos_tab, sin_tab,
    a1_send, a1_recv, a2_send, a2_recv,
    lat_all, lat_send, lat_recv,
    b_send, b_recv, q_tab, o_tab, d_send, d_recv,
    c1_send, c1_recv, c1_lse, c1_lser, c2_send, c2_recv, c2_lse, c2_lser,
    f_recv, f_send, g_send, g_recv,
    load_sem, cache_sem,
    a1_ss, a1_rs, a2_ss, a2_rs, lat_ss, lat_rs, b_ss, b_rs, d_ss, d_rs,
    c1_ss, c1_rs, c2_ss, c2_rs, cl1_ss, cl1_rs, cl2_ss, cl2_rs, f_ss, f_rs, g_ss, g_rs,
):
    kv = lax.axis_index("kv")
    tp = lax.axis_index("tp")
    z = kv // 4
    x = kv % 4

    barrier = pltpu.get_barrier_semaphore()

    def greet_kv(d, c):
        pl.semaphore_signal(barrier, inc=1, device_id=((kv + d) % 16, tp), device_id_type=MESH)
        return c

    def greet_tp(d, c):
        pl.semaphore_signal(barrier, inc=1, device_id=(kv, (tp + d) % 8), device_id_type=MESH)
        return c

    lax.fori_loop(1, 16, greet_kv, 0)
    lax.fori_loop(1, 8, greet_tp, 0)

    pairs = [
        (tok_h, tok), (tgain_h, tgain), (wq_h, wq), (len_h, lens), (freq_h, freq), (wd_h, wd), (wr_h, wr),
        (wk_h, wk), (lgain_h, lgain), (wv_h, wv), (wo_h, wo), (ogain_h, ogain),
    ]
    loads = [pltpu.make_async_copy(s, d, load_sem.at[i]) for i, (s, d) in enumerate(pairs)]
    for copy in loads:
        copy.start()
    cache_loads = []
    for s in range(8):
        cache_loads.append(pltpu.make_async_copy(cl_h.at[s], cl.at[s], cache_sem.at[s]))
        cache_loads.append(pltpu.make_async_copy(cr_h.at[s], cr.at[s], cache_sem.at[8 + s]))
    for copy in cache_loads:
        copy.start()

    for i in range(3):
        loads[i].wait()
    scaled = (tok[...].astype(F32) * tgain[...]).astype(BF16)
    q_part = dot_nt(scaled, wq[...])
    rope_part = q_part[:, 128:192]
    q_nope_part = q_part[:, :128]
    q_rope_part = jnp.concatenate([rope_part[:32], rope_part[32:]], axis=1)
    a1_send[0:64, :] = q_nope_part.astype(BF16)
    a1_send[64:96, :] = q_rope_part.astype(BF16)

    pl.semaphore_wait(barrier, 22)

    def x_dev(d):
        return (z * 4 + (x + d) % 4, tp)

    def z_dev(d):
        return (((z + d) % 4) * 4 + x, tp)

    def line(src, dst, ss, rs, dev):
        return [
            pltpu.make_async_remote_copy(
                src_ref=src, dst_ref=dst.at[d - 1], send_sem=ss.at[d - 1], recv_sem=rs.at[d - 1],
                device_id=dev(d), device_id_type=MESH,
            )
            for d in (1, 2, 3)
        ]

    a1 = line(a1_send, a1_recv, a1_ss, a1_rs, x_dev)
    for copy in a1:
        copy.start()

    for i in range(3, 7):
        loads[i].wait()
    lat_all[:, 0:512] = dot(scaled, wd[...])
    lat_all[:, 512:576] = dot_nt(scaled, wr[...])
    lat_all[:, 576:640] = jnp.zeros((64, 64), F32)
    mine = lat_all[pl.ds(pl.multiple_of(tp * 8, 8), 8), :]
    for r in range(8):
        lat_send[r] = mine[r : r + 1, :]
    lat_recv[kv] = lat_send[kv // 2]

    def lat_copy(d):
        to = (kv + d) % 16
        return pltpu.make_async_remote_copy(
            src_ref=lat_send.at[to // 2], dst_ref=lat_recv.at[kv], send_sem=lat_ss.at[d], recv_sem=lat_rs.at[kv],
            device_id=(to, tp), device_id_type=MESH,
        )

    def lat_start(d, c):
        lat_copy(d).start()
        return c

    lax.fori_loop(1, 16, lat_start, 0)

    len_col = to_column(lens[...].astype(F32), 64)
    len_tab[...] = jnp.broadcast_to(len_col, (64, 128))
    lane = iota((32, 128), 1)
    packed_len = jnp.where(lane < 64, len_col[:32], len_col[32:])
    angle = packed_len * freq[...]
    cosine = jnp.cos(angle)
    sine = jnp.sin(angle)
    sine = jnp.where(lane % 64 < 32, -sine, sine)
    cos_tab[0:32, :] = cosine[:, :64]
    cos_tab[32:64, :] = cosine[:, 64:]
    sin_tab[0:32, :] = sine[:, :64]
    sin_tab[32:64, :] = sine[:, 64:]

    def added(own, recv, rows):
        total = own
        for d in range(3):
            total = total + recv[d, rows, :].astype(F32)
        return total

    for copy in a1:
        copy.wait_recv()
    q_nope_sum = added(q_nope_part, a1_recv, slice(0, 64))
    q_rope_sum = added(q_rope_part, a1_recv, slice(64, 96))
    a2_send[0:64, :] = q_nope_sum.astype(BF16)
    a2_send[64:96, :] = q_rope_sum.astype(BF16)
    a2 = line(a2_send, a2_recv, a2_ss, a2_rs, z_dev)
    for copy in a2:
        copy.start()
    for copy in a2:
        copy.wait_recv()
    q_nope = added(q_nope_sum, a2_recv, slice(0, 64)).astype(BF16)
    q_rope = added(q_rope_sum, a2_recv, slice(64, 96)).astype(BF16).astype(F32)
    swapped = jnp.where(lane % 64 < 32, pltpu.roll(q_rope, 96, 1), pltpu.roll(q_rope, 32, 1))
    q_rope = q_rope * cosine + swapped * sine
    q_rope = jnp.concatenate([q_rope[:, :64], q_rope[:, 64:]], axis=0)

    loads[7].wait()
    q_lat = dot_nt(q_nope, wk[...])
    pad = jnp.zeros((8, 64), F32)
    for j in range(8):
        block = jnp.concatenate([q_lat[8 * j : 8 * j + 8], q_rope[8 * j : 8 * j + 8], pad], axis=1)
        b_send[j] = block.astype(BF16)

    def tp_copy(d, src, dst, ss, rs):
        to = (tp + d) % 8
        return pltpu.make_async_remote_copy(
            src_ref=src.at[to], dst_ref=dst.at[tp], send_sem=ss.at[d], recv_sem=rs.at[tp],
            device_id=(kv, to), device_id_type=MESH,
        )

    def tp_wait_copy(d, src, dst, ss, rs):
        frm = (tp + d) % 8
        return pltpu.make_async_remote_copy(
            src_ref=src.at[frm], dst_ref=dst.at[frm], send_sem=ss.at[d], recv_sem=rs.at[frm],
            device_id=(kv, frm), device_id_type=MESH,
        )

    def tp_exchange(src, dst, ss, rs):
        for d in range(1, 8):
            tp_copy(d, src, dst, ss, rs).start()
        dst[tp] = src[tp]
        for d in range(1, 8):
            tp_wait_copy(d, src, dst, ss, rs).wait_recv()

    tp_exchange(b_send, b_recv, b_ss, b_rs)

    r64 = iota((64, 64), 0)
    c64 = iota((64, 64), 1)
    swap = (c64 == (r64 % 8) * 8 + r64 // 8).astype(BF16)
    queries = jnp.concatenate([b_recv[h].astype(F32) for h in range(8)], axis=0).astype(BF16)
    queries = dot(swap, queries)
    for s in range(8):
        q_tab[s] = queries[8 * s : 8 * s + 8]

    def lat_wait(d, c):
        frm = (kv + d) % 16
        pltpu.make_async_remote_copy(
            src_ref=lat_send.at[kv // 2], dst_ref=lat_recv.at[frm], send_sem=lat_ss.at[d], recv_sem=lat_rs.at[frm],
            device_id=(frm, tp), device_id_type=MESH,
        ).wait_recv()
        return c

    lax.fori_loop(1, 16, lat_wait, 0)
    lat_sum = lat_recv[0]
    for k in range(1, 16):
        lat_sum = lat_sum + lat_recv[k]
    loads[8].wait()
    lat_raw = lat_sum[:, :512]
    latent = (
        lat_raw * lax.rsqrt(jnp.mean(lat_raw * lat_raw, axis=1, keepdims=True) + EPSILON) * lgain[...]
    ).astype(BF16).astype(F32)
    key_raw = lat_sum[:, 512:576]
    new_seq = kv // 2
    new_row = tp * 8 + new_seq
    key_swapped = jnp.concatenate([key_raw[:, 32:], key_raw[:, :32]], axis=1)
    new_rope = key_raw * cos_tab[pl.ds(new_row, 1), :] + key_swapped * sin_tab[pl.ds(new_row, 1), :]
    new_rope = new_rope.astype(BF16).astype(F32)
    factor = 192.0 ** (-0.5)
    q_new = q_tab[new_seq]
    new_score = (
        jnp.sum(q_new[:, :512] * latent, axis=1, keepdims=True)
        + jnp.sum(q_new[:, 512:576] * new_rope, axis=1, keepdims=True)
    ) * factor

    positions = (kv * 512 + iota((8, 512), 1)).astype(F32)
    lane8 = iota((8, 128), 1)
    for s in range(8):
        cache_loads[2 * s].wait()
        cache_loads[2 * s + 1].wait()
        q = q_tab[s].astype(BF16)
        scores = (dot_nt(q[:, :512], cl[s]) + dot(q[:, 512:576], cr[s])) * factor
        length = len_tab[pl.ds(tp * 8 + s, 1), 0:1]
        visible = positions < length
        is_new = jnp.logical_and(new_seq == s, kv % 2 == 0)
        own_new = jnp.where(is_new, new_score, NEGATIVE)
        top = jnp.maximum(jnp.max(jnp.where(visible, scores, NEGATIVE), axis=1, keepdims=True), own_new)
        weights = jnp.where(visible, jnp.exp(scores - top), 0.0)
        new_weight = jnp.where(is_new, jnp.exp(own_new - top), 0.0)
        total = jnp.sum(weights, axis=1, keepdims=True) + new_weight
        acc = dot(weights.astype(BF16), cl[s]) + new_weight.astype(BF16).astype(F32) * latent
        some = total > 0.0
        safe = jnp.where(some, total, 1.0)
        lse = jnp.where(some, top + jnp.log(safe), NEGATIVE)
        hi = lse.astype(BF16).astype(F32)
        mid = (lse - hi).astype(BF16).astype(F32)
        low = lse - hi - mid
        o_tab[8 * s : 8 * s + 8, 0:512] = acc / safe
        o_tab[8 * s : 8 * s + 8, 512:640] = jnp.where(
            lane8 == 0, hi, jnp.where(lane8 == 1, mid, jnp.where(lane8 == 2, low, 0.0))
        )

    by_head = dot(swap, o_tab[...].astype(BF16))
    for h in range(8):
        d_send[h] = by_head[8 * h : 8 * h + 8].astype(BF16)
    tp_exchange(d_send, d_recv, d_ss, d_rs)

    parts = jnp.concatenate([d_recv[j].astype(F32) for j in range(8)], axis=0)
    lse = jnp.sum(parts[:, 512:640], axis=1, keepdims=True)
    loads[9].wait()
    value = dot(parts[:, :512].astype(BF16), wv[...])

    def combine(value, lse, send, recv, lse_send, lse_recv, sems, dev):
        send[...] = value.astype(BF16)
        lse_send[...] = to_row(lse, 64)
        copies = line(send, recv, sems[0], sems[1], dev)
        lse_copies = line(lse_send, lse_recv, sems[2], sems[3], dev)
        for copy in lse_copies + copies:
            copy.start()
        for copy in lse_copies:
            copy.wait_recv()
        others = [to_column(lse_recv[d], 64) for d in range(3)]
        top = lse
        for other in others:
            top = jnp.maximum(top, other)
        own_scale = jnp.exp(lse - top)
        scales = [jnp.exp(other - top) for other in others]
        total = own_scale + scales[0] + scales[1] + scales[2]
        for copy in copies:
            copy.wait_recv()
        merged = value * (own_scale / total)
        for d in range(3):
            merged = merged + recv[d].astype(F32) * (scales[d] / total)
        return merged, top + jnp.log(total), copies + lse_copies

    value, lse, c1 = combine(
        value, lse, c1_send, c1_recv, c1_lse, c1_lser, (c1_ss, c1_rs, cl1_ss, cl1_rs), x_dev
    )
    value, lse, c2 = combine(
        value, lse, c2_send, c2_recv, c2_lse, c2_lser, (c2_ss, c2_rs, cl2_ss, cl2_rs), z_dev
    )
    head_out = value.astype(BF16)

    loads[10].wait()
    f_send[...] = dot(head_out, wo[...]).astype(BF16)

    def f_copy(d, slot, to):
        return pltpu.make_async_remote_copy(
            src_ref=f_send, dst_ref=f_recv.at[slot], send_sem=f_ss.at[d], recv_sem=f_rs.at[slot],
            device_id=(kv, to), device_id_type=MESH,
        )

    for d in range(1, 8):
        f_copy(d, tp, (tp + d) % 8).start()
    f_recv[tp] = f_send[...]
    for d in range(1, 8):
        frm = (tp + d) % 8
        f_copy(d, frm, frm).wait_recv()
    mixed = f_recv[0].astype(F32)
    for h in range(1, 8):
        mixed = mixed + f_recv[h].astype(F32)

    g_send[...] = to_row(jnp.sum(mixed * mixed, axis=1, keepdims=True), 64)

    def g_copy(d, slot, to):
        return pltpu.make_async_remote_copy(
            src_ref=g_send, dst_ref=g_recv.at[slot], send_sem=g_ss.at[d], recv_sem=g_rs.at[slot],
            device_id=(to, tp), device_id_type=MESH,
        )

    def g_start(d, c):
        g_copy(d, kv, (kv + d) % 16).start()
        return c

    def g_wait(d, c):
        frm = (kv + d) % 16
        g_copy(d, frm, frm).wait_recv()
        return c

    lax.fori_loop(1, 16, g_start, 0)
    g_recv[kv] = g_send[...]
    loads[11].wait()
    lax.fori_loop(1, 16, g_wait, 0)
    squares = g_recv[0]
    for k in range(1, 16):
        squares = squares + g_recv[k]
    inverse = to_column(lax.rsqrt(squares / 2048.0 + EPSILON), 64)
    out_ref[...] = (mixed * inverse * ogain[...]).astype(BF16)

    for copy in a1 + a2 + c1 + c2:
        copy.wait_send()

    def drain_kv(d, c):
        lat_copy(d).wait_send()
        g_copy(d, kv, (kv + d) % 16).wait_send()
        return c

    def drain_tp(d, c):
        tp_copy(d, b_send, b_recv, b_ss, b_rs).wait_send()
        tp_copy(d, d_send, d_recv, d_ss, d_rs).wait_send()
        f_copy(d, tp, (tp + d) % 8).wait_send()
        return c

    lax.fori_loop(1, 16, drain_kv, 0)
    lax.fori_loop(1, 8, drain_tp, 0)


def on_device(
    tokens, token_gain, w_query, w_down_kv, w_rope_key, latent_gain, w_key_up, w_value_up, w_out, out_gain,
    cache_latent, cache_rope, lengths,
):
    freq = 1.0 / 10000.0 ** (np.arange(0, 64, 2, dtype=np.float32) / np.float32(64.0))
    freq = jnp.asarray(np.tile(freq.astype(np.float32), 4)[None, :])
    operands = (
        tokens, token_gain.reshape(1, 128), w_query.T, w_down_kv, w_rope_key.T, latent_gain.reshape(1, 512),
        w_key_up.reshape(512, 128), w_value_up.reshape(512, 128), w_out, out_gain.reshape(1, 128),
        cache_latent, cache_rope.transpose(0, 2, 1), lengths.reshape(1, 64), freq,
    )
    order = (0, 1, 2, 3, 4, 5, 6, 7, 8, 9, 10, 11, 12, 13)
    local = [pltpu.VMEM(operands[i].shape, operands[i].dtype) for i in order]
    dma = pltpu.SemaphoreType.DMA
    scratch = local + [
        pltpu.VMEM((64, 128), F32), pltpu.VMEM((64, 64), F32), pltpu.VMEM((64, 64), F32),
        pltpu.VMEM((96, 128), BF16), pltpu.VMEM((3, 96, 128), BF16),
        pltpu.VMEM((96, 128), BF16), pltpu.VMEM((3, 96, 128), BF16),
        pltpu.VMEM((64, 640), F32), pltpu.VMEM((8, 1, 640), F32), pltpu.VMEM((16, 1, 640), F32),
        pltpu.VMEM((8, 8, 640), BF16), pltpu.VMEM((8, 8, 640), BF16),
        pltpu.VMEM((8, 8, 640), F32), pltpu.VMEM((64, 640), F32),
        pltpu.VMEM((8, 8, 640), BF16), pltpu.VMEM((8, 8, 640), BF16),
        pltpu.VMEM((64, 128), BF16), pltpu.VMEM((3, 64, 128), BF16),
        pltpu.VMEM((1, 128), F32), pltpu.VMEM((3, 1, 128), F32),
        pltpu.VMEM((64, 128), BF16), pltpu.VMEM((3, 64, 128), BF16),
        pltpu.VMEM((1, 128), F32), pltpu.VMEM((3, 1, 128), F32),
        pltpu.VMEM((8, 64, 128), BF16), pltpu.VMEM((64, 128), BF16),
        pltpu.VMEM((1, 128), F32), pltpu.VMEM((16, 1, 128), F32),
        dma((12,)), dma((16,)),
        dma((3,)), dma((3,)), dma((3,)), dma((3,)), dma((16,)), dma((16,)),
        dma((8,)), dma((8,)), dma((8,)), dma((8,)),
        dma((3,)), dma((3,)), dma((3,)), dma((3,)), dma((3,)), dma((3,)), dma((3,)), dma((3,)),
        dma((8,)), dma((8,)), dma((16,)), dma((16,)),
    ]
    return pl.pallas_call(
        kernel,
        out_shape=jax.ShapeDtypeStruct((64, 128), BF16),
        in_specs=[pl.BlockSpec(memory_space=pl.ANY)] * len(operands),
        out_specs=pl.BlockSpec(memory_space=pltpu.VMEM),
        scratch_shapes=scratch,
        compiler_params=pltpu.CompilerParams(
            collective_id=0, has_side_effects=True, vmem_limit_bytes=67043328
        ),
    )(*operands)


def solution(mesh):
    return jax.shard_map(
        on_device,
        mesh=mesh,
        in_specs=(
            P(None, "kv"), P("kv"), P("kv", "tp"), P("kv", None), P("kv", None), P(),
            P("tp", None, None), P("tp", None, None), P("tp", "kv"), P("kv"),
            P("tp", "kv", None), P("tp", "kv", None), P(),
        ),
        out_specs=P(None, "kv"),
        check_vma=False,
    )
```

```python
import functools

import jax
import jax.numpy as jnp
import numpy as np
from jax import lax
from jax.experimental import pallas as pl
from jax.experimental.pallas import tpu as pltpu
from jax.sharding import PartitionSpec as P

MESH = pl.DeviceIdType.MESH
EPSILON = 1e-06
NEGATIVE = -1e30
BF16 = jnp.bfloat16
F32 = jnp.float32


def dot(a, b):
    return jnp.dot(a, b, preferred_element_type=F32)


def dot_nt(a, b):
    return lax.dot_general(a, b, (((1,), (1,)), ((), ())), preferred_element_type=F32)


def iota(shape, axis):
    return lax.broadcasted_iota(jnp.int32, shape, axis)


def to_column(row, rows):
    picked = iota((rows, rows), 0) == iota((rows, rows), 1)
    return jnp.sum(jnp.where(picked, row[:, :rows], 0.0), axis=1, keepdims=True)


def to_row(column, rows):
    picked = iota((rows, 128), 0) == iota((rows, 128), 1)
    return jnp.sum(jnp.where(picked, column, 0.0), axis=0, keepdims=True)


def kernel(
    tok_h, tgain_h, wq_h, wd_h, wr_h, lgain_h, wk_h, wv_h, wo_h, ogain_h, cl_h, cr_h, len_h, freq_h,
    out_ref,
    tok, tgain, wq, wd, wr, lgain, wk, wv, wo, ogain, cl, cr, lens, freq,
    len_tab, cos_tab, sin_tab,
    a1_send, a1_recv, a2_send, a2_recv,
    lat_all, lat_send, lat_recv,
    b_send, b_recv, q_tab, o_tab,
    c1_send, c1_recv, c1_lse, c1_lser, c2_send, c2_recv, c2_lse, c2_lser,
    m_send, m_recv, g_send, g_recv,
    load_sem, cache_sem,
    a1_ss, a1_rs, a2_ss, a2_rs, lat_ss, lat_rs, b_ss, b_rs, gv_ss, gv_rs, go_ss, go_rs,
    c1_ss, c1_rs, c2_ss, c2_rs, cl1_ss, cl1_rs, cl2_ss, cl2_rs, m_ss, m_rs, g_ss, g_rs,
):
    kv = lax.axis_index("kv")
    tp = lax.axis_index("tp")
    z = kv // 4
    x = kv % 4

    barrier = pltpu.get_barrier_semaphore()

    def greet_line(d, c):
        pl.semaphore_signal(barrier, inc=1, device_id=(z * 4 + (x + d) % 4, tp), device_id_type=MESH)
        pl.semaphore_signal(barrier, inc=1, device_id=((z + d) % 4 * 4 + x, tp), device_id_type=MESH)
        return c

    def greet_tp(d, c):
        pl.semaphore_signal(barrier, inc=1, device_id=(kv, (tp + d) % 8), device_id_type=MESH)
        return c

    lax.fori_loop(1, 4, greet_line, 0)
    lax.fori_loop(1, 8, greet_tp, 0)

    pairs = [
        (tok_h, tok), (tgain_h, tgain), (wq_h, wq), (len_h, lens), (freq_h, freq), (wd_h, wd), (wr_h, wr),
        (wk_h, wk), (lgain_h, lgain), (wv_h, wv.at[tp]), (wo_h, wo.at[tp]), (ogain_h, ogain),
    ]
    loads = [pltpu.make_async_copy(s, d, load_sem.at[i]) for i, (s, d) in enumerate(pairs)]
    for copy in loads:
        copy.start()
    cache_loads = []
    for s in range(8):
        cache_loads.append(pltpu.make_async_copy(cl_h.at[s], cl.at[s], cache_sem.at[s]))
        cache_loads.append(pltpu.make_async_copy(cr_h.at[s], cr.at[s], cache_sem.at[8 + s]))
    for copy in cache_loads:
        copy.start()

    for i in range(3):
        loads[i].wait()
    scaled = (tok[...].astype(F32) * tgain[...]).astype(BF16)
    q_part = dot_nt(scaled, wq[...])
    rope_part = q_part[:, 128:192]
    q_nope_part = q_part[:, :128]
    q_rope_part = jnp.concatenate([rope_part[:32], rope_part[32:]], axis=1)
    a1_send[0:64, :] = q_nope_part.astype(BF16)
    a1_send[64:96, :] = q_rope_part.astype(BF16)

    pl.semaphore_wait(barrier, 13)

    def x_dev(d):
        return (z * 4 + (x + d) % 4, tp)

    def z_dev(d):
        return (((z + d) % 4) * 4 + x, tp)

    def line(src, dst, ss, rs, dev):
        return [
            pltpu.make_async_remote_copy(
                src_ref=src, dst_ref=dst.at[d - 1], send_sem=ss.at[d - 1], recv_sem=rs.at[d - 1],
                device_id=dev(d), device_id_type=MESH,
            )
            for d in (1, 2, 3)
        ]

    a1 = line(a1_send, a1_recv, a1_ss, a1_rs, x_dev)
    for copy in a1:
        copy.start()

    twin = tp + 1 - 2 * (tp % 2)

    def gather_copy(buf, ss, rs, i, slot, to):
        return pltpu.make_async_remote_copy(
            src_ref=buf.at[slot], dst_ref=buf.at[slot], send_sem=ss.at[i], recv_sem=rs.at[slot],
            device_id=(kv, to), device_id_type=MESH,
        )

    def gather_first(buf, ss, rs):
        copies = [gather_copy(buf, ss, rs, i, tp, (tp + 2 * d) % 8) for i, d in enumerate((1, 3, 2))]
        return copies + [gather_copy(buf, ss, rs, 3, tp, twin)]

    def gather_forward(buf, ss, rs):
        slots = [(tp + 2 * d) % 8 for d in (1, 3, 2)]
        return [gather_copy(buf, ss, rs, 4 + i, slot, twin) for i, slot in enumerate(slots)]

    loads[9].wait()
    loads[10].wait()
    value_sends = gather_first(wv, gv_ss, gv_rs)
    out_sends = gather_first(wo, go_ss, go_rs)
    for copy in value_sends + out_sends:
        copy.start()
    value_forwards = gather_forward(wv, gv_ss, gv_rs)
    out_forwards = gather_forward(wo, go_ss, go_rs)

    for i in range(3, 7):
        loads[i].wait()
    lat_all[:, 0:512] = dot(scaled, wd[...])
    lat_all[:, 512:576] = dot_nt(scaled, wr[...])
    lat_all[:, 576:640] = jnp.zeros((64, 64), F32)
    mine = lat_all[pl.ds(pl.multiple_of(tp * 8, 8), 8), :]
    for r in range(8):
        lat_send[r] = mine[r : r + 1, :]
    lat_recv[kv] = lat_send[kv // 2]

    def lat_copy(d):
        to = (kv + d) % 16
        return pltpu.make_async_remote_copy(
            src_ref=lat_send.at[to // 2], dst_ref=lat_recv.at[kv], send_sem=lat_ss.at[d], recv_sem=lat_rs.at[kv],
            device_id=(to, tp), device_id_type=MESH,
        )

    def lat_start(d, c):
        lat_copy(d).start()
        return c


    len_col = to_column(lens[...].astype(F32), 64)
    len_tab[...] = jnp.broadcast_to(len_col, (64, 128))
    lane = iota((32, 128), 1)
    packed_len = jnp.where(lane < 64, len_col[:32], len_col[32:])
    angle = packed_len * freq[...]
    cosine = jnp.cos(angle)
    sine = jnp.sin(angle)
    sine = jnp.where(lane % 64 < 32, -sine, sine)
    cos_tab[0:32, :] = cosine[:, :64]
    cos_tab[32:64, :] = cosine[:, 64:]
    sin_tab[0:32, :] = sine[:, :64]
    sin_tab[32:64, :] = sine[:, 64:]

    def added(own, recv, rows):
        total = own
        for d in range(3):
            total = total + recv[d, rows, :].astype(F32)
        return total

    for copy in a1:
        copy.wait_recv()
    q_nope_sum = added(q_nope_part, a1_recv, slice(0, 64))
    q_rope_sum = added(q_rope_part, a1_recv, slice(64, 96))
    a2_send[0:64, :] = q_nope_sum.astype(BF16)
    a2_send[64:96, :] = q_rope_sum.astype(BF16)
    a2 = line(a2_send, a2_recv, a2_ss, a2_rs, z_dev)
    for copy in a2:
        copy.start()
    for copy in a2:
        copy.wait_recv()
    q_nope = added(q_nope_sum, a2_recv, slice(0, 64)).astype(BF16)
    q_rope = added(q_rope_sum, a2_recv, slice(64, 96)).astype(BF16).astype(F32)
    swapped = jnp.where(lane % 64 < 32, pltpu.roll(q_rope, 96, 1), pltpu.roll(q_rope, 32, 1))
    q_rope = q_rope * cosine + swapped * sine
    q_rope = jnp.concatenate([q_rope[:, :64], q_rope[:, 64:]], axis=0)

    lax.fori_loop(1, 16, lat_start, 0)

    loads[7].wait()
    q_lat = dot_nt(q_nope, wk[...])
    pad = jnp.zeros((8, 64), F32)
    for j in range(8):
        block = jnp.concatenate([q_lat[8 * j : 8 * j + 8], q_rope[8 * j : 8 * j + 8], pad], axis=1)
        b_send[j] = block.astype(BF16)

    def tp_copy(d, src, dst, ss, rs):
        to = (tp + d) % 8
        return pltpu.make_async_remote_copy(
            src_ref=src.at[to], dst_ref=dst.at[tp], send_sem=ss.at[d], recv_sem=rs.at[tp],
            device_id=(kv, to), device_id_type=MESH,
        )

    def tp_wait_copy(d, src, dst, ss, rs):
        frm = (tp + d) % 8
        return pltpu.make_async_remote_copy(
            src_ref=src.at[frm], dst_ref=dst.at[frm], send_sem=ss.at[d], recv_sem=rs.at[frm],
            device_id=(kv, frm), device_id_type=MESH,
        )

    def tp_exchange(src, dst, ss, rs):
        for d in range(1, 8):
            tp_copy(d, src, dst, ss, rs).start()
        dst[tp] = src[tp]
        for d in range(1, 8):
            tp_wait_copy(d, src, dst, ss, rs).wait_recv()

    tp_exchange(b_send, b_recv, b_ss, b_rs)

    for copy in value_forwards + out_forwards:
        copy.wait_recv()
        copy.start()

    r64 = iota((64, 64), 0)
    c64 = iota((64, 64), 1)
    swap = (c64 == (r64 % 8) * 8 + r64 // 8).astype(BF16)
    queries = jnp.concatenate([b_recv[h].astype(F32) for h in range(8)], axis=0).astype(BF16)
    queries = dot(swap, queries)
    for s in range(8):
        q_tab[s] = queries[8 * s : 8 * s + 8]

    def lat_wait(d, c):
        frm = (kv + d) % 16
        pltpu.make_async_remote_copy(
            src_ref=lat_send.at[kv // 2], dst_ref=lat_recv.at[frm], send_sem=lat_ss.at[d], recv_sem=lat_rs.at[frm],
            device_id=(frm, tp), device_id_type=MESH,
        ).wait_recv()
        return c

    lax.fori_loop(1, 16, lat_wait, 0)
    lat_sum = lat_recv[0]
    for k in range(1, 16):
        lat_sum = lat_sum + lat_recv[k]
    loads[8].wait()
    lat_raw = lat_sum[:, :512]
    latent = (
        lat_raw * lax.rsqrt(jnp.mean(lat_raw * lat_raw, axis=1, keepdims=True) + EPSILON) * lgain[...]
    ).astype(BF16).astype(F32)
    key_raw = lat_sum[:, 512:576]
    new_seq = kv // 2
    new_row = tp * 8 + new_seq
    key_swapped = jnp.concatenate([key_raw[:, 32:], key_raw[:, :32]], axis=1)
    new_rope = key_raw * cos_tab[pl.ds(new_row, 1), :] + key_swapped * sin_tab[pl.ds(new_row, 1), :]
    new_rope = new_rope.astype(BF16).astype(F32)
    factor = 192.0 ** (-0.5)
    q_new = q_tab[new_seq]
    new_score = (
        jnp.sum(q_new[:, :512] * latent, axis=1, keepdims=True)
        + jnp.sum(q_new[:, 512:576] * new_rope, axis=1, keepdims=True)
    ) * factor

    positions = (kv * 512 + iota((8, 512), 1)).astype(F32)
    lane8 = iota((8, 128), 1)
    for s in range(8):
        cache_loads[2 * s].wait()
        cache_loads[2 * s + 1].wait()
        q = q_tab[s].astype(BF16)
        scores = (dot_nt(q[:, :512], cl[s]) + dot(q[:, 512:576], cr[s])) * factor
        length = len_tab[pl.ds(tp * 8 + s, 1), 0:1]
        visible = positions < length
        is_new = jnp.logical_and(new_seq == s, kv % 2 == 0)
        own_new = jnp.where(is_new, new_score, NEGATIVE)
        top = jnp.maximum(jnp.max(jnp.where(visible, scores, NEGATIVE), axis=1, keepdims=True), own_new)
        weights = jnp.where(visible, jnp.exp(scores - top), 0.0)
        new_weight = jnp.where(is_new, jnp.exp(own_new - top), 0.0)
        total = jnp.sum(weights, axis=1, keepdims=True) + new_weight
        acc = dot(weights.astype(BF16), cl[s]) + new_weight.astype(BF16).astype(F32) * latent
        some = total > 0.0
        safe = jnp.where(some, total, 1.0)
        lse = jnp.where(some, top + jnp.log(safe), NEGATIVE)
        hi = lse.astype(BF16).astype(F32)
        mid = (lse - hi).astype(BF16).astype(F32)
        low = lse - hi - mid
        o_tab[8 * s : 8 * s + 8, 0:512] = acc / safe
        o_tab[8 * s : 8 * s + 8, 512:640] = jnp.where(
            lane8 == 0, hi, jnp.where(lane8 == 1, mid, jnp.where(lane8 == 2, low, 0.0))
        )

    parts = dot(swap, o_tab[...].astype(BF16))
    lse = jnp.sum(parts[:, 512:640], axis=1, keepdims=True)

    def gather_wait(buf, ss, rs):
        for d in range(4):
            slot = (twin + 2 * d) % 8
            gather_copy(buf, ss, rs, 0, slot, twin).wait_recv()

    gather_wait(wv, gv_ss, gv_rs)
    value = jnp.concatenate(
        [dot(parts[8 * h : 8 * h + 8, :512].astype(BF16), wv[h]) for h in range(8)], axis=0
    )

    def combine(value, lse, send, recv, lse_send, lse_recv, sems, dev):
        send[...] = value.astype(BF16)
        lse_send[...] = to_row(lse, 64)
        copies = line(send, recv, sems[0], sems[1], dev)
        lse_copies = line(lse_send, lse_recv, sems[2], sems[3], dev)
        for copy in lse_copies + copies:
            copy.start()
        for copy in lse_copies:
            copy.wait_recv()
        others = [to_column(lse_recv[d], 64) for d in range(3)]
        top = lse
        for other in others:
            top = jnp.maximum(top, other)
        own_scale = jnp.exp(lse - top)
        scales = [jnp.exp(other - top) for other in others]
        total = own_scale + scales[0] + scales[1] + scales[2]
        for copy in copies:
            copy.wait_recv()
        merged = value * (own_scale / total)
        for d in range(3):
            merged = merged + recv[d].astype(F32) * (scales[d] / total)
        return merged, top + jnp.log(total), copies + lse_copies

    value, lse, c1 = combine(
        value, lse, c1_send, c1_recv, c1_lse, c1_lser, (c1_ss, c1_rs, cl1_ss, cl1_rs), x_dev
    )
    value, lse, c2 = combine(
        value, lse, c2_send, c2_recv, c2_lse, c2_lser, (c2_ss, c2_rs, cl2_ss, cl2_rs), z_dev
    )
    gather_wait(wo, go_ss, go_rs)
    head_out = jnp.concatenate([value[8 * h : 8 * h + 8] for h in range(8)], axis=1).astype(BF16)
    m_send[...] = dot(head_out, wo[...].reshape(1024, 128))

    def m_copy(d, slot, to):
        return pltpu.make_async_remote_copy(
            src_ref=m_send, dst_ref=m_recv.at[slot], send_sem=m_ss.at[d], recv_sem=m_rs.at[slot],
            device_id=(kv, to), device_id_type=MESH,
        )

    for d in range(1, 8):
        m_copy(d, tp, (tp + d) % 8).start()
    m_recv[tp] = m_send[...]
    for d in range(1, 8):
        frm = (tp + d) % 8
        m_copy(d, frm, frm).wait_recv()
    mixed = m_recv[...].reshape(64, 128)

    g_send[...] = to_row(jnp.sum(mixed * mixed, axis=1, keepdims=True), 64)

    def g_copy(d, slot, to):
        return pltpu.make_async_remote_copy(
            src_ref=g_send, dst_ref=g_recv.at[slot], send_sem=g_ss.at[d], recv_sem=g_rs.at[slot],
            device_id=(to, tp), device_id_type=MESH,
        )

    def g_start(d, c):
        g_copy(d, kv, (kv + d) % 16).start()
        return c

    def g_wait(d, c):
        frm = (kv + d) % 16
        g_copy(d, frm, frm).wait_recv()
        return c

    lax.fori_loop(1, 16, g_start, 0)
    g_recv[kv] = g_send[...]
    loads[11].wait()
    lax.fori_loop(1, 16, g_wait, 0)
    squares = g_recv[0]
    for k in range(1, 16):
        squares = squares + g_recv[k]
    inverse = to_column(lax.rsqrt(squares / 2048.0 + EPSILON), 64)
    out_ref[...] = (mixed * inverse * ogain[...]).astype(BF16)

    for copy in a1 + a2 + c1 + c2 + value_sends + out_sends + value_forwards + out_forwards:
        copy.wait_send()

    def drain_kv(d, c):
        lat_copy(d).wait_send()
        g_copy(d, kv, (kv + d) % 16).wait_send()
        return c

    def drain_tp(d, c):
        tp_copy(d, b_send, b_recv, b_ss, b_rs).wait_send()
        m_copy(d, tp, (tp + d) % 8).wait_send()
        return c

    lax.fori_loop(1, 16, drain_kv, 0)
    lax.fori_loop(1, 8, drain_tp, 0)


def on_device(
    tokens, token_gain, w_query, w_down_kv, w_rope_key, latent_gain, w_key_up, w_value_up, w_out, out_gain,
    cache_latent, cache_rope, lengths,
):
    freq = 1.0 / 10000.0 ** (np.arange(0, 64, 2, dtype=np.float32) / np.float32(64.0))
    freq = jnp.asarray(np.tile(freq.astype(np.float32), 4)[None, :])
    operands = (
        tokens, token_gain.reshape(1, 128), w_query.T, w_down_kv, w_rope_key.T, latent_gain.reshape(1, 512),
        w_key_up.reshape(512, 128), w_value_up.reshape(512, 128), w_out, out_gain.reshape(1, 128),
        cache_latent, cache_rope.transpose(0, 2, 1), lengths.reshape(1, 64), freq,
    )
    shapes = [(a.shape, a.dtype) for a in operands]
    shapes[7] = ((8, 512, 128), BF16)
    shapes[8] = ((8, 128, 128), BF16)
    local = [pltpu.VMEM(*a) for a in shapes]
    dma = pltpu.SemaphoreType.DMA
    scratch = local + [
        pltpu.VMEM((64, 128), F32), pltpu.VMEM((64, 64), F32), pltpu.VMEM((64, 64), F32),
        pltpu.VMEM((96, 128), BF16), pltpu.VMEM((3, 96, 128), BF16),
        pltpu.VMEM((96, 128), BF16), pltpu.VMEM((3, 96, 128), BF16),
        pltpu.VMEM((64, 640), F32), pltpu.VMEM((8, 1, 640), F32), pltpu.VMEM((16, 1, 640), F32),
        pltpu.VMEM((8, 8, 640), BF16), pltpu.VMEM((8, 8, 640), BF16),
        pltpu.VMEM((8, 8, 640), F32), pltpu.VMEM((64, 640), F32),
        pltpu.VMEM((64, 128), BF16), pltpu.VMEM((3, 64, 128), BF16),
        pltpu.VMEM((1, 128), F32), pltpu.VMEM((3, 1, 128), F32),
        pltpu.VMEM((64, 128), BF16), pltpu.VMEM((3, 64, 128), BF16),
        pltpu.VMEM((1, 128), F32), pltpu.VMEM((3, 1, 128), F32),
        pltpu.VMEM((8, 128), F32), pltpu.VMEM((8, 8, 128), F32),
        pltpu.VMEM((1, 128), F32), pltpu.VMEM((16, 1, 128), F32),
        dma((12,)), dma((16,)),
        dma((3,)), dma((3,)), dma((3,)), dma((3,)), dma((16,)), dma((16,)),
        dma((8,)), dma((8,)), dma((8,)), dma((8,)), dma((8,)), dma((8,)),
        dma((3,)), dma((3,)), dma((3,)), dma((3,)), dma((3,)), dma((3,)), dma((3,)), dma((3,)),
        dma((8,)), dma((8,)), dma((16,)), dma((16,)),
    ]
    return pl.pallas_call(
        kernel,
        out_shape=jax.ShapeDtypeStruct((64, 128), BF16),
        in_specs=[pl.BlockSpec(memory_space=pltpu.HBM)] * len(operands),
        out_specs=pl.BlockSpec(memory_space=pltpu.VMEM),
        scratch_shapes=scratch,
        compiler_params=pltpu.CompilerParams(
            collective_id=0, has_side_effects=True, vmem_limit_bytes=67043328
        ),
    )(*operands)


def solution(mesh):
    return jax.shard_map(
        on_device,
        mesh=mesh,
        in_specs=(
            P(None, "kv"), P("kv"), P("kv", "tp"), P("kv", None), P("kv", None), P(),
            P("tp", None, None), P("tp", None, None), P("tp", "kv"), P("kv"),
            P("tp", "kv", None), P("tp", "kv", None), P(),
        ),
        out_specs=P(None, "kv"),
        check_vma=False,
    )
```

```python
import functools

import jax
import jax.numpy as jnp
import numpy as np
from jax import lax
from jax.experimental import pallas as pl
from jax.experimental.pallas import tpu as pltpu
from jax.sharding import PartitionSpec as P

MESH = pl.DeviceIdType.MESH
EPSILON = 1e-06
NEGATIVE = -1e30
BF16 = jnp.bfloat16
F32 = jnp.float32


def dot(a, b):
    return jnp.dot(a, b, preferred_element_type=F32)


def dot_nt(a, b):
    return lax.dot_general(a, b, (((1,), (1,)), ((), ())), preferred_element_type=F32)


def iota(shape, axis):
    return lax.broadcasted_iota(jnp.int32, shape, axis)


def to_column(row, rows):
    picked = iota((rows, rows), 0) == iota((rows, rows), 1)
    return jnp.sum(jnp.where(picked, row[:, :rows], 0.0), axis=1, keepdims=True)


def to_row(column, rows):
    picked = iota((rows, 128), 0) == iota((rows, 128), 1)
    return jnp.sum(jnp.where(picked, column, 0.0), axis=0, keepdims=True)


def kernel(
    tok_h, tgain_h, wq_h, wd_h, wr_h, lgain_h, wk_h, wv_h, wo_h, ogain_h, cl_h, cr_h, len_h, freq_h,
    out_ref,
    tok, tgain, wq, wd, wr, lgain, wk, wv, wo, ogain, cl, cr, lens, freq,
    len_tab, cos_tab, sin_tab,
    a1_send, a1_recv, a2_send, a2_recv,
    lat_all, lat_send, lat_recv,
    b_send, b_recv, q_tab, o_tab,
    c1_send, c1_recv, c1_lse, c1_lser, c2_send, c2_recv, c2_lse, c2_lser,
    m_send, m_recv, g_send, g_recv,
    load_sem, cache_sem,
    a1_ss, a1_rs, a2_ss, a2_rs, lat_ss, lat_rs, b_ss, b_rs, gv_ss, gv_rs, go_ss, go_rs,
    c1_ss, c1_rs, c2_ss, c2_rs, cl1_ss, cl1_rs, cl2_ss, cl2_rs, m_ss, m_rs, g_ss, g_rs,
):
    kv = lax.axis_index("kv")
    tp = lax.axis_index("tp")
    z = kv // 4
    x = kv % 4

    barrier = pltpu.get_barrier_semaphore()

    def greet_line(d, c):
        pl.semaphore_signal(barrier, inc=1, device_id=(z * 4 + (x + d) % 4, tp), device_id_type=MESH)
        pl.semaphore_signal(barrier, inc=1, device_id=((z + d) % 4 * 4 + x, tp), device_id_type=MESH)
        return c

    def greet_tp(d, c):
        pl.semaphore_signal(barrier, inc=1, device_id=(kv, (tp + d) % 8), device_id_type=MESH)
        return c

    lax.fori_loop(1, 4, greet_line, 0)
    lax.fori_loop(1, 8, greet_tp, 0)

    pairs = [
        (tok_h, tok), (tgain_h, tgain), (wq_h, wq), (len_h, lens), (freq_h, freq), (wd_h, wd), (wr_h, wr),
        (wk_h, wk), (lgain_h, lgain), (wv_h, wv.at[tp]), (wo_h, wo.at[tp]), (ogain_h, ogain),
    ]
    loads = [pltpu.make_async_copy(s, d, load_sem.at[i]) for i, (s, d) in enumerate(pairs)]
    for copy in loads:
        copy.start()
    cache_loads = []
    for s in range(8):
        cache_loads.append(pltpu.make_async_copy(cl_h.at[s], cl.at[s], cache_sem.at[s]))
        cache_loads.append(pltpu.make_async_copy(cr_h.at[s], cr.at[s], cache_sem.at[8 + s]))
    for copy in cache_loads:
        copy.start()

    for i in range(3):
        loads[i].wait()
    scaled = (tok[...].astype(F32) * tgain[...]).astype(BF16)
    q_part = dot_nt(scaled, wq[...])
    rope_part = q_part[:, 128:192]
    q_nope_part = q_part[:, :128]
    q_rope_part = jnp.concatenate([rope_part[:32], rope_part[32:]], axis=1)
    a1_send[0:64, :] = q_nope_part.astype(BF16)
    a1_send[64:96, :] = q_rope_part.astype(BF16)

    pl.semaphore_wait(barrier, 13)

    def x_dev(d):
        return (z * 4 + (x + d) % 4, tp)

    def z_dev(d):
        return (((z + d) % 4) * 4 + x, tp)

    def line(src, dst, ss, rs, dev):
        return [
            pltpu.make_async_remote_copy(
                src_ref=src, dst_ref=dst.at[d - 1], send_sem=ss.at[d - 1], recv_sem=rs.at[d - 1],
                device_id=dev(d), device_id_type=MESH,
            )
            for d in (1, 2, 3)
        ]

    a1 = line(a1_send, a1_recv, a1_ss, a1_rs, x_dev)
    for copy in a1:
        copy.start()

    twin = tp + 1 - 2 * (tp % 2)

    def gather_copy(buf, ss, rs, i, slot, to):
        return pltpu.make_async_remote_copy(
            src_ref=buf.at[slot], dst_ref=buf.at[slot], send_sem=ss.at[i], recv_sem=rs.at[slot],
            device_id=(kv, to), device_id_type=MESH,
        )

    def gather_first(buf, ss, rs):
        copies = [gather_copy(buf, ss, rs, i, tp, (tp + 2 * d) % 8) for i, d in enumerate((1, 3, 2))]
        return copies + [gather_copy(buf, ss, rs, 3, tp, twin)]

    def gather_forward(buf, ss, rs):
        slots = [(tp + 2 * d) % 8 for d in (1, 3, 2)]
        return [gather_copy(buf, ss, rs, 4 + i, slot, twin) for i, slot in enumerate(slots)]

    loads[9].wait()
    loads[10].wait()
    value_sends = gather_first(wv, gv_ss, gv_rs)
    out_sends = gather_first(wo, go_ss, go_rs)
    for copy in value_sends + out_sends:
        copy.start()
    value_forwards = gather_forward(wv, gv_ss, gv_rs)
    out_forwards = gather_forward(wo, go_ss, go_rs)

    for i in range(3, 7):
        loads[i].wait()
    lat_all[:, 0:512] = dot(scaled, wd[...])
    lat_all[:, 512:576] = dot_nt(scaled, wr[...])
    lat_all[:, 576:640] = jnp.zeros((64, 64), F32)
    mine = lat_all[pl.ds(pl.multiple_of(tp * 8, 8), 8), :]
    for r in range(8):
        lat_send[r] = mine[r : r + 1, :]
    lat_recv[kv] = lat_send[kv // 2]

    def lat_copy(d):
        to = (kv + d) % 16
        return pltpu.make_async_remote_copy(
            src_ref=lat_send.at[to // 2], dst_ref=lat_recv.at[kv], send_sem=lat_ss.at[d], recv_sem=lat_rs.at[kv],
            device_id=(to, tp), device_id_type=MESH,
        )

    def lat_start(d, c):
        lat_copy(d).start()
        return c


    len_col = to_column(lens[...].astype(F32), 64)
    len_tab[...] = jnp.broadcast_to(len_col, (64, 128))
    lane = iota((32, 128), 1)
    packed_len = jnp.where(lane < 64, len_col[:32], len_col[32:])
    angle = packed_len * freq[...]
    cosine = jnp.cos(angle)
    sine = jnp.sin(angle)
    sine = jnp.where(lane % 64 < 32, -sine, sine)
    cos_tab[0:32, :] = cosine[:, :64]
    cos_tab[32:64, :] = cosine[:, 64:]
    sin_tab[0:32, :] = sine[:, :64]
    sin_tab[32:64, :] = sine[:, 64:]

    def added(own, recv, rows):
        total = own
        for d in range(3):
            total = total + recv[d, rows, :].astype(F32)
        return total

    for copy in a1:
        copy.wait_recv()
    q_nope_sum = added(q_nope_part, a1_recv, slice(0, 64))
    q_rope_sum = added(q_rope_part, a1_recv, slice(64, 96))
    a2_send[0:64, :] = q_nope_sum.astype(BF16)
    a2_send[64:96, :] = q_rope_sum.astype(BF16)
    a2 = line(a2_send, a2_recv, a2_ss, a2_rs, z_dev)
    for copy in a2:
        copy.start()
    for copy in a2:
        copy.wait_recv()
    q_nope = added(q_nope_sum, a2_recv, slice(0, 64)).astype(BF16)
    q_rope = added(q_rope_sum, a2_recv, slice(64, 96)).astype(BF16).astype(F32)
    swapped = jnp.where(lane % 64 < 32, pltpu.roll(q_rope, 96, 1), pltpu.roll(q_rope, 32, 1))
    q_rope = q_rope * cosine + swapped * sine
    q_rope = jnp.concatenate([q_rope[:, :64], q_rope[:, 64:]], axis=0)

    lax.fori_loop(1, 16, lat_start, 0)

    loads[7].wait()
    q_lat = dot_nt(q_nope, wk[...])
    pad = jnp.zeros((8, 64), F32)
    for j in range(8):
        block = jnp.concatenate([q_lat[8 * j : 8 * j + 8], q_rope[8 * j : 8 * j + 8], pad], axis=1)
        b_send[j] = block.astype(BF16)

    def tp_copy(d, src, dst, ss, rs):
        to = (tp + d) % 8
        return pltpu.make_async_remote_copy(
            src_ref=src.at[to], dst_ref=dst.at[tp], send_sem=ss.at[d], recv_sem=rs.at[tp],
            device_id=(kv, to), device_id_type=MESH,
        )

    def tp_wait_copy(d, src, dst, ss, rs):
        frm = (tp + d) % 8
        return pltpu.make_async_remote_copy(
            src_ref=src.at[frm], dst_ref=dst.at[frm], send_sem=ss.at[d], recv_sem=rs.at[frm],
            device_id=(kv, frm), device_id_type=MESH,
        )

    def tp_exchange(src, dst, ss, rs):
        for d in range(1, 8):
            tp_copy(d, src, dst, ss, rs).start()
        dst[tp] = src[tp]
        for d in range(1, 8):
            tp_wait_copy(d, src, dst, ss, rs).wait_recv()

    tp_exchange(b_send, b_recv, b_ss, b_rs)

    for copy in value_forwards + out_forwards:
        copy.wait_recv()
        copy.start()

    r64 = iota((64, 64), 0)
    c64 = iota((64, 64), 1)
    swap = (c64 == (r64 % 8) * 8 + r64 // 8).astype(BF16)
    queries = jnp.concatenate([b_recv[h].astype(F32) for h in range(8)], axis=0).astype(BF16)
    queries = dot(swap, queries)
    for s in range(8):
        q_tab[s] = queries[8 * s : 8 * s + 8]

    def lat_wait(d, c):
        frm = (kv + d) % 16
        pltpu.make_async_remote_copy(
            src_ref=lat_send.at[kv // 2], dst_ref=lat_recv.at[frm], send_sem=lat_ss.at[d], recv_sem=lat_rs.at[frm],
            device_id=(frm, tp), device_id_type=MESH,
        ).wait_recv()
        return c

    lax.fori_loop(1, 16, lat_wait, 0)
    lat_sum = lat_recv[0]
    for k in range(1, 16):
        lat_sum = lat_sum + lat_recv[k]
    loads[8].wait()
    lat_raw = lat_sum[:, :512]
    latent = (
        lat_raw * lax.rsqrt(jnp.mean(lat_raw * lat_raw, axis=1, keepdims=True) + EPSILON) * lgain[...]
    ).astype(BF16).astype(F32)
    key_raw = lat_sum[:, 512:576]
    new_seq = kv // 2
    new_row = tp * 8 + new_seq
    key_swapped = jnp.concatenate([key_raw[:, 32:], key_raw[:, :32]], axis=1)
    new_rope = key_raw * cos_tab[pl.ds(new_row, 1), :] + key_swapped * sin_tab[pl.ds(new_row, 1), :]
    new_rope = new_rope.astype(BF16).astype(F32)
    factor = 192.0 ** (-0.5)
    q_new = q_tab[new_seq]
    new_score = (
        jnp.sum(q_new[:, :512] * latent, axis=1, keepdims=True)
        + jnp.sum(q_new[:, 512:576] * new_rope, axis=1, keepdims=True)
    ) * factor

    for copy in cache_loads:
        copy.wait()
    scores = jnp.concatenate(
        [
            dot_nt(q_tab[s].astype(BF16)[:, :512], cl[s]) + dot(q_tab[s].astype(BF16)[:, 512:576], cr[s])
            for s in range(8)
        ],
        axis=0,
    ) * factor
    row_seq = iota((64, 1), 0) // 8
    row_length = jnp.concatenate(
        [jnp.broadcast_to(len_tab[pl.ds(tp * 8 + s, 1), 0:1], (8, 1)) for s in range(8)], axis=0
    )
    positions = (kv * 512 + iota((64, 512), 1)).astype(F32)
    visible = positions < row_length
    is_new = jnp.logical_and(row_seq == new_seq, kv % 2 == 0)
    own_new = jnp.where(is_new, jnp.concatenate([new_score] * 8, axis=0), NEGATIVE)
    top = jnp.maximum(jnp.max(jnp.where(visible, scores, NEGATIVE), axis=1, keepdims=True), own_new)
    weights = jnp.where(visible, jnp.exp(scores - top), 0.0)
    new_weight = jnp.where(is_new, jnp.exp(own_new - top), 0.0)
    total = jnp.sum(weights, axis=1, keepdims=True) + new_weight
    some = total > 0.0
    safe = jnp.where(some, total, 1.0)
    lse = jnp.where(some, top + jnp.log(safe), NEGATIVE)
    hi = lse.astype(BF16).astype(F32)
    mid = (lse - hi).astype(BF16).astype(F32)
    low = lse - hi - mid
    lane64 = iota((64, 128), 1)
    acc = jnp.concatenate(
        [dot(weights[8 * s : 8 * s + 8].astype(BF16), cl[s]) for s in range(8)], axis=0
    ) + new_weight.astype(BF16).astype(F32) * latent
    o_tab[:, 0:512] = acc / safe
    o_tab[:, 512:640] = jnp.where(
        lane64 == 0, hi, jnp.where(lane64 == 1, mid, jnp.where(lane64 == 2, low, 0.0))
    )

    parts = dot(swap, o_tab[...].astype(BF16))
    lse = jnp.sum(parts[:, 512:640], axis=1, keepdims=True)

    def gather_wait(buf, ss, rs):
        for d in range(4):
            slot = (twin + 2 * d) % 8
            gather_copy(buf, ss, rs, 0, slot, twin).wait_recv()

    gather_wait(wv, gv_ss, gv_rs)
    value = jnp.concatenate(
        [dot(parts[8 * h : 8 * h + 8, :512].astype(BF16), wv[h]) for h in range(8)], axis=0
    )

    def combine(value, lse, send, recv, lse_send, lse_recv, sems, dev):
        send[...] = value.astype(BF16)
        lse_send[...] = to_row(lse, 64)
        copies = line(send, recv, sems[0], sems[1], dev)
        lse_copies = line(lse_send, lse_recv, sems[2], sems[3], dev)
        for copy in lse_copies + copies:
            copy.start()
        for copy in lse_copies:
            copy.wait_recv()
        others = [to_column(lse_recv[d], 64) for d in range(3)]
        top = lse
        for other in others:
            top = jnp.maximum(top, other)
        own_scale = jnp.exp(lse - top)
        scales = [jnp.exp(other - top) for other in others]
        total = own_scale + scales[0] + scales[1] + scales[2]
        for copy in copies:
            copy.wait_recv()
        merged = value * (own_scale / total)
        for d in range(3):
            merged = merged + recv[d].astype(F32) * (scales[d] / total)
        return merged, top + jnp.log(total), copies + lse_copies

    value, lse, c1 = combine(
        value, lse, c1_send, c1_recv, c1_lse, c1_lser, (c1_ss, c1_rs, cl1_ss, cl1_rs), x_dev
    )
    value, lse, c2 = combine(
        value, lse, c2_send, c2_recv, c2_lse, c2_lser, (c2_ss, c2_rs, cl2_ss, cl2_rs), z_dev
    )
    gather_wait(wo, go_ss, go_rs)
    head_out = jnp.concatenate([value[8 * h : 8 * h + 8] for h in range(8)], axis=1).astype(BF16)
    m_send[...] = dot(head_out, wo[...].reshape(1024, 128))

    def m_copy(d, slot, to):
        return pltpu.make_async_remote_copy(
            src_ref=m_send, dst_ref=m_recv.at[slot], send_sem=m_ss.at[d], recv_sem=m_rs.at[slot],
            device_id=(kv, to), device_id_type=MESH,
        )

    for d in range(1, 8):
        m_copy(d, tp, (tp + d) % 8).start()
    m_recv[tp] = m_send[...]
    for d in range(1, 8):
        frm = (tp + d) % 8
        m_copy(d, frm, frm).wait_recv()
    mixed = m_recv[...].reshape(64, 128)

    g_send[...] = to_row(jnp.sum(mixed * mixed, axis=1, keepdims=True), 64)

    def g_copy(d, slot, to):
        return pltpu.make_async_remote_copy(
            src_ref=g_send, dst_ref=g_recv.at[slot], send_sem=g_ss.at[d], recv_sem=g_rs.at[slot],
            device_id=(to, tp), device_id_type=MESH,
        )

    def g_start(d, c):
        g_copy(d, kv, (kv + d) % 16).start()
        return c

    def g_wait(d, c):
        frm = (kv + d) % 16
        g_copy(d, frm, frm).wait_recv()
        return c

    lax.fori_loop(1, 16, g_start, 0)
    g_recv[kv] = g_send[...]
    loads[11].wait()
    lax.fori_loop(1, 16, g_wait, 0)
    squares = g_recv[0]
    for k in range(1, 16):
        squares = squares + g_recv[k]
    inverse = to_column(lax.rsqrt(squares / 2048.0 + EPSILON), 64)
    out_ref[...] = (mixed * inverse * ogain[...]).astype(BF16)

    for copy in a1 + a2 + c1 + c2 + value_sends + out_sends + value_forwards + out_forwards:
        copy.wait_send()

    def drain_kv(d, c):
        lat_copy(d).wait_send()
        g_copy(d, kv, (kv + d) % 16).wait_send()
        return c

    def drain_tp(d, c):
        tp_copy(d, b_send, b_recv, b_ss, b_rs).wait_send()
        m_copy(d, tp, (tp + d) % 8).wait_send()
        return c

    lax.fori_loop(1, 16, drain_kv, 0)
    lax.fori_loop(1, 8, drain_tp, 0)


def on_device(
    tokens, token_gain, w_query, w_down_kv, w_rope_key, latent_gain, w_key_up, w_value_up, w_out, out_gain,
    cache_latent, cache_rope, lengths,
):
    freq = 1.0 / 10000.0 ** (np.arange(0, 64, 2, dtype=np.float32) / np.float32(64.0))
    freq = jnp.asarray(np.tile(freq.astype(np.float32), 4)[None, :])
    operands = (
        tokens, token_gain.reshape(1, 128), w_query.T, w_down_kv, w_rope_key.T, latent_gain.reshape(1, 512),
        w_key_up.reshape(512, 128), w_value_up.reshape(512, 128), w_out, out_gain.reshape(1, 128),
        cache_latent, cache_rope.transpose(0, 2, 1), lengths.reshape(1, 64), freq,
    )
    shapes = [(a.shape, a.dtype) for a in operands]
    shapes[7] = ((8, 512, 128), BF16)
    shapes[8] = ((8, 128, 128), BF16)
    local = [pltpu.VMEM(*a) for a in shapes]
    dma = pltpu.SemaphoreType.DMA
    scratch = local + [
        pltpu.VMEM((64, 128), F32), pltpu.VMEM((64, 64), F32), pltpu.VMEM((64, 64), F32),
        pltpu.VMEM((96, 128), BF16), pltpu.VMEM((3, 96, 128), BF16),
        pltpu.VMEM((96, 128), BF16), pltpu.VMEM((3, 96, 128), BF16),
        pltpu.VMEM((64, 640), F32), pltpu.VMEM((8, 1, 640), F32), pltpu.VMEM((16, 1, 640), F32),
        pltpu.VMEM((8, 8, 640), BF16), pltpu.VMEM((8, 8, 640), BF16),
        pltpu.VMEM((8, 8, 640), F32), pltpu.VMEM((64, 640), F32),
        pltpu.VMEM((64, 128), BF16), pltpu.VMEM((3, 64, 128), BF16),
        pltpu.VMEM((1, 128), F32), pltpu.VMEM((3, 1, 128), F32),
        pltpu.VMEM((64, 128), BF16), pltpu.VMEM((3, 64, 128), BF16),
        pltpu.VMEM((1, 128), F32), pltpu.VMEM((3, 1, 128), F32),
        pltpu.VMEM((8, 128), F32), pltpu.VMEM((8, 8, 128), F32),
        pltpu.VMEM((1, 128), F32), pltpu.VMEM((16, 1, 128), F32),
        dma((12,)), dma((16,)),
        dma((3,)), dma((3,)), dma((3,)), dma((3,)), dma((16,)), dma((16,)),
        dma((8,)), dma((8,)), dma((8,)), dma((8,)), dma((8,)), dma((8,)),
        dma((3,)), dma((3,)), dma((3,)), dma((3,)), dma((3,)), dma((3,)), dma((3,)), dma((3,)),
        dma((8,)), dma((8,)), dma((16,)), dma((16,)),
    ]
    return pl.pallas_call(
        kernel,
        out_shape=jax.ShapeDtypeStruct((64, 128), BF16),
        in_specs=[pl.BlockSpec(memory_space=pltpu.HBM)] * len(operands),
        out_specs=pl.BlockSpec(memory_space=pltpu.VMEM),
        scratch_shapes=scratch,
        compiler_params=pltpu.CompilerParams(
            collective_id=0, has_side_effects=True, vmem_limit_bytes=67043328
        ),
    )(*operands)


def solution(mesh):
    return jax.shard_map(
        on_device,
        mesh=mesh,
        in_specs=(
            P(None, "kv"), P("kv"), P("kv", "tp"), P("kv", None), P("kv", None), P(),
            P("tp", None, None), P("tp", None, None), P("tp", "kv"), P("kv"),
            P("tp", "kv", None), P("tp", "kv", None), P(),
        ),
        out_specs=P(None, "kv"),
        check_vma=False,
    )
```

```python
import functools

import jax
import jax.numpy as jnp
import numpy as np
from jax import lax
from jax.experimental import pallas as pl
from jax.experimental.pallas import tpu as pltpu
from jax.sharding import PartitionSpec as P

MESH = pl.DeviceIdType.MESH
EPSILON = 1e-06
NEGATIVE = -1e30
BF16 = jnp.bfloat16
F32 = jnp.float32


def dot(a, b):
    return jnp.dot(a, b, preferred_element_type=F32)


def dot_nt(a, b):
    return lax.dot_general(a, b, (((1,), (1,)), ((), ())), preferred_element_type=F32)


def iota(shape, axis):
    return lax.broadcasted_iota(jnp.int32, shape, axis)


def to_column(row, rows):
    picked = iota((rows, rows), 0) == iota((rows, rows), 1)
    return jnp.sum(jnp.where(picked, row[:, :rows], 0.0), axis=1, keepdims=True)


def to_row(column, rows):
    picked = iota((rows, 128), 0) == iota((rows, 128), 1)
    return jnp.sum(jnp.where(picked, column, 0.0), axis=0, keepdims=True)


def kernel(
    tok_h, tgain_h, wq_h, wd_h, wr_h, lgain_h, wk_h, wv_h, wo_h, ogain_h, cl_h, cr_h, len_h, freq_h,
    out_ref,
    tok, tgain, wq, wd, wr, lgain, wk, wv, wo, ogain, cl, cr, lens, freq,
    len_tab, cos_tab, sin_tab,
    a1_send, a1_recv, a2_send, a2_recv,
    lat_all, lat_send, lat_recv,
    b_send, b_recv, q_tab, o_tab,
    c1_send, c1_recv, c1_lse, c1_lser, c2_send, c2_recv, c2_lse, c2_lser,
    m_send, m_recv, g_send, g_recv,
    load_sem, cache_sem,
    a1_ss, a1_rs, a2_ss, a2_rs, lat_ss, lat_rs, b_ss, b_rs, gv_ss, gv_rs, oy_ss, oy_rs, oz_ss, oz_rs, ot_ss, ot_rs,
    c1_ss, c1_rs, c2_ss, c2_rs, cl1_ss, cl1_rs, cl2_ss, cl2_rs, m_ss, m_rs, g_ss, g_rs,
):
    kv = lax.axis_index("kv")
    tp = lax.axis_index("tp")
    z = kv // 4
    x = kv % 4
    y = tp // 2
    core = tp % 2

    barrier = pltpu.get_barrier_semaphore()

    def greet_line(d, c):
        pl.semaphore_signal(barrier, inc=1, device_id=(z * 4 + (x + d) % 4, tp), device_id_type=MESH)
        pl.semaphore_signal(barrier, inc=1, device_id=((z + d) % 4 * 4 + x, tp), device_id_type=MESH)
        return c

    def greet_tp(d, c):
        pl.semaphore_signal(barrier, inc=1, device_id=(kv, (tp + d) % 8), device_id_type=MESH)
        return c

    lax.fori_loop(1, 4, greet_line, 0)
    lax.fori_loop(1, 8, greet_tp, 0)

    pairs = [
        (tok_h, tok), (tgain_h, tgain), (wq_h, wq), (len_h, lens), (freq_h, freq), (wd_h, wd), (wr_h, wr),
        (wk_h, wk), (lgain_h, lgain), (wv_h, wv.at[tp]), (wo_h, wo.at[z, core, y]), (ogain_h, ogain),
    ]
    loads = [pltpu.make_async_copy(s, d, load_sem.at[i]) for i, (s, d) in enumerate(pairs)]
    for copy in loads:
        copy.start()
    cache_loads = []
    for s in range(8):
        cache_loads.append(pltpu.make_async_copy(cl_h.at[s], cl.at[s], cache_sem.at[s]))
        cache_loads.append(pltpu.make_async_copy(cr_h.at[s], cr.at[s], cache_sem.at[8 + s]))
    for copy in cache_loads:
        copy.start()

    for i in range(3):
        loads[i].wait()
    scaled = (tok[...].astype(F32) * tgain[...]).astype(BF16)
    q_part = dot_nt(scaled, wq[...])
    rope_part = q_part[:, 128:192]
    q_nope_part = q_part[:, :128]
    q_rope_part = jnp.concatenate([rope_part[:32], rope_part[32:]], axis=1)
    a1_send[0:64, :] = q_nope_part.astype(BF16)
    a1_send[64:96, :] = q_rope_part.astype(BF16)

    pl.semaphore_wait(barrier, 13)

    def x_dev(d):
        return (z * 4 + (x + d) % 4, tp)

    def z_dev(d):
        return (((z + d) % 4) * 4 + x, tp)

    def line(src, dst, ss, rs, dev):
        return [
            pltpu.make_async_remote_copy(
                src_ref=src, dst_ref=dst.at[d - 1], send_sem=ss.at[d - 1], recv_sem=rs.at[d - 1],
                device_id=dev(d), device_id_type=MESH,
            )
            for d in (1, 2, 3)
        ]

    a1 = line(a1_send, a1_recv, a1_ss, a1_rs, x_dev)
    for copy in a1:
        copy.start()

    twin = tp + 1 - 2 * core

    def gather_copy(buf, ss, rs, i, slot, to):
        return pltpu.make_async_remote_copy(
            src_ref=buf.at[slot], dst_ref=buf.at[slot], send_sem=ss.at[i], recv_sem=rs.at[slot],
            device_id=(kv, to), device_id_type=MESH,
        )

    def gather_first(buf, ss, rs):
        copies = [gather_copy(buf, ss, rs, i, tp, (tp + 2 * d) % 8) for i, d in enumerate((1, 3, 2))]
        return copies + [gather_copy(buf, ss, rs, 3, tp, twin)]

    def gather_forward(buf, ss, rs):
        slots = [(tp + 2 * d) % 8 for d in (1, 3, 2)]
        return [gather_copy(buf, ss, rs, 4 + i, slot, twin) for i, slot in enumerate(slots)]

    loads[9].wait()
    loads[10].wait()
    value_sends = gather_first(wv, gv_ss, gv_rs)
    value_forwards = gather_forward(wv, gv_ss, gv_rs)

    def out_y(d, at):
        return pltpu.make_async_remote_copy(
            src_ref=wo.at[z, core, y], dst_ref=wo.at[z, core, at], send_sem=oy_ss.at[d], recv_sem=oy_rs.at[at],
            device_id=(kv, (tp + 2 * d) % 8), device_id_type=MESH,
        )

    def out_z(d, at):
        return pltpu.make_async_remote_copy(
            src_ref=wo.at[z, core], dst_ref=wo.at[at, core], send_sem=oz_ss.at[d], recv_sem=oz_rs.at[at],
            device_id=((z + d) % 4 * 4 + x, tp), device_id_type=MESH,
        )

    def out_twin(d, half):
        at = (z + d) % 4
        return pltpu.make_async_remote_copy(
            src_ref=wo.at[at, core], dst_ref=wo.at[at, half], send_sem=ot_ss.at[d], recv_sem=ot_rs.at[at],
            device_id=(kv, twin), device_id_type=MESH,
        )

    for d in (1, 3, 2):
        out_y(d, y).start()
    for copy in value_sends:
        copy.start()

    for i in range(3, 7):
        loads[i].wait()
    lat_all[:, 0:512] = dot(scaled, wd[...])
    lat_all[:, 512:576] = dot_nt(scaled, wr[...])
    lat_all[:, 576:640] = jnp.zeros((64, 64), F32)
    mine = lat_all[pl.ds(pl.multiple_of(tp * 8, 8), 8), :]
    for r in range(8):
        lat_send[r] = mine[r : r + 1, :]
    lat_recv[kv] = lat_send[kv // 2]

    def lat_copy(d):
        to = (kv + d) % 16
        return pltpu.make_async_remote_copy(
            src_ref=lat_send.at[to // 2], dst_ref=lat_recv.at[kv], send_sem=lat_ss.at[d], recv_sem=lat_rs.at[kv],
            device_id=(to, tp), device_id_type=MESH,
        )

    def lat_start(d, c):
        lat_copy(d).start()
        return c


    len_col = to_column(lens[...].astype(F32), 64)
    len_tab[...] = jnp.broadcast_to(len_col, (64, 128))
    lane = iota((32, 128), 1)
    packed_len = jnp.where(lane < 64, len_col[:32], len_col[32:])
    angle = packed_len * freq[...]
    cosine = jnp.cos(angle)
    sine = jnp.sin(angle)
    sine = jnp.where(lane % 64 < 32, -sine, sine)
    cos_tab[0:32, :] = cosine[:, :64]
    cos_tab[32:64, :] = cosine[:, 64:]
    sin_tab[0:32, :] = sine[:, :64]
    sin_tab[32:64, :] = sine[:, 64:]

    def added(own, recv, rows):
        total = own
        for d in range(3):
            total = total + recv[d, rows, :].astype(F32)
        return total

    for copy in a1:
        copy.wait_recv()
    q_nope_sum = added(q_nope_part, a1_recv, slice(0, 64))
    q_rope_sum = added(q_rope_part, a1_recv, slice(64, 96))
    a2_send[0:64, :] = q_nope_sum.astype(BF16)
    a2_send[64:96, :] = q_rope_sum.astype(BF16)
    a2 = line(a2_send, a2_recv, a2_ss, a2_rs, z_dev)
    for copy in a2:
        copy.start()
    for copy in a2:
        copy.wait_recv()
    q_nope = added(q_nope_sum, a2_recv, slice(0, 64)).astype(BF16)
    q_rope = added(q_rope_sum, a2_recv, slice(64, 96)).astype(BF16).astype(F32)
    swapped = jnp.where(lane % 64 < 32, pltpu.roll(q_rope, 96, 1), pltpu.roll(q_rope, 32, 1))
    q_rope = q_rope * cosine + swapped * sine
    q_rope = jnp.concatenate([q_rope[:, :64], q_rope[:, 64:]], axis=0)

    lax.fori_loop(1, 16, lat_start, 0)

    for d in (1, 3, 2):
        out_y(d, (y + d) % 4).wait_recv()
    for d in (1, 3, 2):
        out_z(d, z).start()
    out_twin(0, core).start()

    loads[7].wait()
    q_lat = dot_nt(q_nope, wk[...])
    pad = jnp.zeros((8, 64), F32)
    for j in range(8):
        block = jnp.concatenate([q_lat[8 * j : 8 * j + 8], q_rope[8 * j : 8 * j + 8], pad], axis=1)
        b_send[j] = block.astype(BF16)

    def tp_copy(d, src, dst, ss, rs):
        to = (tp + d) % 8
        return pltpu.make_async_remote_copy(
            src_ref=src.at[to], dst_ref=dst.at[tp], send_sem=ss.at[d], recv_sem=rs.at[tp],
            device_id=(kv, to), device_id_type=MESH,
        )

    def tp_wait_copy(d, src, dst, ss, rs):
        frm = (tp + d) % 8
        return pltpu.make_async_remote_copy(
            src_ref=src.at[frm], dst_ref=dst.at[frm], send_sem=ss.at[d], recv_sem=rs.at[frm],
            device_id=(kv, frm), device_id_type=MESH,
        )

    def tp_exchange(src, dst, ss, rs):
        for d in range(1, 8):
            tp_copy(d, src, dst, ss, rs).start()
        dst[tp] = src[tp]
        for d in range(1, 8):
            tp_wait_copy(d, src, dst, ss, rs).wait_recv()

    tp_exchange(b_send, b_recv, b_ss, b_rs)

    for copy in value_forwards:
        copy.wait_recv()
        copy.start()

    r64 = iota((64, 64), 0)
    c64 = iota((64, 64), 1)
    swap = (c64 == (r64 % 8) * 8 + r64 // 8).astype(BF16)
    queries = jnp.concatenate([b_recv[h].astype(F32) for h in range(8)], axis=0).astype(BF16)
    queries = dot(swap, queries)
    for s in range(8):
        q_tab[s] = queries[8 * s : 8 * s + 8]

    def lat_wait(d, c):
        frm = (kv + d) % 16
        pltpu.make_async_remote_copy(
            src_ref=lat_send.at[kv // 2], dst_ref=lat_recv.at[frm], send_sem=lat_ss.at[d], recv_sem=lat_rs.at[frm],
            device_id=(frm, tp), device_id_type=MESH,
        ).wait_recv()
        return c

    lax.fori_loop(1, 16, lat_wait, 0)
    lat_sum = lat_recv[0]
    for k in range(1, 16):
        lat_sum = lat_sum + lat_recv[k]
    loads[8].wait()
    lat_raw = lat_sum[:, :512]
    latent = (
        lat_raw * lax.rsqrt(jnp.mean(lat_raw * lat_raw, axis=1, keepdims=True) + EPSILON) * lgain[...]
    ).astype(BF16).astype(F32)
    key_raw = lat_sum[:, 512:576]
    new_seq = kv // 2
    new_row = tp * 8 + new_seq
    key_swapped = jnp.concatenate([key_raw[:, 32:], key_raw[:, :32]], axis=1)
    new_rope = key_raw * cos_tab[pl.ds(new_row, 1), :] + key_swapped * sin_tab[pl.ds(new_row, 1), :]
    new_rope = new_rope.astype(BF16).astype(F32)
    factor = 192.0 ** (-0.5)
    q_new = q_tab[new_seq]
    new_score = (
        jnp.sum(q_new[:, :512] * latent, axis=1, keepdims=True)
        + jnp.sum(q_new[:, 512:576] * new_rope, axis=1, keepdims=True)
    ) * factor

    for copy in cache_loads:
        copy.wait()
    scores = jnp.concatenate(
        [
            dot_nt(q_tab[s].astype(BF16)[:, :512], cl[s]) + dot(q_tab[s].astype(BF16)[:, 512:576], cr[s])
            for s in range(8)
        ],
        axis=0,
    ) * factor
    row_seq = iota((64, 1), 0) // 8
    row_length = jnp.concatenate(
        [jnp.broadcast_to(len_tab[pl.ds(tp * 8 + s, 1), 0:1], (8, 1)) for s in range(8)], axis=0
    )
    positions = (kv * 512 + iota((64, 512), 1)).astype(F32)
    visible = positions < row_length
    is_new = jnp.logical_and(row_seq == new_seq, kv % 2 == 0)
    own_new = jnp.where(is_new, jnp.concatenate([new_score] * 8, axis=0), NEGATIVE)
    top = jnp.maximum(jnp.max(jnp.where(visible, scores, NEGATIVE), axis=1, keepdims=True), own_new)
    weights = jnp.where(visible, jnp.exp(scores - top), 0.0)
    new_weight = jnp.where(is_new, jnp.exp(own_new - top), 0.0)
    total = jnp.sum(weights, axis=1, keepdims=True) + new_weight
    some = total > 0.0
    safe = jnp.where(some, total, 1.0)
    lse = jnp.where(some, top + jnp.log(safe), NEGATIVE)
    hi = lse.astype(BF16).astype(F32)
    mid = (lse - hi).astype(BF16).astype(F32)
    low = lse - hi - mid
    lane64 = iota((64, 128), 1)
    acc = jnp.concatenate(
        [dot(weights[8 * s : 8 * s + 8].astype(BF16), cl[s]) for s in range(8)], axis=0
    ) + new_weight.astype(BF16).astype(F32) * latent
    o_tab[:, 0:512] = acc / safe
    o_tab[:, 512:640] = jnp.where(
        lane64 == 0, hi, jnp.where(lane64 == 1, mid, jnp.where(lane64 == 2, low, 0.0))
    )

    parts = dot(swap, o_tab[...].astype(BF16))
    lse = jnp.sum(parts[:, 512:640], axis=1, keepdims=True)

    def gather_wait(buf, ss, rs):
        for d in range(4):
            slot = (twin + 2 * d) % 8
            gather_copy(buf, ss, rs, 0, slot, twin).wait_recv()

    gather_wait(wv, gv_ss, gv_rs)
    value = jnp.concatenate(
        [dot(parts[8 * h : 8 * h + 8, :512].astype(BF16), wv[h]) for h in range(8)], axis=0
    )

    def combine(value, lse, send, recv, lse_send, lse_recv, sems, dev):
        send[...] = value.astype(BF16)
        lse_send[...] = to_row(lse, 64)
        copies = line(send, recv, sems[0], sems[1], dev)
        lse_copies = line(lse_send, lse_recv, sems[2], sems[3], dev)
        for copy in lse_copies + copies:
            copy.start()
        for copy in lse_copies:
            copy.wait_recv()
        others = [to_column(lse_recv[d], 64) for d in range(3)]
        top = lse
        for other in others:
            top = jnp.maximum(top, other)
        own_scale = jnp.exp(lse - top)
        scales = [jnp.exp(other - top) for other in others]
        total = own_scale + scales[0] + scales[1] + scales[2]
        for copy in copies:
            copy.wait_recv()
        merged = value * (own_scale / total)
        for d in range(3):
            merged = merged + recv[d].astype(F32) * (scales[d] / total)
        return merged, top + jnp.log(total), copies + lse_copies

    value, lse, c1 = combine(
        value, lse, c1_send, c1_recv, c1_lse, c1_lser, (c1_ss, c1_rs, cl1_ss, cl1_rs), x_dev
    )
    for d in (1, 3, 2):
        out_z(d, (z + d) % 4).wait_recv()
        out_twin(d, core).start()

    value, lse, c2 = combine(
        value, lse, c2_send, c2_recv, c2_lse, c2_lser, (c2_ss, c2_rs, cl2_ss, cl2_rs), z_dev
    )
    for d in range(4):
        out_twin(d, 1 - core).wait_recv()
    head_out = jnp.concatenate(
        [value[16 * r + 8 * c : 16 * r + 8 * c + 8] for c in range(2) for r in range(4)], axis=1
    ).astype(BF16)
    mixed_z = dot(head_out, jnp.concatenate([wo[k].reshape(1024, 128) for k in range(4)], axis=1))
    own_mixed = mixed_z[:, 0:128]
    for k in range(1, 4):
        own_mixed = jnp.where(z == k, mixed_z[:, 128 * k : 128 * k + 128], own_mixed)
    m_send[...] = own_mixed
    g_send[...] = to_row(jnp.sum(mixed_z * mixed_z, axis=1, keepdims=True), 8)

    def m_copy(d, slot, to):
        return pltpu.make_async_remote_copy(
            src_ref=m_send, dst_ref=m_recv.at[slot], send_sem=m_ss.at[d], recv_sem=m_rs.at[slot],
            device_id=(kv, to), device_id_type=MESH,
        )

    place = x * 8 + tp

    def g_copy(d, slot, to):
        return pltpu.make_async_remote_copy(
            src_ref=g_send, dst_ref=g_recv.at[slot], send_sem=g_ss.at[d], recv_sem=g_rs.at[slot],
            device_id=(z * 4 + to // 8, to % 8), device_id_type=MESH,
        )

    def g_start(d, c):
        g_copy(d, place, (place + d) % 32).start()
        return c

    def g_wait(d, c):
        frm = (place + d) % 32
        g_copy(d, frm, frm).wait_recv()
        return c

    for d in range(1, 8):
        m_copy(d, tp, (tp + d) % 8).start()
    lax.fori_loop(1, 32, g_start, 0)
    m_recv[tp] = m_send[...]
    g_recv[place] = g_send[...]
    loads[11].wait()
    for d in range(1, 8):
        frm = (tp + d) % 8
        m_copy(d, frm, frm).wait_recv()
    lax.fori_loop(1, 32, g_wait, 0)
    mixed = m_recv[...].reshape(64, 128)
    squares = []
    for j in range(8):
        total = g_recv[j]
        for k in range(1, 4):
            total = total + g_recv[8 * k + j]
        squares.append(jnp.broadcast_to(total, (8, 128)))
    inverse = lax.rsqrt(jnp.concatenate(squares, axis=0) / 2048.0 + EPSILON)
    picked = iota((64, 128), 0) % 8 == iota((64, 128), 1)
    inverse = jnp.sum(jnp.where(picked, inverse, 0.0), axis=1, keepdims=True)
    out_ref[...] = (mixed * inverse * ogain[...]).astype(BF16)

    for copy in a1 + a2 + c1 + c2 + value_sends + value_forwards:
        copy.wait_send()

    def drain_kv(d, c):
        lat_copy(d).wait_send()
        return c

    def drain_plane(d, c):
        g_copy(d, place, (place + d) % 32).wait_send()
        return c

    def drain_tp(d, c):
        tp_copy(d, b_send, b_recv, b_ss, b_rs).wait_send()
        m_copy(d, tp, (tp + d) % 8).wait_send()
        return c

    for d in range(4):
        out_twin(d, core).wait_send()
    for d in range(1, 4):
        out_y(d, y).wait_send()
        out_z(d, z).wait_send()
    lax.fori_loop(1, 16, drain_kv, 0)
    lax.fori_loop(1, 32, drain_plane, 0)
    lax.fori_loop(1, 8, drain_tp, 0)


def on_device(
    tokens, token_gain, w_query, w_down_kv, w_rope_key, latent_gain, w_key_up, w_value_up, w_out, out_gain,
    cache_latent, cache_rope, lengths,
):
    freq = 1.0 / 10000.0 ** (np.arange(0, 64, 2, dtype=np.float32) / np.float32(64.0))
    freq = jnp.asarray(np.tile(freq.astype(np.float32), 4)[None, :])
    operands = (
        tokens, token_gain.reshape(1, 128), w_query.T, w_down_kv, w_rope_key.T, latent_gain.reshape(1, 512),
        w_key_up.reshape(512, 128), w_value_up.reshape(512, 128), w_out, out_gain.reshape(1, 128),
        cache_latent, cache_rope.transpose(0, 2, 1), lengths.reshape(1, 64), freq,
    )
    shapes = [(a.shape, a.dtype) for a in operands]
    shapes[7] = ((8, 512, 128), BF16)
    shapes[8] = ((4, 2, 4, 128, 128), BF16)
    local = [pltpu.VMEM(*a) for a in shapes]
    dma = pltpu.SemaphoreType.DMA
    scratch = local + [
        pltpu.VMEM((64, 128), F32), pltpu.VMEM((64, 64), F32), pltpu.VMEM((64, 64), F32),
        pltpu.VMEM((96, 128), BF16), pltpu.VMEM((3, 96, 128), BF16),
        pltpu.VMEM((96, 128), BF16), pltpu.VMEM((3, 96, 128), BF16),
        pltpu.VMEM((64, 640), F32), pltpu.VMEM((8, 1, 640), F32), pltpu.VMEM((16, 1, 640), F32),
        pltpu.VMEM((8, 8, 640), BF16), pltpu.VMEM((8, 8, 640), BF16),
        pltpu.VMEM((8, 8, 640), F32), pltpu.VMEM((64, 640), F32),
        pltpu.VMEM((64, 128), BF16), pltpu.VMEM((3, 64, 128), BF16),
        pltpu.VMEM((1, 128), F32), pltpu.VMEM((3, 1, 128), F32),
        pltpu.VMEM((64, 128), BF16), pltpu.VMEM((3, 64, 128), BF16),
        pltpu.VMEM((1, 128), F32), pltpu.VMEM((3, 1, 128), F32),
        pltpu.VMEM((8, 128), F32), pltpu.VMEM((8, 8, 128), F32),
        pltpu.VMEM((1, 128), F32), pltpu.VMEM((32, 1, 128), F32),
        dma((12,)), dma((16,)),
        dma((3,)), dma((3,)), dma((3,)), dma((3,)), dma((16,)), dma((16,)),
        dma((8,)), dma((8,)), dma((8,)), dma((8,)),
        dma((4,)), dma((4,)), dma((4,)), dma((4,)), dma((4,)), dma((4,)),
        dma((3,)), dma((3,)), dma((3,)), dma((3,)), dma((3,)), dma((3,)), dma((3,)), dma((3,)),
        dma((8,)), dma((8,)), dma((32,)), dma((32,)),
    ]
    return pl.pallas_call(
        kernel,
        out_shape=jax.ShapeDtypeStruct((64, 128), BF16),
        in_specs=[pl.BlockSpec(memory_space=pltpu.HBM)] * len(operands),
        out_specs=pl.BlockSpec(memory_space=pltpu.VMEM),
        scratch_shapes=scratch,
        compiler_params=pltpu.CompilerParams(
            collective_id=0, has_side_effects=True, vmem_limit_bytes=67043328
        ),
    )(*operands)


def solution(mesh):
    return jax.shard_map(
        on_device,
        mesh=mesh,
        in_specs=(
            P(None, "kv"), P("kv"), P("kv", "tp"), P("kv", None), P("kv", None), P(),
            P("tp", None, None), P("tp", None, None), P("tp", "kv"), P("kv"),
            P("tp", "kv", None), P("tp", "kv", None), P(),
        ),
        out_specs=P(None, "kv"),
        check_vma=False,
    )
```

```python
import functools

import jax
import jax.numpy as jnp
import numpy as np
from jax import lax
from jax.experimental import pallas as pl
from jax.experimental.pallas import tpu as pltpu
from jax.sharding import PartitionSpec as P

MESH = pl.DeviceIdType.MESH
EPSILON = 1e-06
NEGATIVE = -1e30
BF16 = jnp.bfloat16
F32 = jnp.float32


def dot(a, b):
    return jnp.dot(a, b, preferred_element_type=F32)


def dot_nt(a, b):
    return lax.dot_general(a, b, (((1,), (1,)), ((), ())), preferred_element_type=F32)


def iota(shape, axis):
    return lax.broadcasted_iota(jnp.int32, shape, axis)


def to_column(row, rows):
    picked = iota((rows, rows), 0) == iota((rows, rows), 1)
    return jnp.sum(jnp.where(picked, row[:, :rows], 0.0), axis=1, keepdims=True)


def to_row(column, rows):
    picked = iota((rows, 128), 0) == iota((rows, 128), 1)
    return jnp.sum(jnp.where(picked, column, 0.0), axis=0, keepdims=True)


def kernel(
    tok_h, tgain_h, wq_h, wd_h, wr_h, lgain_h, wk_h, wv_h, wo_h, ogain_h, cl_h, cr_h, len_h, freq_h,
    out_ref,
    tok, tgain, wq, wd, wr, lgain, wk, wv, wo, ogain, cl, cr, lens, freq,
    len_tab, cos_tab, sin_tab,
    a1_send, a1_recv, a2_send, a2_recv,
    lat_all, lat_send, lat_recv,
    b_send, b_recv, q_tab, o_tab,
    c1_send, c1_recv, c1_lse, c1_lser, c2_send, c2_recv, c2_lse, c2_lser,
    m_send, m_recv, g_send, g_recv, result,
    load_sem, cache_sem, result_sem,
    a1_ss, a1_rs, a2_ss, a2_rs, lat_ss, lat_rs, b_ss, b_rs, gv_ss, gv_rs, oy_ss, oy_rs, oz_ss, oz_rs, ot_ss, ot_rs,
    c1_ss, c1_rs, c2_ss, c2_rs, cl1_ss, cl1_rs, cl2_ss, cl2_rs, m_ss, m_rs, g_ss, g_rs,
):
    kv = lax.axis_index("kv")
    tp = lax.axis_index("tp")
    z = kv // 4
    x = kv % 4
    y = tp // 2
    core = tp % 2

    barrier = pltpu.get_barrier_semaphore()

    def greet_line(d, c):
        pl.semaphore_signal(barrier, inc=1, device_id=(z * 4 + (x + d) % 4, tp), device_id_type=MESH)
        pl.semaphore_signal(barrier, inc=1, device_id=((z + d) % 4 * 4 + x, tp), device_id_type=MESH)
        return c

    def greet_tp(d, c):
        pl.semaphore_signal(barrier, inc=1, device_id=(kv, (tp + d) % 8), device_id_type=MESH)
        return c

    lax.fori_loop(1, 4, greet_line, 0)
    lax.fori_loop(1, 8, greet_tp, 0)

    pairs = [
        (tok_h, tok), (tgain_h, tgain), (wq_h, wq), (len_h, lens), (freq_h, freq), (wd_h, wd), (wr_h, wr),
        (wk_h, wk), (lgain_h, lgain), (wv_h, wv.at[tp]), (wo_h, wo.at[z, core, y]), (ogain_h, ogain),
    ]
    loads = [pltpu.make_async_copy(s, d, load_sem.at[i]) for i, (s, d) in enumerate(pairs)]
    for copy in loads:
        copy.start()
    cache_loads = []
    for s in range(8):
        cache_loads.append(pltpu.make_async_copy(cl_h.at[s], cl.at[s], cache_sem.at[s]))
        cache_loads.append(pltpu.make_async_copy(cr_h.at[s], cr.at[s], cache_sem.at[8 + s]))
    for copy in cache_loads:
        copy.start()

    for i in range(3):
        loads[i].wait()
    scaled = (tok[...].astype(F32) * tgain[...]).astype(BF16)
    q_part = dot_nt(scaled, wq[...])
    rope_part = q_part[:, 128:192]
    q_nope_part = q_part[:, :128]
    q_rope_part = jnp.concatenate([rope_part[:32], rope_part[32:]], axis=1)
    a1_send[0:64, :] = q_nope_part.astype(BF16)
    a1_send[64:96, :] = q_rope_part.astype(BF16)

    pl.semaphore_wait(barrier, 13)

    def x_dev(d):
        return (z * 4 + (x + d) % 4, tp)

    def z_dev(d):
        return (((z + d) % 4) * 4 + x, tp)

    def line(src, dst, ss, rs, dev):
        return [
            pltpu.make_async_remote_copy(
                src_ref=src, dst_ref=dst.at[d - 1], send_sem=ss.at[d - 1], recv_sem=rs.at[d - 1],
                device_id=dev(d), device_id_type=MESH,
            )
            for d in (1, 2, 3)
        ]

    a1 = line(a1_send, a1_recv, a1_ss, a1_rs, x_dev)
    for copy in a1:
        copy.start()

    twin = tp + 1 - 2 * core

    def gather_copy(buf, ss, rs, i, slot, to):
        return pltpu.make_async_remote_copy(
            src_ref=buf.at[slot], dst_ref=buf.at[slot], send_sem=ss.at[i], recv_sem=rs.at[slot],
            device_id=(kv, to), device_id_type=MESH,
        )

    def gather_first(buf, ss, rs):
        copies = [gather_copy(buf, ss, rs, i, tp, (tp + 2 * d) % 8) for i, d in enumerate((1, 3, 2))]
        return copies + [gather_copy(buf, ss, rs, 3, tp, twin)]

    def gather_forward(buf, ss, rs):
        slots = [(tp + 2 * d) % 8 for d in (1, 3, 2)]
        return [gather_copy(buf, ss, rs, 4 + i, slot, twin) for i, slot in enumerate(slots)]

    loads[9].wait()
    loads[10].wait()
    value_sends = gather_first(wv, gv_ss, gv_rs)
    value_forwards = gather_forward(wv, gv_ss, gv_rs)

    def out_y(d, at):
        return pltpu.make_async_remote_copy(
            src_ref=wo.at[z, core, y], dst_ref=wo.at[z, core, at], send_sem=oy_ss.at[d], recv_sem=oy_rs.at[at],
            device_id=(kv, (tp + 2 * d) % 8), device_id_type=MESH,
        )

    def out_z(d, at):
        return pltpu.make_async_remote_copy(
            src_ref=wo.at[z, core], dst_ref=wo.at[at, core], send_sem=oz_ss.at[d], recv_sem=oz_rs.at[at],
            device_id=((z + d) % 4 * 4 + x, tp), device_id_type=MESH,
        )

    def out_twin(d, half):
        at = (z + d) % 4
        return pltpu.make_async_remote_copy(
            src_ref=wo.at[at, core], dst_ref=wo.at[at, half], send_sem=ot_ss.at[d], recv_sem=ot_rs.at[at],
            device_id=(kv, twin), device_id_type=MESH,
        )

    for d in (1, 3, 2):
        out_y(d, y).start()
    for copy in value_sends:
        copy.start()

    for i in range(3, 7):
        loads[i].wait()
    lat_all[:, 0:512] = dot(scaled, wd[...])
    lat_all[:, 512:576] = dot_nt(scaled, wr[...])
    lat_all[:, 576:640] = jnp.zeros((64, 64), F32)
    mine = lat_all[pl.ds(pl.multiple_of(tp * 8, 8), 8), :]
    for r in range(8):
        lat_send[r] = mine[r : r + 1, :]
    lat_recv[kv] = lat_send[kv // 2]

    def lat_copy(d):
        to = (kv + d) % 16
        return pltpu.make_async_remote_copy(
            src_ref=lat_send.at[to // 2], dst_ref=lat_recv.at[kv], send_sem=lat_ss, recv_sem=lat_rs,
            device_id=(to, tp), device_id_type=MESH,
        )

    def lat_start(d, c):
        lat_copy(d).start()
        return c


    len_col = to_column(lens[...].astype(F32), 64)
    len_tab[...] = jnp.broadcast_to(len_col, (64, 128))
    lane = iota((32, 128), 1)
    packed_len = jnp.where(lane < 64, len_col[:32], len_col[32:])
    angle = packed_len * freq[...]
    cosine = jnp.cos(angle)
    sine = jnp.sin(angle)
    sine = jnp.where(lane % 64 < 32, -sine, sine)
    cos_tab[0:32, :] = cosine[:, :64]
    cos_tab[32:64, :] = cosine[:, 64:]
    sin_tab[0:32, :] = sine[:, :64]
    sin_tab[32:64, :] = sine[:, 64:]

    def added(own, recv, rows):
        total = own
        for d in range(3):
            total = total + recv[d, rows, :].astype(F32)
        return total

    for copy in a1:
        copy.wait_recv()
    q_nope_sum = added(q_nope_part, a1_recv, slice(0, 64))
    q_rope_sum = added(q_rope_part, a1_recv, slice(64, 96))
    a2_send[0:64, :] = q_nope_sum.astype(BF16)
    a2_send[64:96, :] = q_rope_sum.astype(BF16)
    a2 = line(a2_send, a2_recv, a2_ss, a2_rs, z_dev)
    for copy in a2:
        copy.start()
    for copy in a2:
        copy.wait_recv()
    q_nope = added(q_nope_sum, a2_recv, slice(0, 64)).astype(BF16)
    q_rope = added(q_rope_sum, a2_recv, slice(64, 96)).astype(BF16).astype(F32)
    swapped = jnp.where(lane % 64 < 32, pltpu.roll(q_rope, 96, 1), pltpu.roll(q_rope, 32, 1))
    q_rope = q_rope * cosine + swapped * sine
    q_rope = jnp.concatenate([q_rope[:, :64], q_rope[:, 64:]], axis=0)


    loads[7].wait()
    q_lat = dot_nt(q_nope, wk[...])
    pad = jnp.zeros((8, 64), F32)
    for j in range(8):
        block = jnp.concatenate([q_lat[8 * j : 8 * j + 8], q_rope[8 * j : 8 * j + 8], pad], axis=1)
        b_send[j] = block.astype(BF16)

    def b_copy(d):
        to = (tp + d) % 8
        return pltpu.make_async_remote_copy(
            src_ref=b_send.at[to], dst_ref=b_recv.at[tp], send_sem=b_ss, recv_sem=b_rs,
            device_id=(kv, to), device_id_type=MESH,
        )

    def all_of(ref, count, ss, rs):
        part = ref.at[pl.ds(0, count)]
        return pltpu.make_async_remote_copy(
            src_ref=part, dst_ref=part, send_sem=ss, recv_sem=rs, device_id=(kv, twin), device_id_type=MESH
        )

    for d in (4, 5, 3, 2, 6, 7, 1):
        b_copy(d).start()
    lax.fori_loop(1, 16, lat_start, 0)
    b_recv[tp] = b_send[tp]
    for d in (1, 3, 2):
        out_y(d, (y + d) % 4).wait_recv()
    for d in (1, 3, 2):
        out_z(d, z).start()
    out_twin(0, core).start()
    all_of(b_recv, 7, b_ss, b_rs).wait_recv()

    for copy in value_forwards:
        copy.wait_recv()
        copy.start()

    for h in range(8):
        rows = b_recv[h].astype(F32)
        for i in range(5):
            q_tab[i, 8 * h : 8 * h + 8, :] = rows[:, 128 * i : 128 * i + 128]

    def query_of(s):
        return jnp.concatenate([q_tab[i, pl.ds(s, 8, stride=8), :] for i in range(5)], axis=1)

    for copy in cache_loads:
        copy.wait()
    factor = 192.0 ** (-0.5)

    def scores_of(s):
        q = query_of(s).astype(BF16)
        return dot_nt(q[:, :512], cl[s]) + dot(q[:, 512:576], cr[s])

    scores = jnp.concatenate([scores_of(s) for s in range(8)], axis=0) * factor

    all_of(lat_recv, 15, lat_ss, lat_rs).wait_recv()
    lat_sum = lat_recv[0]
    for k in range(1, 16):
        lat_sum = lat_sum + lat_recv[k]
    loads[8].wait()
    lat_raw = lat_sum[:, :512]
    latent = (
        lat_raw * lax.rsqrt(jnp.mean(lat_raw * lat_raw, axis=1, keepdims=True) + EPSILON) * lgain[...]
    ).astype(BF16).astype(F32)
    key_raw = lat_sum[:, 512:576]
    new_seq = kv // 2
    new_row = tp * 8 + new_seq
    key_swapped = jnp.concatenate([key_raw[:, 32:], key_raw[:, :32]], axis=1)
    new_rope = key_raw * cos_tab[pl.ds(new_row, 1), :] + key_swapped * sin_tab[pl.ds(new_row, 1), :]
    new_rope = new_rope.astype(BF16).astype(F32)
    q_new = query_of(new_seq)
    new_score = (
        jnp.sum(q_new[:, :512] * latent, axis=1, keepdims=True)
        + jnp.sum(q_new[:, 512:576] * new_rope, axis=1, keepdims=True)
    ) * factor

    row_seq = iota((64, 1), 0) // 8
    row_length = jnp.concatenate(
        [jnp.broadcast_to(len_tab[pl.ds(tp * 8 + s, 1), 0:1], (8, 1)) for s in range(8)], axis=0
    )
    positions = (kv * 512 + iota((64, 512), 1)).astype(F32)
    visible = positions < row_length
    is_new = jnp.logical_and(row_seq == new_seq, kv % 2 == 0)
    own_new = jnp.where(is_new, jnp.concatenate([new_score] * 8, axis=0), NEGATIVE)
    top = jnp.maximum(jnp.max(jnp.where(visible, scores, NEGATIVE), axis=1, keepdims=True), own_new)
    weights = jnp.where(visible, jnp.exp(scores - top), 0.0)
    new_weight = jnp.where(is_new, jnp.exp(own_new - top), 0.0)
    total = jnp.sum(weights, axis=1, keepdims=True) + new_weight
    some = total > 0.0
    safe = jnp.where(some, total, 1.0)
    lse = jnp.where(some, top + jnp.log(safe), NEGATIVE)
    acc = jnp.concatenate(
        [dot(weights[8 * s : 8 * s + 8].astype(BF16), cl[s]) for s in range(8)], axis=0
    ) + new_weight.astype(BF16).astype(F32) * latent

    def gather_wait(buf, ss, rs):
        for d in range(4):
            slot = (twin + 2 * d) % 8
            gather_copy(buf, ss, rs, 0, slot, twin).wait_recv()

    gather_wait(wv, gv_ss, gv_rs)
    by_head = dot(acc.astype(BF16), jnp.concatenate([wv[h] for h in range(8)], axis=1))
    value = by_head[:, 0:128]
    row_head = iota((64, 128), 0) % 8
    for h in range(1, 8):
        value = jnp.where(row_head == h, by_head[:, 128 * h : 128 * h + 128], value)
    value = value / safe

    def combine(value, lse, send, recv, lse_send, lse_recv, sems, dev):
        send[...] = value.astype(BF16)
        lse_send[...] = to_row(lse, 64)
        copies = line(send, recv, sems[0], sems[1], dev)
        lse_copies = line(lse_send, lse_recv, sems[2], sems[3], dev)
        for copy in lse_copies + copies:
            copy.start()
        for copy in lse_copies:
            copy.wait_recv()
        others = [to_column(lse_recv[d], 64) for d in range(3)]
        top = lse
        for other in others:
            top = jnp.maximum(top, other)
        own_scale = jnp.exp(lse - top)
        scales = [jnp.exp(other - top) for other in others]
        total = own_scale + scales[0] + scales[1] + scales[2]
        for copy in copies:
            copy.wait_recv()
        merged = value * (own_scale / total)
        for d in range(3):
            merged = merged + recv[d].astype(F32) * (scales[d] / total)
        return merged, top + jnp.log(total), copies + lse_copies

    value, lse, c1 = combine(
        value, lse, c1_send, c1_recv, c1_lse, c1_lser, (c1_ss, c1_rs, cl1_ss, cl1_rs), x_dev
    )
    for d in (1, 3, 2):
        out_z(d, (z + d) % 4).wait_recv()
        out_twin(d, core).start()

    value, lse, c2 = combine(
        value, lse, c2_send, c2_recv, c2_lse, c2_lser, (c2_ss, c2_rs, cl2_ss, cl2_rs), z_dev
    )
    for d in range(4):
        out_twin(d, 1 - core).wait_recv()
    o_tab[...] = value
    head_out = jnp.concatenate(
        [o_tab[pl.ds(2 * r + c, 8, stride=8), :] for c in range(2) for r in range(4)], axis=1
    ).astype(BF16)
    mixed_z = dot(head_out, jnp.concatenate([wo[k].reshape(1024, 128) for k in range(4)], axis=1))
    own_mixed = mixed_z[:, 0:128]
    for k in range(1, 4):
        own_mixed = jnp.where(z == k, mixed_z[:, 128 * k : 128 * k + 128], own_mixed)
    m_send[...] = own_mixed
    g_send[...] = to_row(jnp.sum(mixed_z * mixed_z, axis=1, keepdims=True), 8)

    def m_copy(slot, to):
        return pltpu.make_async_remote_copy(
            src_ref=m_send, dst_ref=m_recv.at[slot], send_sem=m_ss, recv_sem=m_rs,
            device_id=(kv, to), device_id_type=MESH,
        )

    place = x * 8 + tp

    def g_copy(slot, to):
        return pltpu.make_async_remote_copy(
            src_ref=g_send, dst_ref=g_recv.at[slot], send_sem=g_ss, recv_sem=g_rs,
            device_id=(z * 4 + to // 8, to % 8), device_id_type=MESH,
        )

    def g_start(i, c):
        g_copy(place, (place + (i + 12) % 31 + 1) % 32).start()
        return c

    lax.fori_loop(0, 31, g_start, 0)
    for d in (4, 5, 3, 2, 6, 7, 1):
        m_copy(tp, (tp + d) % 8).start()
    m_recv[tp] = m_send[...]
    g_recv[place] = g_send[...]
    loads[11].wait()

    for copy in a1 + a2 + c1 + c2 + value_sends + value_forwards:
        copy.wait_send()
    for d in range(4):
        out_twin(d, core).wait_send()
    for d in range(1, 4):
        out_y(d, y).wait_send()
        out_z(d, z).wait_send()
    all_of(b_recv, 7, b_ss, b_rs).wait_send()
    all_of(lat_recv, 15, lat_ss, lat_rs).wait_send()

    all_of(m_recv, 7, m_ss, m_rs).wait_recv()
    all_of(g_recv, 31, g_ss, g_rs).wait_recv()
    mixed = m_recv[...].reshape(64, 128)
    squares = []
    for j in range(8):
        total = g_recv[j]
        for k in range(1, 4):
            total = total + g_recv[8 * k + j]
        squares.append(jnp.broadcast_to(total, (8, 128)))
    inverse = lax.rsqrt(jnp.concatenate(squares, axis=0) / 2048.0 + EPSILON)
    picked = iota((64, 128), 0) % 8 == iota((64, 128), 1)
    inverse = jnp.sum(jnp.where(picked, inverse, 0.0), axis=1, keepdims=True)
    result[...] = (mixed * inverse * ogain[...]).astype(BF16)
    leaving = pltpu.make_async_copy(result, out_ref, result_sem)
    leaving.start()

    all_of(m_recv, 7, m_ss, m_rs).wait_send()
    all_of(g_recv, 31, g_ss, g_rs).wait_send()
    leaving.wait()


def on_device(
    tokens, token_gain, w_query, w_down_kv, w_rope_key, latent_gain, w_key_up, w_value_up, w_out, out_gain,
    cache_latent, cache_rope, lengths,
):
    freq = 1.0 / 10000.0 ** (np.arange(0, 64, 2, dtype=np.float32) / np.float32(64.0))
    freq = jnp.asarray(np.tile(freq.astype(np.float32), 4)[None, :])
    operands = (
        tokens, token_gain.reshape(1, 128), w_query.T, w_down_kv, w_rope_key.T, latent_gain.reshape(1, 512),
        w_key_up.reshape(512, 128), w_value_up.reshape(512, 128), w_out, out_gain.reshape(1, 128),
        cache_latent, cache_rope.transpose(0, 2, 1), lengths.reshape(1, 64), freq,
    )
    shapes = [(a.shape, a.dtype) for a in operands]
    shapes[7] = ((8, 512, 128), BF16)
    shapes[8] = ((4, 2, 4, 128, 128), BF16)
    local = [pltpu.VMEM(*a) for a in shapes]
    dma = pltpu.SemaphoreType.DMA
    scratch = local + [
        pltpu.VMEM((64, 128), F32), pltpu.VMEM((64, 64), F32), pltpu.VMEM((64, 64), F32),
        pltpu.VMEM((96, 128), BF16), pltpu.VMEM((3, 96, 128), BF16),
        pltpu.VMEM((96, 128), BF16), pltpu.VMEM((3, 96, 128), BF16),
        pltpu.VMEM((64, 640), F32), pltpu.VMEM((8, 1, 640), F32), pltpu.VMEM((16, 1, 640), F32),
        pltpu.VMEM((8, 8, 640), BF16), pltpu.VMEM((8, 8, 640), BF16),
        pltpu.VMEM((5, 64, 128), F32), pltpu.VMEM((64, 128), F32),
        pltpu.VMEM((64, 128), BF16), pltpu.VMEM((3, 64, 128), BF16),
        pltpu.VMEM((1, 128), F32), pltpu.VMEM((3, 1, 128), F32),
        pltpu.VMEM((64, 128), BF16), pltpu.VMEM((3, 64, 128), BF16),
        pltpu.VMEM((1, 128), F32), pltpu.VMEM((3, 1, 128), F32),
        pltpu.VMEM((8, 128), F32), pltpu.VMEM((8, 8, 128), F32),
        pltpu.VMEM((1, 128), F32), pltpu.VMEM((32, 1, 128), F32),
        pltpu.VMEM((64, 128), BF16),
        dma((12,)), dma((16,)), dma,
        dma((3,)), dma((3,)), dma((3,)), dma((3,)), dma, dma,
        dma, dma, dma((8,)), dma((8,)),
        dma((4,)), dma((4,)), dma((4,)), dma((4,)), dma((4,)), dma((4,)),
        dma((3,)), dma((3,)), dma((3,)), dma((3,)), dma((3,)), dma((3,)), dma((3,)), dma((3,)),
        dma, dma, dma, dma,
    ]
    return pl.pallas_call(
        kernel,
        out_shape=jax.ShapeDtypeStruct((64, 128), BF16),
        in_specs=[pl.BlockSpec(memory_space=pltpu.HBM)] * len(operands),
        out_specs=pl.BlockSpec(memory_space=pl.ANY),
        scratch_shapes=scratch,
        compiler_params=pltpu.CompilerParams(
            collective_id=0, has_side_effects=True, vmem_limit_bytes=67043328
        ),
    )(*operands)


def solution(mesh):
    return jax.shard_map(
        on_device,
        mesh=mesh,
        in_specs=(
            P(None, "kv"), P("kv"), P("kv", "tp"), P("kv", None), P("kv", None), P(),
            P("tp", None, None), P("tp", None, None), P("tp", "kv"), P("kv"),
            P("tp", "kv", None), P("tp", "kv", None), P(),
        ),
        out_specs=P(None, "kv"),
        check_vma=False,
    )
```

```python
import functools

import jax
import jax.numpy as jnp
import numpy as np
from jax import lax
from jax.experimental import pallas as pl
from jax.experimental.pallas import tpu as pltpu
from jax.sharding import PartitionSpec as P

MESH = pl.DeviceIdType.MESH
EPSILON = 1e-06
NEGATIVE = -1e30
BF16 = jnp.bfloat16
F32 = jnp.float32


def dot(a, b):
    return jnp.dot(a, b, preferred_element_type=F32)


def dot_nt(a, b):
    return lax.dot_general(a, b, (((1,), (1,)), ((), ())), preferred_element_type=F32)


def iota(shape, axis):
    return lax.broadcasted_iota(jnp.int32, shape, axis)


def to_column(row, rows):
    picked = iota((rows, rows), 0) == iota((rows, rows), 1)
    return jnp.sum(jnp.where(picked, row[:, :rows], 0.0), axis=1, keepdims=True)


def to_row(column, rows):
    picked = iota((rows, 128), 0) == iota((rows, 128), 1)
    return jnp.sum(jnp.where(picked, column, 0.0), axis=0, keepdims=True)


def kernel(
    tok_h, tgain_h, wq_h, wd_h, wr_h, lgain_h, wk_h, wv_h, wo_h, ogain_h, cl_h, cr_h, len_h, freq_h,
    out_ref,
    tok, tgain, wq, wd, wr, lgain, wk, wv, wo, ogain, cl, cr, lens, freq,
    len_tab, cos_tab, sin_tab,
    a1_send, a1_recv, a2_send, a2_recv,
    lat_all, lat_send, lat_recv,
    b_send, b_recv, q_tab, o_tab,
    c1_send, c1_recv, c2_send, c2_recv, l_send, l_recv,
    m_send, m_recv, g_send, g_recv,
    load_sem, cache_sem,
    a1_ss, a1_rs, a2_ss, a2_rs, lat_ss, lat_rs, b_ss, b_rs, gv_ss, gv_rs, oy_ss, oy_rs, oz_ss, oz_rs, ot_ss, ot_rs,
    c1_ss, c1_rs, c2_ss, c2_rs, lx_ss, lx_rs, lo_ss, lo_rs, m_ss, m_rs, g_ss, g_rs,
):
    kv = lax.axis_index("kv")
    tp = lax.axis_index("tp")
    z = kv // 4
    x = kv % 4
    y = tp // 2
    core = tp % 2

    pairs = [
        (tok_h, tok), (tgain_h, tgain), (wq_h, wq), (len_h, lens), (freq_h, freq), (wd_h, wd), (wr_h, wr),
        (wk_h, wk), (lgain_h, lgain), (wv_h, wv.at[tp]), (wo_h, wo.at[z, core, y]), (ogain_h, ogain),
    ]
    loads = [pltpu.make_async_copy(s, d, load_sem.at[i]) for i, (s, d) in enumerate(pairs)]
    cache_loads = []
    for s in range(8):
        cache_loads.append(pltpu.make_async_copy(cl_h.at[s], cl.at[s], cache_sem.at[s]))
        cache_loads.append(pltpu.make_async_copy(cr_h.at[s], cr.at[s], cache_sem.at[8 + s]))
    for copy in loads[:3]:
        copy.start()
    barrier = pltpu.get_barrier_semaphore()

    def greet_line(d, c):
        pl.semaphore_signal(barrier, inc=1, device_id=(z * 4 + (x + d) % 4, tp), device_id_type=MESH)
        pl.semaphore_signal(barrier, inc=1, device_id=((z + d) % 4 * 4 + x, tp), device_id_type=MESH)
        return c

    def greet_tp(d, c):
        pl.semaphore_signal(barrier, inc=1, device_id=(kv, (tp + d) % 8), device_id_type=MESH)
        return c

    lax.fori_loop(1, 4, greet_line, 0)
    lax.fori_loop(1, 8, greet_tp, 0)


    for i in range(3):
        loads[i].wait()
    scaled = (tok[...].astype(F32) * tgain[...]).astype(BF16)
    q_part = dot_nt(scaled, wq[...])
    rope_part = q_part[:, 128:192]
    q_nope_part = q_part[:, :128]
    q_rope_part = jnp.concatenate([rope_part[:32], rope_part[32:]], axis=1)
    a1_send[0:64, :] = q_nope_part.astype(BF16)
    a1_send[64:96, :] = q_rope_part.astype(BF16)

    for copy in loads[3:] + cache_loads:
        copy.start()
    pl.semaphore_wait(barrier, 13)

    def x_dev(d):
        return (z * 4 + (x + d) % 4, tp)

    def z_dev(d):
        return (((z + d) % 4) * 4 + x, tp)

    def line(src, dst, ss, rs, dev):
        return [
            pltpu.make_async_remote_copy(
                src_ref=src, dst_ref=dst.at[d - 1], send_sem=ss.at[d - 1], recv_sem=rs.at[d - 1],
                device_id=dev(d), device_id_type=MESH,
            )
            for d in (1, 2, 3)
        ]

    a1 = line(a1_send, a1_recv, a1_ss, a1_rs, x_dev)
    for copy in a1:
        copy.start()

    twin = tp + 1 - 2 * core

    def gather_copy(buf, ss, rs, i, slot, to):
        return pltpu.make_async_remote_copy(
            src_ref=buf.at[slot], dst_ref=buf.at[slot], send_sem=ss.at[i], recv_sem=rs.at[slot],
            device_id=(kv, to), device_id_type=MESH,
        )

    def gather_first(buf, ss, rs):
        copies = [gather_copy(buf, ss, rs, i, tp, (tp + 2 * d) % 8) for i, d in enumerate((1, 3, 2))]
        return copies + [gather_copy(buf, ss, rs, 3, tp, twin)]

    def gather_forward(buf, ss, rs):
        slots = [(tp + 2 * d) % 8 for d in (1, 3, 2)]
        return [gather_copy(buf, ss, rs, 4 + i, slot, twin) for i, slot in enumerate(slots)]

    loads[9].wait()
    loads[10].wait()
    value_sends = gather_first(wv, gv_ss, gv_rs)
    value_forwards = gather_forward(wv, gv_ss, gv_rs)

    def out_y(d, at):
        return pltpu.make_async_remote_copy(
            src_ref=wo.at[z, core, y], dst_ref=wo.at[z, core, at], send_sem=oy_ss.at[d], recv_sem=oy_rs.at[at],
            device_id=(kv, (tp + 2 * d) % 8), device_id_type=MESH,
        )

    def out_z(d, at):
        return pltpu.make_async_remote_copy(
            src_ref=wo.at[z, core], dst_ref=wo.at[at, core], send_sem=oz_ss.at[d], recv_sem=oz_rs.at[at],
            device_id=((z + d) % 4 * 4 + x, tp), device_id_type=MESH,
        )

    def out_twin(d, half):
        at = (z + d) % 4
        return pltpu.make_async_remote_copy(
            src_ref=wo.at[at, core], dst_ref=wo.at[at, half], send_sem=ot_ss.at[d], recv_sem=ot_rs.at[at],
            device_id=(kv, twin), device_id_type=MESH,
        )

    for d in (1, 3, 2):
        out_y(d, y).start()
    for copy in value_sends:
        copy.start()

    for i in range(3, 7):
        loads[i].wait()
    lat_all[:, 0:512] = dot(scaled, wd[...])
    lat_all[:, 512:576] = dot_nt(scaled, wr[...])
    lat_all[:, 576:640] = jnp.zeros((64, 64), F32)
    mine = lat_all[pl.ds(pl.multiple_of(tp * 8, 8), 8), :]
    for r in range(8):
        lat_send[r] = mine[r : r + 1, :]
    lat_recv[kv] = lat_send[kv // 2]

    def lat_copy(d):
        to = (kv + d) % 16
        return pltpu.make_async_remote_copy(
            src_ref=lat_send.at[to // 2], dst_ref=lat_recv.at[kv], send_sem=lat_ss, recv_sem=lat_rs,
            device_id=(to, tp), device_id_type=MESH,
        )

    def lat_start(d, c):
        lat_copy(d).start()
        return c


    len_col = to_column(lens[...].astype(F32), 64)
    len_tab[...] = jnp.broadcast_to(len_col, (64, 128))
    lane = iota((32, 128), 1)
    packed_len = jnp.where(lane < 64, len_col[:32], len_col[32:])
    angle = packed_len * freq[...]
    cosine = jnp.cos(angle)
    sine = jnp.sin(angle)
    sine = jnp.where(lane % 64 < 32, -sine, sine)
    cos_tab[0:32, :] = cosine[:, :64]
    cos_tab[32:64, :] = cosine[:, 64:]
    sin_tab[0:32, :] = sine[:, :64]
    sin_tab[32:64, :] = sine[:, 64:]

    def added(own, recv, rows):
        total = own
        for d in range(3):
            total = total + recv[d, rows, :].astype(F32)
        return total

    for copy in a1:
        copy.wait_recv()
    q_nope_sum = added(q_nope_part, a1_recv, slice(0, 64))
    q_rope_sum = added(q_rope_part, a1_recv, slice(64, 96))
    a2_send[0:64, :] = q_nope_sum.astype(BF16)
    a2_send[64:96, :] = q_rope_sum.astype(BF16)
    a2 = line(a2_send, a2_recv, a2_ss, a2_rs, z_dev)
    for copy in a2:
        copy.start()
    for copy in a2:
        copy.wait_recv()
    q_nope = added(q_nope_sum, a2_recv, slice(0, 64)).astype(BF16)
    q_rope = added(q_rope_sum, a2_recv, slice(64, 96)).astype(BF16).astype(F32)
    swapped = jnp.where(lane % 64 < 32, pltpu.roll(q_rope, 96, 1), pltpu.roll(q_rope, 32, 1))
    q_rope = q_rope * cosine + swapped * sine
    q_rope = jnp.concatenate([q_rope[:, :64], q_rope[:, 64:]], axis=0)


    loads[7].wait()
    q_lat = dot_nt(q_nope, wk[...])
    pad = jnp.zeros((8, 64), F32)
    for j in range(8):
        block = jnp.concatenate([q_lat[8 * j : 8 * j + 8], q_rope[8 * j : 8 * j + 8], pad], axis=1)
        b_send[j] = block.astype(BF16)

    def b_copy(d):
        to = (tp + d) % 8
        return pltpu.make_async_remote_copy(
            src_ref=b_send.at[to], dst_ref=b_recv.at[tp], send_sem=b_ss, recv_sem=b_rs,
            device_id=(kv, to), device_id_type=MESH,
        )

    def all_of(ref, count, ss, rs):
        part = ref.at[pl.ds(0, count)]
        return pltpu.make_async_remote_copy(
            src_ref=part, dst_ref=part, send_sem=ss, recv_sem=rs, device_id=(kv, twin), device_id_type=MESH
        )

    for d in (4, 5, 3, 2, 6, 7, 1):
        b_copy(d).start()
    lax.fori_loop(1, 16, lat_start, 0)
    b_recv[tp] = b_send[tp]
    for d in (1, 3, 2):
        out_y(d, (y + d) % 4).wait_recv()
    for d in (1, 3, 2):
        out_z(d, z).start()
    out_twin(0, core).start()
    all_of(b_recv, 7, b_ss, b_rs).wait_recv()

    for copy in value_forwards:
        copy.wait_recv()
        copy.start()

    for h in range(8):
        rows = b_recv[h].astype(F32)
        for i in range(5):
            q_tab[i, 8 * h : 8 * h + 8, :] = rows[:, 128 * i : 128 * i + 128]

    def query_of(s):
        return jnp.concatenate([q_tab[i, pl.ds(s, 8, stride=8), :] for i in range(5)], axis=1)

    for copy in cache_loads:
        copy.wait()
    factor = 192.0 ** (-0.5)

    def scores_of(s):
        q = query_of(s).astype(BF16)
        return dot_nt(q[:, :512], cl[s]) + dot(q[:, 512:576], cr[s])

    scores = jnp.concatenate([scores_of(s) for s in range(8)], axis=0) * factor

    all_of(lat_recv, 15, lat_ss, lat_rs).wait_recv()
    lat_sum = lat_recv[0]
    for k in range(1, 16):
        lat_sum = lat_sum + lat_recv[k]
    loads[8].wait()
    lat_raw = lat_sum[:, :512]
    latent = (
        lat_raw * lax.rsqrt(jnp.mean(lat_raw * lat_raw, axis=1, keepdims=True) + EPSILON) * lgain[...]
    ).astype(BF16).astype(F32)
    key_raw = lat_sum[:, 512:576]
    new_seq = kv // 2
    new_row = tp * 8 + new_seq
    key_swapped = jnp.concatenate([key_raw[:, 32:], key_raw[:, :32]], axis=1)
    new_rope = key_raw * cos_tab[pl.ds(new_row, 1), :] + key_swapped * sin_tab[pl.ds(new_row, 1), :]
    new_rope = new_rope.astype(BF16).astype(F32)
    q_new = query_of(new_seq)
    new_score = (
        jnp.sum(q_new[:, :512] * latent, axis=1, keepdims=True)
        + jnp.sum(q_new[:, 512:576] * new_rope, axis=1, keepdims=True)
    ) * factor

    row_seq = iota((64, 1), 0) // 8
    row_length = jnp.concatenate(
        [jnp.broadcast_to(len_tab[pl.ds(tp * 8 + s, 1), 0:1], (8, 1)) for s in range(8)], axis=0
    )
    positions = (kv * 512 + iota((64, 512), 1)).astype(F32)
    visible = positions < row_length
    is_new = jnp.logical_and(row_seq == new_seq, kv % 2 == 0)
    own_new = jnp.where(is_new, jnp.concatenate([new_score] * 8, axis=0), NEGATIVE)
    top = jnp.maximum(jnp.max(jnp.where(visible, scores, NEGATIVE), axis=1, keepdims=True), own_new)
    weights = jnp.where(visible, jnp.exp(scores - top), 0.0)
    new_weight = jnp.where(is_new, jnp.exp(own_new - top), 0.0)
    total = jnp.sum(weights, axis=1, keepdims=True) + new_weight
    some = total > 0.0
    safe = jnp.where(some, total, 1.0)
    lse = jnp.where(some, top + jnp.log(safe), NEGATIVE)
    acc = jnp.concatenate(
        [dot(weights[8 * s : 8 * s + 8].astype(BF16), cl[s]) for s in range(8)], axis=0
    ) + new_weight.astype(BF16).astype(F32) * latent

    def gather_wait(buf, ss, rs):
        for d in range(4):
            slot = (twin + 2 * d) % 8
            gather_copy(buf, ss, rs, 0, slot, twin).wait_recv()

    gather_wait(wv, gv_ss, gv_rs)
    by_head = dot(acc.astype(BF16), jnp.concatenate([wv[h] for h in range(8)], axis=1))
    value = by_head[:, 0:128]
    row_head = iota((64, 128), 0) % 8
    for h in range(1, 8):
        value = jnp.where(row_head == h, by_head[:, 128 * h : 128 * h + 128], value)
    value = value / safe

    def merge(value, lse, others, recv, copies):
        top = lse
        for other in others:
            top = jnp.maximum(top, other)
        own_scale = jnp.exp(lse - top)
        scales = [jnp.exp(other - top) for other in others]
        total = own_scale + scales[0] + scales[1] + scales[2]
        merged_scales = [scale / total for scale in scales]
        merged = value * (own_scale / total)
        for copy in copies:
            copy.wait_recv()
        for d in range(3):
            merged = merged + recv[d].astype(F32) * merged_scales[d]
        return merged, top + jnp.log(total)

    c1_send[...] = value.astype(BF16)
    l_send[...] = to_row(lse, 64)
    l_recv[kv] = l_send[...]

    def l_copy(i, ss, rs):
        to = (z + i // 4) % 4 * 4 + (x + i) % 4
        return pltpu.make_async_remote_copy(
            src_ref=l_send, dst_ref=l_recv.at[kv], send_sem=ss, recv_sem=rs,
            device_id=(to, tp), device_id_type=MESH,
        )

    def l_start(i, c):
        l_copy(i, lo_ss, lo_rs).start()
        return c

    c1 = line(c1_send, c1_recv, c1_ss, c1_rs, x_dev)
    for i in (2, 1, 3):
        l_copy(i, lx_ss, lx_rs).start()
    for copy in (c1[1], c1[0], c1[2]):
        copy.start()
    lax.fori_loop(4, 16, l_start, 0)
    all_of(l_recv, 3, lx_ss, lx_rs).wait_recv()
    others = [to_column(l_recv[z * 4 + (x + 4 - d) % 4], 64) for d in (1, 2, 3)]
    value, lse = merge(value, lse, others, c1_recv, c1)

    for d in (1, 3, 2):
        out_z(d, (z + d) % 4).wait_recv()
        out_twin(d, core).start()

    c2_send[...] = value.astype(BF16)
    c2 = line(c2_send, c2_recv, c2_ss, c2_rs, z_dev)
    for copy in c2:
        copy.start()
    all_of(l_recv, 12, lo_ss, lo_rs).wait_recv()
    others = []
    for d in (1, 2, 3):
        rows = [l_recv[(z + 4 - d) % 4 * 4 + i] for i in range(4)]
        best = jnp.maximum(jnp.maximum(rows[0], rows[1]), jnp.maximum(rows[2], rows[3]))
        mass = jnp.exp(rows[0] - best)
        for i in range(1, 4):
            mass = mass + jnp.exp(rows[i] - best)
        others.append(to_column(best + jnp.log(mass), 64))
    value, lse = merge(value, lse, others, c2_recv, c2)

    for d in range(4):
        out_twin(d, 1 - core).wait_recv()
    o_tab[...] = value
    head_out = jnp.concatenate(
        [o_tab[pl.ds(2 * r + c, 8, stride=8), :] for c in range(2) for r in range(4)], axis=1
    ).astype(BF16)
    mixed_z = dot(head_out, jnp.concatenate([wo[k].reshape(1024, 128) for k in range(4)], axis=1))
    own_mixed = mixed_z[:, 0:128]
    for k in range(1, 4):
        own_mixed = jnp.where(z == k, mixed_z[:, 128 * k : 128 * k + 128], own_mixed)
    m_send[...] = own_mixed
    g_send[...] = to_row(jnp.sum(mixed_z * mixed_z, axis=1, keepdims=True), 8)

    def m_copy(slot, to):
        return pltpu.make_async_remote_copy(
            src_ref=m_send, dst_ref=m_recv.at[slot], send_sem=m_ss, recv_sem=m_rs,
            device_id=(kv, to), device_id_type=MESH,
        )

    place = x * 8 + tp

    def g_copy(slot, to):
        return pltpu.make_async_remote_copy(
            src_ref=g_send, dst_ref=g_recv.at[slot], send_sem=g_ss, recv_sem=g_rs,
            device_id=(z * 4 + to // 8, to % 8), device_id_type=MESH,
        )

    def g_start(i, c):
        g_copy(place, (place + (i + 12) % 31 + 1) % 32).start()
        return c

    lax.fori_loop(0, 31, g_start, 0)
    for d in (4, 5, 3, 2, 6, 7, 1):
        m_copy(tp, (tp + d) % 8).start()
    m_recv[tp] = m_send[...]
    g_recv[place] = g_send[...]
    loads[11].wait()

    for copy in a1 + a2 + c1 + c2 + value_sends + value_forwards:
        copy.wait_send()
    for d in range(4):
        out_twin(d, core).wait_send()
    for d in range(1, 4):
        out_y(d, y).wait_send()
        out_z(d, z).wait_send()
    all_of(b_recv, 7, b_ss, b_rs).wait_send()
    all_of(lat_recv, 15, lat_ss, lat_rs).wait_send()
    all_of(l_recv, 3, lx_ss, lx_rs).wait_send()
    all_of(l_recv, 12, lo_ss, lo_rs).wait_send()

    all_of(m_recv, 7, m_ss, m_rs).wait_recv()
    all_of(g_recv, 31, g_ss, g_rs).wait_recv()
    mixed = m_recv[...].reshape(64, 128)
    squares = []
    for j in range(8):
        total = g_recv[j]
        for k in range(1, 4):
            total = total + g_recv[8 * k + j]
        squares.append(jnp.broadcast_to(total, (8, 128)))
    inverse = lax.rsqrt(jnp.concatenate(squares, axis=0) / 2048.0 + EPSILON)
    picked = iota((64, 128), 0) % 8 == iota((64, 128), 1)
    inverse = jnp.sum(jnp.where(picked, inverse, 0.0), axis=1, keepdims=True)
    out_ref[...] = (mixed * inverse * ogain[...]).astype(BF16)

    all_of(m_recv, 7, m_ss, m_rs).wait_send()
    all_of(g_recv, 31, g_ss, g_rs).wait_send()


def on_device(
    tokens, token_gain, w_query, w_down_kv, w_rope_key, latent_gain, w_key_up, w_value_up, w_out, out_gain,
    cache_latent, cache_rope, lengths,
):
    freq = 1.0 / 10000.0 ** (np.arange(0, 64, 2, dtype=np.float32) / np.float32(64.0))
    freq = jnp.asarray(np.tile(freq.astype(np.float32), 4)[None, :])
    operands = (
        tokens, token_gain.reshape(1, 128), w_query.T, w_down_kv, w_rope_key.T, latent_gain.reshape(1, 512),
        w_key_up.reshape(512, 128), w_value_up.reshape(512, 128), w_out, out_gain.reshape(1, 128),
        cache_latent, cache_rope.transpose(0, 2, 1), lengths.reshape(1, 64), freq,
    )
    shapes = [(a.shape, a.dtype) for a in operands]
    shapes[7] = ((8, 512, 128), BF16)
    shapes[8] = ((4, 2, 4, 128, 128), BF16)
    local = [pltpu.VMEM(*a) for a in shapes]
    operands = tuple(pltpu.with_memory_space_constraint(v, pltpu.HBM) for v in operands)
    dma = pltpu.SemaphoreType.DMA
    scratch = local + [
        pltpu.VMEM((64, 128), F32), pltpu.VMEM((64, 64), F32), pltpu.VMEM((64, 64), F32),
        pltpu.VMEM((96, 128), BF16), pltpu.VMEM((3, 96, 128), BF16),
        pltpu.VMEM((96, 128), BF16), pltpu.VMEM((3, 96, 128), BF16),
        pltpu.VMEM((64, 640), F32), pltpu.VMEM((8, 1, 640), F32), pltpu.VMEM((16, 1, 640), F32),
        pltpu.VMEM((8, 8, 640), BF16), pltpu.VMEM((8, 8, 640), BF16),
        pltpu.VMEM((5, 64, 128), F32), pltpu.VMEM((64, 128), F32),
        pltpu.VMEM((64, 128), BF16), pltpu.VMEM((3, 64, 128), BF16),
        pltpu.VMEM((64, 128), BF16), pltpu.VMEM((3, 64, 128), BF16),
        pltpu.VMEM((1, 128), F32), pltpu.VMEM((16, 1, 128), F32),
        pltpu.VMEM((8, 128), F32), pltpu.VMEM((8, 8, 128), F32),
        pltpu.VMEM((1, 128), F32), pltpu.VMEM((32, 1, 128), F32),
        dma((12,)), dma((16,)),
        dma((3,)), dma((3,)), dma((3,)), dma((3,)), dma, dma,
        dma, dma, dma((8,)), dma((8,)),
        dma((4,)), dma((4,)), dma((4,)), dma((4,)), dma((4,)), dma((4,)),
        dma((3,)), dma((3,)), dma((3,)), dma((3,)), dma, dma, dma, dma,
        dma, dma, dma, dma,
    ]
    return pl.pallas_call(
        kernel,
        out_shape=pltpu.VMEM((64, 128), BF16),
        in_specs=[pl.BlockSpec(memory_space=pltpu.HBM)] * len(operands),
        out_specs=pl.BlockSpec(memory_space=pltpu.VMEM),
        scratch_shapes=scratch,
        compiler_params=pltpu.CompilerParams(
            collective_id=0, has_side_effects=True, vmem_limit_bytes=48 * 1024 * 1024
        ),
    )(*operands)


def solution(mesh):
    return jax.shard_map(
        on_device,
        mesh=mesh,
        in_specs=(
            P(None, "kv"), P("kv"), P("kv", "tp"), P("kv", None), P("kv", None), P(),
            P("tp", None, None), P("tp", None, None), P("tp", "kv"), P("kv"),
            P("tp", "kv", None), P("tp", "kv", None), P(),
        ),
        out_specs=P(None, "kv"),
        check_vma=False,
    )
```

```python
import functools

import jax
import jax.numpy as jnp
import numpy as np
from jax import lax
from jax.experimental import pallas as pl
from jax.experimental.pallas import tpu as pltpu
from jax.sharding import PartitionSpec as P

MESH = pl.DeviceIdType.MESH
EPSILON = 1e-06
NEGATIVE = -1e30
BF16 = jnp.bfloat16
F32 = jnp.float32


def dot(a, b):
    return jnp.dot(a, b, preferred_element_type=F32)


def dot_nt(a, b):
    return lax.dot_general(a, b, (((1,), (1,)), ((), ())), preferred_element_type=F32)


def iota(shape, axis):
    return lax.broadcasted_iota(jnp.int32, shape, axis)


def to_column(row, rows):
    picked = iota((rows, rows), 0) == iota((rows, rows), 1)
    return jnp.sum(jnp.where(picked, row[:, :rows], 0.0), axis=1, keepdims=True)


def to_row(column, rows):
    picked = iota((rows, 128), 0) == iota((rows, 128), 1)
    return jnp.sum(jnp.where(picked, column, 0.0), axis=0, keepdims=True)


def kernel(
    tok_h, tgain_h, wq_h, wd_h, wr_h, lgain_h, wk_h, wv_h, wo_h, ogain_h, cl_h, cr_h, len_h, freq_h,
    out_ref,
    tok, tgain, wq, wd, wr, lgain, wk, wv, wo, ogain, cl, cr, lens, freq,
    len_tab, cos_tab, sin_tab,
    a1_send, a1_recv, a2_send, a2_recv,
    lat_all, lat_send, lat_recv,
    b_send, b_recv, q_tab, o_tab,
    c1_send, c1_recv, c2_send, c2_recv, l_send, l_recv,
    m_send, m_recv, g_send, g_recv,
    load_sem, cache_sem,
    a1_ss, a1_rs, a2_ss, a2_rs, lat_ss, lat_rs, b_ss, b_rs, gv_ss, gv_rs, oy_ss, oy_rs, oz_ss, oz_rs, ot_ss, ot_rs,
    c1_ss, c1_rs, c2_ss, c2_rs, lx_ss, lx_rs, lo_ss, lo_rs, m_ss, m_rs, g_ss, g_rs,
):
    kv = lax.axis_index("kv")
    tp = lax.axis_index("tp")
    z = kv // 4
    x = kv % 4
    y = tp // 2
    core = tp % 2

    pairs = [
        (tok_h, tok), (tgain_h, tgain), (wq_h, wq), (len_h, lens), (freq_h, freq), (wd_h, wd), (wr_h, wr),
        (wk_h, wk), (lgain_h, lgain), (wv_h, wv.at[tp]), (wo_h, wo.at[z, core, y]), (ogain_h, ogain),
    ]
    loads = [pltpu.make_async_copy(s, d, load_sem.at[i]) for i, (s, d) in enumerate(pairs)]
    cache_loads = []
    for s in range(8):
        cache_loads.append(pltpu.make_async_copy(cl_h.at[s], cl.at[s], cache_sem.at[s]))
        cache_loads.append(pltpu.make_async_copy(cr_h.at[s], cr.at[s], cache_sem.at[8 + s]))
    for copy in loads[:3]:
        copy.start()
    barrier = pltpu.get_barrier_semaphore()

    def greet_line(d, c):
        pl.semaphore_signal(barrier, inc=1, device_id=(z * 4 + (x + d) % 4, tp), device_id_type=MESH)
        pl.semaphore_signal(barrier, inc=1, device_id=((z + d) % 4 * 4 + x, tp), device_id_type=MESH)
        return c

    def greet_tp(d, c):
        pl.semaphore_signal(barrier, inc=1, device_id=(kv, (tp + d) % 8), device_id_type=MESH)
        return c

    lax.fori_loop(1, 4, greet_line, 0)
    lax.fori_loop(1, 8, greet_tp, 0)


    for i in range(3):
        loads[i].wait()
    scaled = (tok[...].astype(F32) * tgain[...]).astype(BF16)
    q_part = dot_nt(scaled, wq[...])
    rope_part = q_part[:, 128:192]
    q_nope_part = q_part[:, :128]
    q_rope_part = jnp.concatenate([rope_part[:32], rope_part[32:]], axis=1)
    a1_send[0:64, :] = q_nope_part.astype(BF16)
    a1_send[64:96, :] = q_rope_part.astype(BF16)

    for copy in loads[3:] + cache_loads:
        copy.start()
    pl.semaphore_wait(barrier, 13)

    def x_dev(d):
        return (z * 4 + (x + d) % 4, tp)

    def z_dev(d):
        return (((z + d) % 4) * 4 + x, tp)

    def line(src, dst, ss, rs, dev):
        return [
            pltpu.make_async_remote_copy(
                src_ref=src, dst_ref=dst.at[d - 1], send_sem=ss.at[d - 1], recv_sem=rs.at[d - 1],
                device_id=dev(d), device_id_type=MESH,
            )
            for d in (1, 2, 3)
        ]

    a1 = line(a1_send, a1_recv, a1_ss, a1_rs, x_dev)
    for copy in a1:
        copy.start()

    twin = tp + 1 - 2 * core

    def gather_copy(buf, ss, rs, i, slot, to):
        return pltpu.make_async_remote_copy(
            src_ref=buf.at[slot], dst_ref=buf.at[slot], send_sem=ss.at[i], recv_sem=rs.at[slot],
            device_id=(kv, to), device_id_type=MESH,
        )

    def gather_first(buf, ss, rs):
        copies = [gather_copy(buf, ss, rs, i, tp, (tp + 2 * d) % 8) for i, d in enumerate((1, 3, 2))]
        return copies + [gather_copy(buf, ss, rs, 3, tp, twin)]

    def gather_forward(buf, ss, rs):
        slots = [(tp + 2 * d) % 8 for d in (1, 3, 2)]
        return [gather_copy(buf, ss, rs, 4 + i, slot, twin) for i, slot in enumerate(slots)]

    loads[9].wait()
    loads[10].wait()
    value_sends = gather_first(wv, gv_ss, gv_rs)
    value_forwards = gather_forward(wv, gv_ss, gv_rs)

    def out_y(d, at):
        return pltpu.make_async_remote_copy(
            src_ref=wo.at[z, core, y], dst_ref=wo.at[z, core, at], send_sem=oy_ss.at[d], recv_sem=oy_rs.at[at],
            device_id=(kv, (tp + 2 * d) % 8), device_id_type=MESH,
        )

    def out_z(d, at):
        return pltpu.make_async_remote_copy(
            src_ref=wo.at[z, core], dst_ref=wo.at[at, core], send_sem=oz_ss.at[d], recv_sem=oz_rs.at[at],
            device_id=((z + d) % 4 * 4 + x, tp), device_id_type=MESH,
        )

    def out_twin(d, half):
        at = (z + d) % 4
        return pltpu.make_async_remote_copy(
            src_ref=wo.at[at, core], dst_ref=wo.at[at, half], send_sem=ot_ss.at[d], recv_sem=ot_rs.at[at],
            device_id=(kv, twin), device_id_type=MESH,
        )

    for d in (1, 3, 2):
        out_y(d, y).start()
    for copy in value_sends:
        copy.start()

    for i in range(3, 7):
        loads[i].wait()
    lat_all[:, 0:512] = dot(scaled, wd[...])
    lat_all[:, 512:576] = dot_nt(scaled, wr[...])
    lat_all[:, 576:640] = jnp.zeros((64, 64), F32)
    mine = lat_all[pl.ds(pl.multiple_of(tp * 8, 8), 8), :]
    for r in range(8):
        lat_send[r] = mine[r : r + 1, :]
    lat_recv[kv] = lat_send[kv // 2]

    def lat_copy(dz, dx):
        at_z = lax.rem(z + dz, 4)
        at_x = lax.rem(x + dx, 4)
        return pltpu.make_async_remote_copy(
            src_ref=lat_send.at[at_z * 2 + at_x // 2], dst_ref=lat_recv.at[kv], send_sem=lat_ss, recv_sem=lat_rs,
            device_id=(at_z * 4 + at_x, tp), device_id_type=MESH,
        )

    len_col = to_column(lens[...].astype(F32), 64)
    len_tab[...] = jnp.broadcast_to(len_col, (64, 128))
    lane = iota((32, 128), 1)
    packed_len = jnp.where(lane < 64, len_col[:32], len_col[32:])
    angle = packed_len * freq[...]
    cosine = jnp.cos(angle)
    sine = jnp.sin(angle)
    sine = jnp.where(lane % 64 < 32, -sine, sine)
    cos_tab[0:32, :] = cosine[:, :64]
    cos_tab[32:64, :] = cosine[:, 64:]
    sin_tab[0:32, :] = sine[:, :64]
    sin_tab[32:64, :] = sine[:, 64:]

    def added(own, recv, rows):
        total = own
        for d in range(3):
            total = total + recv[d, rows, :].astype(F32)
        return total

    for copy in a1:
        copy.wait_recv()
    q_nope_sum = added(q_nope_part, a1_recv, slice(0, 64))
    q_rope_sum = added(q_rope_part, a1_recv, slice(64, 96))
    a2_send[0:64, :] = q_nope_sum.astype(BF16)
    a2_send[64:96, :] = q_rope_sum.astype(BF16)
    a2 = line(a2_send, a2_recv, a2_ss, a2_rs, z_dev)
    for copy in a2:
        copy.start()
    for dz in (2, 1, 3, 0):
        for dx in (2, 1, 3, 0):
            if (dz, dx) != (0, 0):
                lat_copy(dz, dx).start()
    for copy in a2:
        copy.wait_recv()
    q_nope = added(q_nope_sum, a2_recv, slice(0, 64)).astype(BF16)
    q_rope = added(q_rope_sum, a2_recv, slice(64, 96)).astype(BF16).astype(F32)
    swapped = jnp.where(lane % 64 < 32, pltpu.roll(q_rope, 96, 1), pltpu.roll(q_rope, 32, 1))
    q_rope = q_rope * cosine + swapped * sine
    q_rope = jnp.concatenate([q_rope[:, :64], q_rope[:, 64:]], axis=0)


    loads[7].wait()
    q_lat = dot_nt(q_nope, wk[...])
    pad = jnp.zeros((8, 64), F32)
    for j in range(8):
        block = jnp.concatenate([q_lat[8 * j : 8 * j + 8], q_rope[8 * j : 8 * j + 8], pad], axis=1)
        b_send[j] = block.astype(BF16)

    def b_copy(d):
        to = (tp + d) % 8
        return pltpu.make_async_remote_copy(
            src_ref=b_send.at[to], dst_ref=b_recv.at[tp], send_sem=b_ss, recv_sem=b_rs,
            device_id=(kv, to), device_id_type=MESH,
        )

    def all_of(ref, count, ss, rs):
        part = ref.at[pl.ds(0, count)]
        return pltpu.make_async_remote_copy(
            src_ref=part, dst_ref=part, send_sem=ss, recv_sem=rs, device_id=(kv, twin), device_id_type=MESH
        )

    for d in (4, 5, 3, 2, 6, 7, 1):
        b_copy(d).start()
    b_recv[tp] = b_send[tp]
    for d in (1, 3, 2):
        out_y(d, (y + d) % 4).wait_recv()
    for d in (1, 3, 2):
        out_z(d, z).start()
    out_twin(0, core).start()
    all_of(lat_recv, 15, lat_ss, lat_rs).wait_recv()
    lat_sum = lat_recv[0]
    for k in range(1, 16):
        lat_sum = lat_sum + lat_recv[k]
    loads[8].wait()
    lat_raw = lat_sum[:, :512]
    latent = (
        lat_raw * lax.rsqrt(jnp.mean(lat_raw * lat_raw, axis=1, keepdims=True) + EPSILON) * lgain[...]
    ).astype(BF16).astype(F32)
    key_raw = lat_sum[:, 512:576]
    new_seq = kv // 2
    new_row = tp * 8 + new_seq
    key_swapped = jnp.concatenate([key_raw[:, 32:], key_raw[:, :32]], axis=1)
    new_rope = key_raw * cos_tab[pl.ds(new_row, 1), :] + key_swapped * sin_tab[pl.ds(new_row, 1), :]
    new_rope = new_rope.astype(BF16).astype(F32)
    all_of(b_recv, 7, b_ss, b_rs).wait_recv()

    for copy in value_forwards:
        copy.wait_recv()
        copy.start()

    for h in range(8):
        rows = b_recv[h].astype(F32)
        for i in range(5):
            q_tab[i, 8 * h : 8 * h + 8, :] = rows[:, 128 * i : 128 * i + 128]

    def query_of(s):
        return jnp.concatenate([q_tab[i, pl.ds(s, 8, stride=8), :] for i in range(5)], axis=1)

    for copy in cache_loads:
        copy.wait()
    factor = 192.0 ** (-0.5)

    def scores_of(s):
        q = query_of(s).astype(BF16)
        return dot_nt(q[:, :512], cl[s]) + dot(q[:, 512:576], cr[s])

    scores = jnp.concatenate([scores_of(s) for s in range(8)], axis=0) * factor

    q_new = query_of(new_seq)
    new_score = (
        jnp.sum(q_new[:, :512] * latent, axis=1, keepdims=True)
        + jnp.sum(q_new[:, 512:576] * new_rope, axis=1, keepdims=True)
    ) * factor

    row_seq = iota((64, 1), 0) // 8
    row_length = jnp.concatenate(
        [jnp.broadcast_to(len_tab[pl.ds(tp * 8 + s, 1), 0:1], (8, 1)) for s in range(8)], axis=0
    )
    positions = (kv * 512 + iota((64, 512), 1)).astype(F32)
    visible = positions < row_length
    is_new = jnp.logical_and(row_seq == new_seq, kv % 2 == 0)
    own_new = jnp.where(is_new, jnp.concatenate([new_score] * 8, axis=0), NEGATIVE)
    top = jnp.maximum(jnp.max(jnp.where(visible, scores, NEGATIVE), axis=1, keepdims=True), own_new)
    weights = jnp.where(visible, jnp.exp(scores - top), 0.0)
    new_weight = jnp.where(is_new, jnp.exp(own_new - top), 0.0)
    total = jnp.sum(weights, axis=1, keepdims=True) + new_weight
    some = total > 0.0
    safe = jnp.where(some, total, 1.0)
    lse = jnp.where(some, top + jnp.log(safe), NEGATIVE)
    acc = jnp.concatenate(
        [dot(weights[8 * s : 8 * s + 8].astype(BF16), cl[s]) for s in range(8)], axis=0
    ) + new_weight.astype(BF16).astype(F32) * latent

    def gather_wait(buf, ss, rs):
        for d in range(4):
            slot = (twin + 2 * d) % 8
            gather_copy(buf, ss, rs, 0, slot, twin).wait_recv()

    gather_wait(wv, gv_ss, gv_rs)
    by_head = dot(acc.astype(BF16), jnp.concatenate([wv[h] for h in range(8)], axis=1))
    value = by_head[:, 0:128]
    row_head = iota((64, 128), 0) % 8
    for h in range(1, 8):
        value = jnp.where(row_head == h, by_head[:, 128 * h : 128 * h + 128], value)
    value = value / safe

    def merge(value, lse, others, recv, copies):
        top = lse
        for other in others:
            top = jnp.maximum(top, other)
        own_scale = jnp.exp(lse - top)
        scales = [jnp.exp(other - top) for other in others]
        total = own_scale + scales[0] + scales[1] + scales[2]
        merged_scales = [scale / total for scale in scales]
        merged = value * (own_scale / total)
        for copy in copies:
            copy.wait_recv()
        for d in range(3):
            merged = merged + recv[d].astype(F32) * merged_scales[d]
        return merged, top + jnp.log(total)

    c1_send[...] = value.astype(BF16)
    l_send[...] = to_row(lse, 64)
    l_recv[kv] = l_send[...]

    def l_copy(i, ss, rs):
        to = (z + i // 4) % 4 * 4 + (x + i) % 4
        return pltpu.make_async_remote_copy(
            src_ref=l_send, dst_ref=l_recv.at[kv], send_sem=ss, recv_sem=rs,
            device_id=(to, tp), device_id_type=MESH,
        )

    def l_start(i, c):
        l_copy(i, lo_ss, lo_rs).start()
        return c

    c1 = line(c1_send, c1_recv, c1_ss, c1_rs, x_dev)
    for i in (2, 1, 3):
        l_copy(i, lx_ss, lx_rs).start()
    for copy in (c1[1], c1[0], c1[2]):
        copy.start()
    lax.fori_loop(4, 16, l_start, 0)
    all_of(l_recv, 3, lx_ss, lx_rs).wait_recv()
    others = [to_column(l_recv[z * 4 + (x + 4 - d) % 4], 64) for d in (1, 2, 3)]
    value, lse = merge(value, lse, others, c1_recv, c1)

    for d in (1, 3, 2):
        out_z(d, (z + d) % 4).wait_recv()
        out_twin(d, core).start()

    c2_send[...] = value.astype(BF16)
    c2 = line(c2_send, c2_recv, c2_ss, c2_rs, z_dev)
    for copy in c2:
        copy.start()
    all_of(l_recv, 12, lo_ss, lo_rs).wait_recv()
    others = []
    for d in (1, 2, 3):
        rows = [l_recv[(z + 4 - d) % 4 * 4 + i] for i in range(4)]
        best = jnp.maximum(jnp.maximum(rows[0], rows[1]), jnp.maximum(rows[2], rows[3]))
        mass = jnp.exp(rows[0] - best)
        for i in range(1, 4):
            mass = mass + jnp.exp(rows[i] - best)
        others.append(to_column(best + jnp.log(mass), 64))
    value, lse = merge(value, lse, others, c2_recv, c2)

    for d in range(4):
        out_twin(d, 1 - core).wait_recv()
    o_tab[...] = value
    head_out = jnp.concatenate(
        [o_tab[pl.ds(2 * r + c, 8, stride=8), :] for c in range(2) for r in range(4)], axis=1
    ).astype(BF16)
    mixed_z = dot(head_out, jnp.concatenate([wo[k].reshape(1024, 128) for k in range(4)], axis=1))
    own_mixed = mixed_z[:, 0:128]
    for k in range(1, 4):
        own_mixed = jnp.where(z == k, mixed_z[:, 128 * k : 128 * k + 128], own_mixed)
    m_send[...] = own_mixed
    g_send[...] = to_row(jnp.sum(mixed_z * mixed_z, axis=1, keepdims=True), 8)

    def m_copy(slot, to):
        return pltpu.make_async_remote_copy(
            src_ref=m_send, dst_ref=m_recv.at[slot], send_sem=m_ss, recv_sem=m_rs,
            device_id=(kv, to), device_id_type=MESH,
        )

    place = x * 8 + tp

    def g_copy(at_x, at_tp):
        return pltpu.make_async_remote_copy(
            src_ref=g_send, dst_ref=g_recv.at[place], send_sem=g_ss, recv_sem=g_rs,
            device_id=(z * 4 + at_x, at_tp), device_id_type=MESH,
        )

    for dx in (2, 1, 3, 0):
        for dt in (4, 5, 3, 2, 6, 7, 1, 0):
            if (dx, dt) != (0, 0):
                g_copy(lax.rem(x + dx, 4), lax.rem(tp + dt, 8)).start()
    for d in (4, 5, 3, 2, 6, 7, 1):
        m_copy(tp, (tp + d) % 8).start()
    m_recv[tp] = m_send[...]
    g_recv[place] = g_send[...]
    loads[11].wait()

    for copy in a1 + a2 + c1 + c2 + value_sends + value_forwards:
        copy.wait_send()
    for d in range(4):
        out_twin(d, core).wait_send()
    for d in range(1, 4):
        out_y(d, y).wait_send()
        out_z(d, z).wait_send()
    all_of(b_recv, 7, b_ss, b_rs).wait_send()
    all_of(lat_recv, 15, lat_ss, lat_rs).wait_send()
    all_of(l_recv, 3, lx_ss, lx_rs).wait_send()
    all_of(l_recv, 12, lo_ss, lo_rs).wait_send()

    all_of(m_recv, 7, m_ss, m_rs).wait_recv()
    all_of(g_recv, 31, g_ss, g_rs).wait_recv()
    mixed = m_recv[...].reshape(64, 128)
    squares = []
    for j in range(8):
        total = g_recv[j]
        for k in range(1, 4):
            total = total + g_recv[8 * k + j]
        squares.append(jnp.broadcast_to(total, (8, 128)))
    inverse = lax.rsqrt(jnp.concatenate(squares, axis=0) / 2048.0 + EPSILON)
    picked = iota((64, 128), 0) % 8 == iota((64, 128), 1)
    inverse = jnp.sum(jnp.where(picked, inverse, 0.0), axis=1, keepdims=True)
    out_ref[...] = (mixed * inverse * ogain[...]).astype(BF16)

    all_of(m_recv, 7, m_ss, m_rs).wait_send()
    all_of(g_recv, 31, g_ss, g_rs).wait_send()


def on_device(
    tokens, token_gain, w_query, w_down_kv, w_rope_key, latent_gain, w_key_up, w_value_up, w_out, out_gain,
    cache_latent, cache_rope, lengths,
):
    freq = 1.0 / 10000.0 ** (np.arange(0, 64, 2, dtype=np.float32) / np.float32(64.0))
    freq = jnp.asarray(np.tile(freq.astype(np.float32), 4)[None, :])
    operands = (
        tokens, token_gain.reshape(1, 128), w_query.T, w_down_kv, w_rope_key.T, latent_gain.reshape(1, 512),
        w_key_up.reshape(512, 128), w_value_up.reshape(512, 128), w_out, out_gain.reshape(1, 128),
        cache_latent, cache_rope.transpose(0, 2, 1), lengths.reshape(1, 64), freq,
    )
    shapes = [(a.shape, a.dtype) for a in operands]
    shapes[7] = ((8, 512, 128), BF16)
    shapes[8] = ((4, 2, 4, 128, 128), BF16)
    local = [pltpu.VMEM(*a) for a in shapes]
    operands = tuple(pltpu.with_memory_space_constraint(v, pltpu.HBM) for v in operands)
    dma = pltpu.SemaphoreType.DMA
    scratch = local + [
        pltpu.VMEM((64, 128), F32), pltpu.VMEM((64, 64), F32), pltpu.VMEM((64, 64), F32),
        pltpu.VMEM((96, 128), BF16), pltpu.VMEM((3, 96, 128), BF16),
        pltpu.VMEM((96, 128), BF16), pltpu.VMEM((3, 96, 128), BF16),
        pltpu.VMEM((64, 640), F32), pltpu.VMEM((8, 1, 640), F32), pltpu.VMEM((16, 1, 640), F32),
        pltpu.VMEM((8, 8, 640), BF16), pltpu.VMEM((8, 8, 640), BF16),
        pltpu.VMEM((5, 64, 128), F32), pltpu.VMEM((64, 128), F32),
        pltpu.VMEM((64, 128), BF16), pltpu.VMEM((3, 64, 128), BF16),
        pltpu.VMEM((64, 128), BF16), pltpu.VMEM((3, 64, 128), BF16),
        pltpu.VMEM((1, 128), F32), pltpu.VMEM((16, 1, 128), F32),
        pltpu.VMEM((8, 128), F32), pltpu.VMEM((8, 8, 128), F32),
        pltpu.VMEM((1, 128), F32), pltpu.VMEM((32, 1, 128), F32),
        dma((12,)), dma((16,)),
        dma((3,)), dma((3,)), dma((3,)), dma((3,)), dma, dma,
        dma, dma, dma((8,)), dma((8,)),
        dma((4,)), dma((4,)), dma((4,)), dma((4,)), dma((4,)), dma((4,)),
        dma((3,)), dma((3,)), dma((3,)), dma((3,)), dma, dma, dma, dma,
        dma, dma, dma, dma,
    ]
    return pl.pallas_call(
        kernel,
        out_shape=pltpu.VMEM((64, 128), BF16),
        in_specs=[pl.BlockSpec(memory_space=pltpu.HBM)] * len(operands),
        out_specs=pl.BlockSpec(memory_space=pltpu.VMEM),
        scratch_shapes=scratch,
        compiler_params=pltpu.CompilerParams(
            collective_id=0, has_side_effects=True, vmem_limit_bytes=48 * 1024 * 1024
        ),
    )(*operands)


def solution(mesh):
    return jax.shard_map(
        on_device,
        mesh=mesh,
        in_specs=(
            P(None, "kv"), P("kv"), P("kv", "tp"), P("kv", None), P("kv", None), P(),
            P("tp", None, None), P("tp", None, None), P("tp", "kv"), P("kv"),
            P("tp", "kv", None), P("tp", "kv", None), P(),
        ),
        out_specs=P(None, "kv"),
        check_vma=False,
    )
```

```python
import functools

import jax
import jax.numpy as jnp
import numpy as np
from jax import lax
from jax.experimental import pallas as pl
from jax.experimental.pallas import tpu as pltpu
from jax.sharding import PartitionSpec as P

MESH = pl.DeviceIdType.MESH
EPSILON = 1e-06
NEGATIVE = -1e30
BF16 = jnp.bfloat16
F32 = jnp.float32


def dot(a, b):
    return jnp.dot(a, b, preferred_element_type=F32)


def dot_nt(a, b):
    return lax.dot_general(a, b, (((1,), (1,)), ((), ())), preferred_element_type=F32)


def iota(shape, axis):
    return lax.broadcasted_iota(jnp.int32, shape, axis)


def to_column(row, rows):
    picked = iota((rows, rows), 0) == iota((rows, rows), 1)
    return jnp.sum(jnp.where(picked, row[:, :rows], 0.0), axis=1, keepdims=True)


def to_row(column, rows):
    picked = iota((rows, 128), 0) == iota((rows, 128), 1)
    return jnp.sum(jnp.where(picked, column, 0.0), axis=0, keepdims=True)


def kernel(
    tok_h, tgain_h, wq_h, wd_h, wr_h, lgain_h, wk_h, wv_h, wo_h, ogain_h, cl_h, cr_h, len_h, freq_h,
    out_ref,
    tok, tgain, wq, wd, wr, lgain, wk, wv, wo, ogain, cl, cr, lens, freq,
    len_tab, cos_tab, sin_tab,
    a1_send, a1_recv, a2_send, a2_recv,
    lat_all, lat_send, lat_recv,
    b_send, b_recv, q_tab, o_tab,
    c1_send, c1_recv, c2_send, c2_recv, l_send, l_recv,
    m_send, m_recv, g_send, g_recv,
    load_sem, cache_sem,
    a1_ss, a1_rs, a2_ss, a2_rs, lat_ss, lat_rs, b_ss, b_rs, gv_ss, gv_rs, oy_ss, oy_rs, oz_ss, oz_rs, ot_ss, ot_rs,
    c1_ss, c1_rs, c2_ss, c2_rs, lx_ss, lx_rs, lo_ss, lo_rs, m_ss, m_rs, g_ss, g_rs,
):
    kv = lax.axis_index("kv")
    tp = lax.axis_index("tp")
    z = kv // 4
    x = kv % 4
    y = tp // 2
    core = tp % 2

    pairs = [
        (tok_h, tok), (tgain_h, tgain), (wq_h, wq), (len_h, lens), (freq_h, freq), (wd_h, wd), (wr_h, wr),
        (wk_h, wk), (lgain_h, lgain), (wv_h, wv.at[tp]), (wo_h, wo.at[z, core, y]), (ogain_h, ogain),
    ]
    loads = [pltpu.make_async_copy(s, d, load_sem.at[i]) for i, (s, d) in enumerate(pairs)]
    cache_loads = []
    for s in range(8):
        cache_loads.append(pltpu.make_async_copy(cl_h.at[s], cl.at[s], cache_sem.at[s]))
        cache_loads.append(pltpu.make_async_copy(cr_h.at[s], cr.at[s], cache_sem.at[8 + s]))
    for copy in loads[:3]:
        copy.start()
    barrier = pltpu.get_barrier_semaphore()

    def greet(to_kv, to_tp):
        pl.semaphore_signal(barrier, inc=1, device_id=(to_kv, to_tp), device_id_type=MESH)

    for d in (2, 1, 3):
        greet(z * 4 + lax.rem(x + d, 4), tp)
    for d in (2, 1, 3):
        greet(lax.rem(z + d, 4) * 4 + x, tp)
    for d in (4, 5, 3, 2, 6, 7, 1):
        greet(kv, lax.rem(tp + d, 8))

    for i in range(3):
        loads[i].wait()
    scaled = (tok[...].astype(F32) * tgain[...]).astype(BF16)
    q_part = dot_nt(scaled, wq[...])
    rope_part = q_part[:, 128:192]
    q_nope_part = q_part[:, :128]
    q_rope_part = jnp.concatenate([rope_part[:32], rope_part[32:]], axis=1)
    a1_send[0:64, :] = q_nope_part.astype(BF16)
    a1_send[64:96, :] = q_rope_part.astype(BF16)

    for copy in loads[3:] + cache_loads:
        copy.start()
    pl.semaphore_wait(barrier, 13)

    def x_dev(d):
        return (z * 4 + (x + d) % 4, tp)

    def z_dev(d):
        return (((z + d) % 4) * 4 + x, tp)

    def line(src, dst, ss, rs, first, second):
        half = src.shape[0] // 2
        copies = []
        for d in (2, 1, 3):
            for k, dev in enumerate((first, second)):
                rows = pl.ds(k * half, half)
                copies.append(
                    pltpu.make_async_remote_copy(
                        src_ref=src.at[rows], dst_ref=dst.at[d - 1, rows],
                        send_sem=ss.at[3 * k + d - 1], recv_sem=rs.at[3 * k + d - 1],
                        device_id=dev(d), device_id_type=MESH,
                    )
                )
        return copies

    def line1(src, dst, ss, rs, dev):
        return [
            pltpu.make_async_remote_copy(
                src_ref=src, dst_ref=dst.at[d - 1], send_sem=ss.at[d - 1], recv_sem=rs.at[d - 1],
                device_id=dev(d), device_id_type=MESH,
            )
            for d in (1, 2, 3)
        ]

    a1 = line(a1_send, a1_recv, a1_ss, a1_rs, x_dev, z_dev)
    for copy in a1:
        copy.start()

    twin = tp + 1 - 2 * core

    def gather_copy(buf, ss, rs, i, slot, to):
        return pltpu.make_async_remote_copy(
            src_ref=buf.at[slot], dst_ref=buf.at[slot], send_sem=ss.at[i], recv_sem=rs.at[slot],
            device_id=(kv, to), device_id_type=MESH,
        )

    def gather_first(buf, ss, rs):
        copies = [gather_copy(buf, ss, rs, i, tp, (tp + 2 * d) % 8) for i, d in enumerate((1, 3, 2))]
        return copies + [gather_copy(buf, ss, rs, 3, tp, twin)]

    def gather_forward(buf, ss, rs):
        slots = [(tp + 2 * d) % 8 for d in (1, 3, 2)]
        return [gather_copy(buf, ss, rs, 4 + i, slot, twin) for i, slot in enumerate(slots)]

    loads[9].wait()
    loads[10].wait()
    value_sends = gather_first(wv, gv_ss, gv_rs)
    value_forwards = gather_forward(wv, gv_ss, gv_rs)

    def out_y(d, at):
        return pltpu.make_async_remote_copy(
            src_ref=wo.at[z, core, y], dst_ref=wo.at[z, core, at], send_sem=oy_ss.at[d], recv_sem=oy_rs.at[at],
            device_id=(kv, (tp + 2 * d) % 8), device_id_type=MESH,
        )

    def out_z(d, at):
        return pltpu.make_async_remote_copy(
            src_ref=wo.at[z, core], dst_ref=wo.at[at, core], send_sem=oz_ss.at[d], recv_sem=oz_rs.at[at],
            device_id=((z + d) % 4 * 4 + x, tp), device_id_type=MESH,
        )

    def out_twin(d, half):
        at = (z + d) % 4
        return pltpu.make_async_remote_copy(
            src_ref=wo.at[at, core], dst_ref=wo.at[at, half], send_sem=ot_ss.at[d], recv_sem=ot_rs.at[at],
            device_id=(kv, twin), device_id_type=MESH,
        )

    for d in (1, 3, 2):
        out_y(d, y).start()
    for copy in value_sends:
        copy.start()

    for i in range(3, 7):
        loads[i].wait()
    lat_all[:, 0:512] = dot(scaled, wd[...])
    lat_all[:, 512:576] = dot_nt(scaled, wr[...])
    lat_all[:, 576:640] = jnp.zeros((64, 64), F32)
    mine = lat_all[pl.ds(pl.multiple_of(tp * 8, 8), 8), :]
    for r in range(8):
        lat_send[r] = mine[r : r + 1, :]
    lat_recv[kv] = lat_send[kv // 2]

    def lat_copy(dz, dx):
        at_z = lax.rem(z + dz, 4)
        at_x = lax.rem(x + dx, 4)
        return pltpu.make_async_remote_copy(
            src_ref=lat_send.at[at_z * 2 + at_x // 2], dst_ref=lat_recv.at[kv], send_sem=lat_ss, recv_sem=lat_rs,
            device_id=(at_z * 4 + at_x, tp), device_id_type=MESH,
        )

    len_col = to_column(lens[...].astype(F32), 64)
    len_tab[...] = jnp.broadcast_to(len_col, (64, 128))
    lane = iota((32, 128), 1)
    packed_len = jnp.where(lane < 64, len_col[:32], len_col[32:])
    angle = packed_len * freq[...]
    cosine = jnp.cos(angle)
    sine = jnp.sin(angle)
    sine = jnp.where(lane % 64 < 32, -sine, sine)
    cos_tab[0:32, :] = cosine[:, :64]
    cos_tab[32:64, :] = cosine[:, 64:]
    sin_tab[0:32, :] = sine[:, :64]
    sin_tab[32:64, :] = sine[:, 64:]

    def added(own, recv, rows):
        total = own
        for d in range(3):
            total = total + recv[d, rows, :].astype(F32)
        return total

    for copy in a1:
        copy.wait_recv()
    q_nope_sum = added(q_nope_part, a1_recv, slice(0, 64))
    q_rope_sum = added(q_rope_part, a1_recv, slice(64, 96))
    a2_send[0:64, :] = q_nope_sum.astype(BF16)
    a2_send[64:96, :] = q_rope_sum.astype(BF16)
    a2 = line(a2_send, a2_recv, a2_ss, a2_rs, z_dev, x_dev)
    for copy in a2:
        copy.start()
    for dz in (2, 1, 3, 0):
        for dx in (2, 1, 3, 0):
            if (dz, dx) != (0, 0):
                lat_copy(dz, dx).start()
    for copy in a2:
        copy.wait_recv()
    q_nope = added(q_nope_sum, a2_recv, slice(0, 64)).astype(BF16)
    q_rope = added(q_rope_sum, a2_recv, slice(64, 96)).astype(BF16).astype(F32)
    swapped = jnp.where(lane % 64 < 32, pltpu.roll(q_rope, 96, 1), pltpu.roll(q_rope, 32, 1))
    q_rope = q_rope * cosine + swapped * sine
    q_rope = jnp.concatenate([q_rope[:, :64], q_rope[:, 64:]], axis=0)


    loads[7].wait()
    q_lat = dot_nt(q_nope, wk[...])
    pad = jnp.zeros((8, 64), F32)
    for j in range(8):
        block = jnp.concatenate([q_lat[8 * j : 8 * j + 8], q_rope[8 * j : 8 * j + 8], pad], axis=1)
        b_send[j] = block.astype(BF16)

    def b_copy(d):
        to = (tp + d) % 8
        return pltpu.make_async_remote_copy(
            src_ref=b_send.at[to], dst_ref=b_recv.at[tp], send_sem=b_ss, recv_sem=b_rs,
            device_id=(kv, to), device_id_type=MESH,
        )

    def all_of(ref, count, ss, rs):
        part = ref.at[pl.ds(0, count)]
        return pltpu.make_async_remote_copy(
            src_ref=part, dst_ref=part, send_sem=ss, recv_sem=rs, device_id=(kv, twin), device_id_type=MESH
        )

    for d in (4, 5, 3, 2, 6, 7, 1):
        b_copy(d).start()
    b_recv[tp] = b_send[tp]
    for d in (1, 3, 2):
        out_y(d, (y + d) % 4).wait_recv()
    for d in (1, 3, 2):
        out_z(d, z).start()
    out_twin(0, core).start()
    all_of(lat_recv, 15, lat_ss, lat_rs).wait_recv()
    lat_sum = lat_recv[0]
    for k in range(1, 16):
        lat_sum = lat_sum + lat_recv[k]
    loads[8].wait()
    lat_raw = lat_sum[:, :512]
    latent = (
        lat_raw * lax.rsqrt(jnp.mean(lat_raw * lat_raw, axis=1, keepdims=True) + EPSILON) * lgain[...]
    ).astype(BF16).astype(F32)
    key_raw = lat_sum[:, 512:576]
    new_seq = kv // 2
    new_row = tp * 8 + new_seq
    key_swapped = jnp.concatenate([key_raw[:, 32:], key_raw[:, :32]], axis=1)
    new_rope = key_raw * cos_tab[pl.ds(new_row, 1), :] + key_swapped * sin_tab[pl.ds(new_row, 1), :]
    new_rope = new_rope.astype(BF16).astype(F32)
    all_of(b_recv, 7, b_ss, b_rs).wait_recv()

    for copy in value_forwards:
        copy.wait_recv()
        copy.start()

    for h in range(8):
        rows = b_recv[h].astype(F32)
        for i in range(5):
            q_tab[i, 8 * h : 8 * h + 8, :] = rows[:, 128 * i : 128 * i + 128]

    def query_of(s):
        return jnp.concatenate([q_tab[i, pl.ds(s, 8, stride=8), :] for i in range(5)], axis=1)

    for copy in cache_loads:
        copy.wait()
    factor = 192.0 ** (-0.5)

    def scores_of(s):
        q = query_of(s).astype(BF16)
        return dot_nt(q[:, :512], cl[s]) + dot(q[:, 512:576], cr[s])

    scores = jnp.concatenate([scores_of(s) for s in range(8)], axis=0) * factor

    q_new = query_of(new_seq)
    new_score = (
        jnp.sum(q_new[:, :512] * latent, axis=1, keepdims=True)
        + jnp.sum(q_new[:, 512:576] * new_rope, axis=1, keepdims=True)
    ) * factor

    row_seq = iota((64, 1), 0) // 8
    row_length = jnp.concatenate(
        [jnp.broadcast_to(len_tab[pl.ds(tp * 8 + s, 1), 0:1], (8, 1)) for s in range(8)], axis=0
    )
    positions = (kv * 512 + iota((64, 512), 1)).astype(F32)
    visible = positions < row_length
    is_new = jnp.logical_and(row_seq == new_seq, kv % 2 == 0)
    own_new = jnp.where(is_new, jnp.concatenate([new_score] * 8, axis=0), NEGATIVE)
    top = jnp.maximum(jnp.max(jnp.where(visible, scores, NEGATIVE), axis=1, keepdims=True), own_new)
    weights = jnp.where(visible, jnp.exp(scores - top), 0.0)
    new_weight = jnp.where(is_new, jnp.exp(own_new - top), 0.0)
    total = jnp.sum(weights, axis=1, keepdims=True) + new_weight
    some = total > 0.0
    safe = jnp.where(some, total, 1.0)
    lse = jnp.where(some, top + jnp.log(safe), NEGATIVE)
    heads = [dot(weights[8 * s : 8 * s + 8].astype(BF16), cl[s]) for s in range(4)]
    def l_copy(dz, dx, ss, rs):
        return pltpu.make_async_remote_copy(
            src_ref=l_send, dst_ref=l_recv.at[kv], send_sem=ss, recv_sem=rs,
            device_id=(lax.rem(z + dz, 4) * 4 + lax.rem(x + dx, 4), tp), device_id_type=MESH,
        )

    l_send[...] = to_row(lse, 64)
    for d in (2, 1, 3):
        l_copy(0, d, lx_ss, lx_rs).start()
    l_recv[kv] = l_send[...]
    heads += [dot(weights[8 * s : 8 * s + 8].astype(BF16), cl[s]) for s in range(4, 8)]
    acc = jnp.concatenate(heads, axis=0) + new_weight.astype(BF16).astype(F32) * latent

    def gather_wait(buf, ss, rs):
        for d in range(4):
            slot = (twin + 2 * d) % 8
            gather_copy(buf, ss, rs, 0, slot, twin).wait_recv()

    gather_wait(wv, gv_ss, gv_rs)
    by_head = dot(acc.astype(BF16), jnp.concatenate([wv[h] for h in range(8)], axis=1))
    value = by_head[:, 0:128]
    row_head = iota((64, 128), 0) % 8
    for h in range(1, 8):
        value = jnp.where(row_head == h, by_head[:, 128 * h : 128 * h + 128], value)
    value = value / safe

    def merge(value, lse, others, recv, copies):
        top = lse
        for other in others:
            top = jnp.maximum(top, other)
        own_scale = jnp.exp(lse - top)
        scales = [jnp.exp(other - top) for other in others]
        total = own_scale + scales[0] + scales[1] + scales[2]
        merged_scales = [scale / total for scale in scales]
        merged = value * (own_scale / total)
        for copy in copies:
            copy.wait_recv()
        for d in range(3):
            merged = merged + recv[d].astype(F32) * merged_scales[d]
        return merged, top + jnp.log(total)

    c1_send[...] = value.astype(BF16)
    c1 = line1(c1_send, c1_recv, c1_ss, c1_rs, x_dev)
    for copy in (c1[1], c1[0], c1[2]):
        copy.start()
    for dz in (2, 1, 3):
        for dx in (2, 1, 3, 0):
            l_copy(dz, dx, lo_ss, lo_rs).start()
    all_of(l_recv, 3, lx_ss, lx_rs).wait_recv()
    others = [to_column(l_recv[z * 4 + (x + 4 - d) % 4], 64) for d in (1, 2, 3)]
    value, lse = merge(value, lse, others, c1_recv, c1)

    for d in (1, 3, 2):
        out_z(d, (z + d) % 4).wait_recv()
        out_twin(d, core).start()

    c2_send[...] = value.astype(BF16)
    c2 = line1(c2_send, c2_recv, c2_ss, c2_rs, z_dev)
    for copy in c2:
        copy.start()
    all_of(l_recv, 12, lo_ss, lo_rs).wait_recv()
    others = []
    for d in (1, 2, 3):
        rows = [l_recv[(z + 4 - d) % 4 * 4 + i] for i in range(4)]
        best = jnp.maximum(jnp.maximum(rows[0], rows[1]), jnp.maximum(rows[2], rows[3]))
        mass = jnp.exp(rows[0] - best)
        for i in range(1, 4):
            mass = mass + jnp.exp(rows[i] - best)
        others.append(to_column(best + jnp.log(mass), 64))
    value, lse = merge(value, lse, others, c2_recv, c2)

    for d in range(4):
        out_twin(d, 1 - core).wait_recv()
    o_tab[...] = value
    head_out = jnp.concatenate(
        [o_tab[pl.ds(2 * r + c, 8, stride=8), :] for c in range(2) for r in range(4)], axis=1
    ).astype(BF16)
    mixed_z = dot(head_out, jnp.concatenate([wo[k].reshape(1024, 128) for k in range(4)], axis=1))
    own_mixed = mixed_z[:, 0:128]
    for k in range(1, 4):
        own_mixed = jnp.where(z == k, mixed_z[:, 128 * k : 128 * k + 128], own_mixed)
    m_send[...] = own_mixed
    g_send[...] = to_row(jnp.sum(mixed_z * mixed_z, axis=1, keepdims=True), 8)

    def m_copy(slot, to):
        return pltpu.make_async_remote_copy(
            src_ref=m_send, dst_ref=m_recv.at[slot], send_sem=m_ss, recv_sem=m_rs,
            device_id=(kv, to), device_id_type=MESH,
        )

    place = x * 8 + tp

    def g_copy(at_x, at_tp):
        return pltpu.make_async_remote_copy(
            src_ref=g_send, dst_ref=g_recv.at[place], send_sem=g_ss, recv_sem=g_rs,
            device_id=(z * 4 + at_x, at_tp), device_id_type=MESH,
        )

    for dx in (2, 1, 3, 0):
        for dt in (4, 5, 3, 2, 6, 7, 1, 0):
            if (dx, dt) != (0, 0):
                g_copy(lax.rem(x + dx, 4), lax.rem(tp + dt, 8)).start()
    for d in (4, 5, 3, 2, 6, 7, 1):
        m_copy(tp, (tp + d) % 8).start()
    m_recv[tp] = m_send[...]
    g_recv[place] = g_send[...]
    loads[11].wait()

    for copy in a1 + a2 + c1 + c2 + value_sends + value_forwards:
        copy.wait_send()
    for d in range(4):
        out_twin(d, core).wait_send()
    for d in range(1, 4):
        out_y(d, y).wait_send()
        out_z(d, z).wait_send()
    all_of(b_recv, 7, b_ss, b_rs).wait_send()
    all_of(lat_recv, 15, lat_ss, lat_rs).wait_send()
    all_of(l_recv, 3, lx_ss, lx_rs).wait_send()
    all_of(l_recv, 12, lo_ss, lo_rs).wait_send()

    all_of(m_recv, 7, m_ss, m_rs).wait_recv()
    all_of(g_recv, 31, g_ss, g_rs).wait_recv()
    mixed = m_recv[...].reshape(64, 128)
    squares = []
    for j in range(8):
        total = g_recv[j]
        for k in range(1, 4):
            total = total + g_recv[8 * k + j]
        squares.append(jnp.broadcast_to(total, (8, 128)))
    inverse = lax.rsqrt(jnp.concatenate(squares, axis=0) / 2048.0 + EPSILON)
    picked = iota((64, 128), 0) % 8 == iota((64, 128), 1)
    inverse = jnp.sum(jnp.where(picked, inverse, 0.0), axis=1, keepdims=True)
    out_ref[...] = (mixed * inverse * ogain[...]).astype(BF16)

    all_of(m_recv, 7, m_ss, m_rs).wait_send()
    all_of(g_recv, 31, g_ss, g_rs).wait_send()


def on_device(
    tokens, token_gain, w_query, w_down_kv, w_rope_key, latent_gain, w_key_up, w_value_up, w_out, out_gain,
    cache_latent, cache_rope, lengths,
):
    freq = 1.0 / 10000.0 ** (np.arange(0, 64, 2, dtype=np.float32) / np.float32(64.0))
    freq = jnp.asarray(np.tile(freq.astype(np.float32), 4)[None, :])
    operands = (
        tokens, token_gain.reshape(1, 128), w_query.T, w_down_kv, w_rope_key.T, latent_gain.reshape(1, 512),
        w_key_up.reshape(512, 128), w_value_up.reshape(512, 128), w_out, out_gain.reshape(1, 128),
        cache_latent, cache_rope.transpose(0, 2, 1), lengths.reshape(1, 64), freq,
    )
    shapes = [(a.shape, a.dtype) for a in operands]
    shapes[7] = ((8, 512, 128), BF16)
    shapes[8] = ((4, 2, 4, 128, 128), BF16)
    local = [pltpu.VMEM(*a) for a in shapes]
    operands = tuple(pltpu.with_memory_space_constraint(v, pltpu.HBM) for v in operands)
    dma = pltpu.SemaphoreType.DMA
    scratch = local + [
        pltpu.VMEM((64, 128), F32), pltpu.VMEM((64, 64), F32), pltpu.VMEM((64, 64), F32),
        pltpu.VMEM((96, 128), BF16), pltpu.VMEM((3, 96, 128), BF16),
        pltpu.VMEM((96, 128), BF16), pltpu.VMEM((3, 96, 128), BF16),
        pltpu.VMEM((64, 640), F32), pltpu.VMEM((8, 1, 640), F32), pltpu.VMEM((16, 1, 640), F32),
        pltpu.VMEM((8, 8, 640), BF16), pltpu.VMEM((8, 8, 640), BF16),
        pltpu.VMEM((5, 64, 128), F32), pltpu.VMEM((64, 128), F32),
        pltpu.VMEM((64, 128), BF16), pltpu.VMEM((3, 64, 128), BF16),
        pltpu.VMEM((64, 128), BF16), pltpu.VMEM((3, 64, 128), BF16),
        pltpu.VMEM((1, 128), F32), pltpu.VMEM((16, 1, 128), F32),
        pltpu.VMEM((8, 128), F32), pltpu.VMEM((8, 8, 128), F32),
        pltpu.VMEM((1, 128), F32), pltpu.VMEM((32, 1, 128), F32),
        dma((12,)), dma((16,)),
        dma((6,)), dma((6,)), dma((6,)), dma((6,)), dma, dma,
        dma, dma, dma((8,)), dma((8,)),
        dma((4,)), dma((4,)), dma((4,)), dma((4,)), dma((4,)), dma((4,)),
        dma((3,)), dma((3,)), dma((3,)), dma((3,)), dma, dma, dma, dma,
        dma, dma, dma, dma,
    ]
    return pl.pallas_call(
        kernel,
        out_shape=pltpu.VMEM((64, 128), BF16),
        in_specs=[pl.BlockSpec(memory_space=pltpu.HBM)] * len(operands),
        out_specs=pl.BlockSpec(memory_space=pltpu.VMEM),
        scratch_shapes=scratch,
        compiler_params=pltpu.CompilerParams(
            collective_id=0, has_side_effects=True, vmem_limit_bytes=48 * 1024 * 1024
        ),
    )(*operands)


def solution(mesh):
    return jax.shard_map(
        on_device,
        mesh=mesh,
        in_specs=(
            P(None, "kv"), P("kv"), P("kv", "tp"), P("kv", None), P("kv", None), P(),
            P("tp", None, None), P("tp", None, None), P("tp", "kv"), P("kv"),
            P("tp", "kv", None), P("tp", "kv", None), P(),
        ),
        out_specs=P(None, "kv"),
        check_vma=False,
    )
```

```python
import functools

import jax
import jax.numpy as jnp
import numpy as np
from jax import lax
from jax.experimental import pallas as pl
from jax.experimental.pallas import tpu as pltpu
from jax.sharding import PartitionSpec as P

MESH = pl.DeviceIdType.MESH
EPSILON = 1e-06
NEGATIVE = -1e30
BF16 = jnp.bfloat16
F32 = jnp.float32


def dot(a, b):
    return jnp.dot(a, b, preferred_element_type=F32)


def dot_nt(a, b):
    return lax.dot_general(a, b, (((1,), (1,)), ((), ())), preferred_element_type=F32)


def iota(shape, axis):
    return lax.broadcasted_iota(jnp.int32, shape, axis)


def to_column(row, rows):
    picked = iota((rows, rows), 0) == iota((rows, rows), 1)
    return jnp.sum(jnp.where(picked, row[:, :rows], 0.0), axis=1, keepdims=True)


def to_row(column, rows):
    picked = iota((rows, 128), 0) == iota((rows, 128), 1)
    return jnp.sum(jnp.where(picked, column, 0.0), axis=0, keepdims=True)


def kernel(
    tok_h, tgain_h, wq_h, wd_h, wr_h, lgain_h, wk_h, wv_h, wo_h, ogain_h, cl_h, cr_h, len_h, freq_h,
    out_ref,
    tok, tgain, wq, wd, wr, lgain, wk, wv, wo, ogain, cl, cr, lens, freq,
    len_tab, cos_tab, sin_tab,
    a1_send, a1_recv, a2_send, a2_recv,
    lat_all, lat_send, lat_recv,
    keys, b_send, b_recv, q_tab, o_tab,
    c1_send, c1_recv, c2_send, c2_recv, l_send, l_recv,
    m_send, m_recv, g_send, g_recv,
    load_sem, cache_sem,
    a1_ss, a1_rs, a2_ss, a2_rs, lat_ss, lat_rs, b_ss, b_rs, gv_ss, gv_rs, oy_ss, oy_rs, oz_ss, oz_rs, ot_ss, ot_rs,
    c1_ss, c1_rs, c2_ss, c2_rs, lx_ss, lx_rs, lo_ss, lo_rs, m_ss, m_rs, g_ss, g_rs,
):
    kv = lax.axis_index("kv")
    tp = lax.axis_index("tp")
    z = kv // 4
    x = kv % 4
    y = tp // 2
    core = tp % 2

    pairs = [
        (tok_h, tok), (tgain_h, tgain), (wq_h, wq), (len_h, lens), (freq_h, freq), (wd_h, wd), (wr_h, wr),
        (wk_h, wk), (lgain_h, lgain), (wv_h, wv.at[tp]), (wo_h, wo.at[z, core, y]), (ogain_h, ogain),
    ]
    loads = [pltpu.make_async_copy(s, d, load_sem.at[i]) for i, (s, d) in enumerate(pairs)]
    cache_loads = []
    for s in range(8):
        cache_loads.append(pltpu.make_async_copy(cl_h.at[s], cl.at[s], cache_sem.at[s]))
        cache_loads.append(pltpu.make_async_copy(cr_h.at[s], cr.at[s], cache_sem.at[8 + s]))
    for copy in loads[:3]:
        copy.start()
    barrier = pltpu.get_barrier_semaphore()

    def greet(to_kv, to_tp):
        pl.semaphore_signal(barrier, inc=1, device_id=(to_kv, to_tp), device_id_type=MESH)

    for d in (2, 1, 3):
        greet(z * 4 + lax.rem(x + d, 4), tp)
    for d in (2, 1, 3):
        greet(lax.rem(z + d, 4) * 4 + x, tp)
    for d in (4, 5, 3, 2, 6, 7, 1):
        greet(kv, lax.rem(tp + d, 8))

    for i in range(3):
        loads[i].wait()
    scaled = (tok[...].astype(F32) * tgain[...]).astype(BF16)
    q_part = dot_nt(scaled, wq[...])
    rope_part = q_part[:, 128:192]
    q_nope_part = q_part[:, :128]
    q_rope_part = jnp.concatenate([rope_part[:32], rope_part[32:]], axis=1)
    a1_send[0:64, :] = q_nope_part.astype(BF16)
    a1_send[64:96, :] = q_rope_part.astype(BF16)

    for copy in loads[3:] + cache_loads:
        copy.start()
    pl.semaphore_wait(barrier, 13)

    def x_dev(d):
        return (z * 4 + (x + d) % 4, tp)

    def z_dev(d):
        return (((z + d) % 4) * 4 + x, tp)

    def line(src, dst, ss, rs, first, second):
        half = src.shape[0] // 2
        copies = []
        for d in (2, 1, 3):
            for k, dev in enumerate((first, second)):
                rows = pl.ds(k * half, half)
                copies.append(
                    pltpu.make_async_remote_copy(
                        src_ref=src.at[rows], dst_ref=dst.at[d - 1, rows],
                        send_sem=ss.at[3 * k + d - 1], recv_sem=rs.at[3 * k + d - 1],
                        device_id=dev(d), device_id_type=MESH,
                    )
                )
        return copies

    def line1(src, dst, ss, rs, dev):
        return [
            pltpu.make_async_remote_copy(
                src_ref=src, dst_ref=dst.at[d - 1], send_sem=ss.at[d - 1], recv_sem=rs.at[d - 1],
                device_id=dev(d), device_id_type=MESH,
            )
            for d in (1, 2, 3)
        ]

    a1 = line(a1_send, a1_recv, a1_ss, a1_rs, x_dev, z_dev)
    for copy in a1:
        copy.start()

    twin = tp + 1 - 2 * core

    def gather_copy(buf, ss, rs, i, slot, to):
        return pltpu.make_async_remote_copy(
            src_ref=buf.at[slot], dst_ref=buf.at[slot], send_sem=ss.at[i], recv_sem=rs.at[slot],
            device_id=(kv, to), device_id_type=MESH,
        )

    def gather_first(buf, ss, rs):
        copies = [gather_copy(buf, ss, rs, i, tp, (tp + 2 * d) % 8) for i, d in enumerate((1, 3, 2))]
        return copies + [gather_copy(buf, ss, rs, 3, tp, twin)]

    def gather_forward(buf, ss, rs):
        slots = [(tp + 2 * d) % 8 for d in (1, 3, 2)]
        return [gather_copy(buf, ss, rs, 4 + i, slot, twin) for i, slot in enumerate(slots)]

    loads[9].wait()
    loads[10].wait()
    value_sends = gather_first(wv, gv_ss, gv_rs)
    value_forwards = gather_forward(wv, gv_ss, gv_rs)

    def out_y(d, at):
        return pltpu.make_async_remote_copy(
            src_ref=wo.at[z, core, y], dst_ref=wo.at[z, core, at], send_sem=oy_ss.at[d], recv_sem=oy_rs.at[at],
            device_id=(kv, (tp + 2 * d) % 8), device_id_type=MESH,
        )

    def out_z(d, at):
        return pltpu.make_async_remote_copy(
            src_ref=wo.at[z, core], dst_ref=wo.at[at, core], send_sem=oz_ss.at[d], recv_sem=oz_rs.at[at],
            device_id=((z + d) % 4 * 4 + x, tp), device_id_type=MESH,
        )

    def out_twin(d, half):
        at = (z + d) % 4
        return pltpu.make_async_remote_copy(
            src_ref=wo.at[at, core], dst_ref=wo.at[at, half], send_sem=ot_ss.at[d], recv_sem=ot_rs.at[at],
            device_id=(kv, twin), device_id_type=MESH,
        )

    for d in (1, 3, 2):
        out_y(d, y).start()
    for copy in value_sends:
        copy.start()

    for i in range(3, 7):
        loads[i].wait()
    lat_all[:, 0:512] = dot(scaled, wd[...])
    lat_all[:, 512:576] = dot_nt(scaled, wr[...])
    lat_all[:, 576:640] = jnp.zeros((64, 64), F32)
    mine = lat_all[pl.ds(pl.multiple_of(tp * 8, 8), 8), :]
    for r in range(8):
        lat_send[r] = mine[r : r + 1, :]
    lat_recv[kv] = lat_send[kv // 2]

    def lat_copy(dz, dx):
        at_z = lax.rem(z + dz, 4)
        at_x = lax.rem(x + dx, 4)
        return pltpu.make_async_remote_copy(
            src_ref=lat_send.at[at_z * 2 + at_x // 2], dst_ref=lat_recv.at[kv], send_sem=lat_ss, recv_sem=lat_rs,
            device_id=(at_z * 4 + at_x, tp), device_id_type=MESH,
        )

    len_col = to_column(lens[...].astype(F32), 64)
    len_tab[...] = jnp.broadcast_to(len_col, (64, 128))
    lane = iota((32, 128), 1)
    packed_len = jnp.where(lane < 64, len_col[:32], len_col[32:])
    angle = packed_len * freq[...]
    cosine = jnp.cos(angle)
    sine = jnp.sin(angle)
    sine = jnp.where(lane % 64 < 32, -sine, sine)
    cos_tab[0:32, :] = cosine[:, :64]
    cos_tab[32:64, :] = cosine[:, 64:]
    sin_tab[0:32, :] = sine[:, :64]
    sin_tab[32:64, :] = sine[:, 64:]

    def added(own, recv, rows):
        total = own
        for d in range(3):
            total = total + recv[d, rows, :].astype(F32)
        return total

    for copy in a1:
        copy.wait_recv()
    q_nope_sum = added(q_nope_part, a1_recv, slice(0, 64))
    q_rope_sum = added(q_rope_part, a1_recv, slice(64, 96))
    a2_send[0:64, :] = q_nope_sum.astype(BF16)
    a2_send[64:96, :] = q_rope_sum.astype(BF16)
    a2 = line(a2_send, a2_recv, a2_ss, a2_rs, z_dev, x_dev)
    for copy in a2:
        copy.start()
    for dz in (2, 1, 3, 0):
        for dx in (2, 1, 3, 0):
            if (dz, dx) != (0, 0):
                lat_copy(dz, dx).start()
    for s in range(4):
        cache_loads[2 * s].wait()
        keys[s] = cl[s].T
    for copy in a2:
        copy.wait_recv()
    q_nope = added(q_nope_sum, a2_recv, slice(0, 64)).astype(BF16)
    q_rope = added(q_rope_sum, a2_recv, slice(64, 96)).astype(BF16).astype(F32)
    swapped = jnp.where(lane % 64 < 32, pltpu.roll(q_rope, 96, 1), pltpu.roll(q_rope, 32, 1))
    q_rope = q_rope * cosine + swapped * sine
    q_rope = jnp.concatenate([q_rope[:, :64], q_rope[:, 64:]], axis=0)


    loads[7].wait()
    q_lat = dot_nt(q_nope, wk[...])
    pad = jnp.zeros((8, 64), F32)
    for j in range(8):
        block = jnp.concatenate([q_lat[8 * j : 8 * j + 8], q_rope[8 * j : 8 * j + 8], pad], axis=1)
        b_send[j] = block.astype(BF16)

    def b_copy(d):
        to = (tp + d) % 8
        return pltpu.make_async_remote_copy(
            src_ref=b_send.at[to], dst_ref=b_recv.at[tp], send_sem=b_ss, recv_sem=b_rs,
            device_id=(kv, to), device_id_type=MESH,
        )

    def all_of(ref, count, ss, rs):
        part = ref.at[pl.ds(0, count)]
        return pltpu.make_async_remote_copy(
            src_ref=part, dst_ref=part, send_sem=ss, recv_sem=rs, device_id=(kv, twin), device_id_type=MESH
        )

    for d in (4, 5, 3, 2, 6, 7, 1):
        b_copy(d).start()
    b_recv[tp] = b_send[tp]
    for d in (1, 3, 2):
        out_y(d, (y + d) % 4).wait_recv()
    for d in (1, 3, 2):
        out_z(d, z).start()
    out_twin(0, core).start()
    all_of(lat_recv, 15, lat_ss, lat_rs).wait_recv()
    lat_sum = lat_recv[0]
    for k in range(1, 16):
        lat_sum = lat_sum + lat_recv[k]
    loads[8].wait()
    lat_raw = lat_sum[:, :512]
    latent = (
        lat_raw * lax.rsqrt(jnp.mean(lat_raw * lat_raw, axis=1, keepdims=True) + EPSILON) * lgain[...]
    ).astype(BF16).astype(F32)
    key_raw = lat_sum[:, 512:576]
    new_seq = kv // 2
    new_row = tp * 8 + new_seq
    key_swapped = jnp.concatenate([key_raw[:, 32:], key_raw[:, :32]], axis=1)
    new_rope = key_raw * cos_tab[pl.ds(new_row, 1), :] + key_swapped * sin_tab[pl.ds(new_row, 1), :]
    new_rope = new_rope.astype(BF16).astype(F32)
    for s in range(4, 8):
        cache_loads[2 * s].wait()
        keys[s] = cl[s].T
    all_of(b_recv, 7, b_ss, b_rs).wait_recv()

    for copy in value_forwards:
        copy.wait_recv()
        copy.start()

    for h in range(8):
        rows = b_recv[h].astype(F32)
        for i in range(5):
            q_tab[i, 8 * h : 8 * h + 8, :] = rows[:, 128 * i : 128 * i + 128]

    def query_of(s):
        return jnp.concatenate([q_tab[i, pl.ds(s, 8, stride=8), :] for i in range(5)], axis=1)

    for copy in cache_loads[1::2]:
        copy.wait()
    factor = 192.0 ** (-0.5)

    def scores_of(s):
        q = query_of(s).astype(BF16)
        return dot(q[:, :512], keys[s]) + dot(q[:, 512:576], cr[s])

    scores = jnp.concatenate([scores_of(s) for s in range(8)], axis=0) * factor

    q_new = query_of(new_seq)
    new_score = (
        jnp.sum(q_new[:, :512] * latent, axis=1, keepdims=True)
        + jnp.sum(q_new[:, 512:576] * new_rope, axis=1, keepdims=True)
    ) * factor

    row_seq = iota((64, 1), 0) // 8
    row_length = jnp.concatenate(
        [jnp.broadcast_to(len_tab[pl.ds(tp * 8 + s, 1), 0:1], (8, 1)) for s in range(8)], axis=0
    )
    positions = (kv * 512 + iota((64, 512), 1)).astype(F32)
    visible = positions < row_length
    is_new = jnp.logical_and(row_seq == new_seq, kv % 2 == 0)
    own_new = jnp.where(is_new, jnp.concatenate([new_score] * 8, axis=0), NEGATIVE)
    top = jnp.maximum(jnp.max(jnp.where(visible, scores, NEGATIVE), axis=1, keepdims=True), own_new)
    weights = jnp.where(visible, jnp.exp(scores - top), 0.0)
    new_weight = jnp.where(is_new, jnp.exp(own_new - top), 0.0)
    total = jnp.sum(weights, axis=1, keepdims=True) + new_weight
    some = total > 0.0
    safe = jnp.where(some, total, 1.0)
    lse = jnp.where(some, top + jnp.log(safe), NEGATIVE)
    heads = [dot(weights[8 * s : 8 * s + 8].astype(BF16), cl[s]) for s in range(4)]
    def l_copy(dz, dx, ss, rs):
        return pltpu.make_async_remote_copy(
            src_ref=l_send, dst_ref=l_recv.at[kv], send_sem=ss, recv_sem=rs,
            device_id=(lax.rem(z + dz, 4) * 4 + lax.rem(x + dx, 4), tp), device_id_type=MESH,
        )

    l_send[...] = to_row(lse, 64)
    for d in (2, 1, 3):
        l_copy(0, d, lx_ss, lx_rs).start()
    l_recv[kv] = l_send[...]
    heads += [dot(weights[8 * s : 8 * s + 8].astype(BF16), cl[s]) for s in range(4, 8)]
    acc = jnp.concatenate(heads, axis=0) + new_weight.astype(BF16).astype(F32) * latent

    def gather_wait(buf, ss, rs):
        for d in range(4):
            slot = (twin + 2 * d) % 8
            gather_copy(buf, ss, rs, 0, slot, twin).wait_recv()

    gather_wait(wv, gv_ss, gv_rs)
    by_head = dot(acc.astype(BF16), jnp.concatenate([wv[h] for h in range(8)], axis=1))
    value = by_head[:, 0:128]
    row_head = iota((64, 128), 0) % 8
    for h in range(1, 8):
        value = jnp.where(row_head == h, by_head[:, 128 * h : 128 * h + 128], value)
    value = value / safe

    def merge(value, lse, others, recv, copies):
        top = lse
        for other in others:
            top = jnp.maximum(top, other)
        own_scale = jnp.exp(lse - top)
        scales = [jnp.exp(other - top) for other in others]
        total = own_scale + scales[0] + scales[1] + scales[2]
        merged_scales = [scale / total for scale in scales]
        merged = value * (own_scale / total)
        for copy in copies:
            copy.wait_recv()
        for d in range(3):
            merged = merged + recv[d].astype(F32) * merged_scales[d]
        return merged, top + jnp.log(total)

    c1_send[...] = value.astype(BF16)
    c1 = line1(c1_send, c1_recv, c1_ss, c1_rs, x_dev)
    for copy in (c1[1], c1[0], c1[2]):
        copy.start()
    for dz in (2, 1, 3):
        for dx in (2, 1, 3, 0):
            l_copy(dz, dx, lo_ss, lo_rs).start()
    all_of(l_recv, 3, lx_ss, lx_rs).wait_recv()
    others = [to_column(l_recv[z * 4 + (x + 4 - d) % 4], 64) for d in (1, 2, 3)]
    value, lse = merge(value, lse, others, c1_recv, c1)

    for d in (1, 3, 2):
        out_z(d, (z + d) % 4).wait_recv()
        out_twin(d, core).start()

    c2_send[...] = value.astype(BF16)
    c2 = line1(c2_send, c2_recv, c2_ss, c2_rs, z_dev)
    for copy in c2:
        copy.start()
    all_of(l_recv, 12, lo_ss, lo_rs).wait_recv()
    others = []
    for d in (1, 2, 3):
        rows = [l_recv[(z + 4 - d) % 4 * 4 + i] for i in range(4)]
        best = jnp.maximum(jnp.maximum(rows[0], rows[1]), jnp.maximum(rows[2], rows[3]))
        mass = jnp.exp(rows[0] - best)
        for i in range(1, 4):
            mass = mass + jnp.exp(rows[i] - best)
        others.append(to_column(best + jnp.log(mass), 64))
    value, lse = merge(value, lse, others, c2_recv, c2)

    for d in range(4):
        out_twin(d, 1 - core).wait_recv()
    o_tab[...] = value
    head_out = jnp.concatenate(
        [o_tab[pl.ds(2 * r + c, 8, stride=8), :] for c in range(2) for r in range(4)], axis=1
    ).astype(BF16)
    mixed_z = dot(head_out, jnp.concatenate([wo[k].reshape(1024, 128) for k in range(4)], axis=1))
    own_mixed = mixed_z[:, 0:128]
    for k in range(1, 4):
        own_mixed = jnp.where(z == k, mixed_z[:, 128 * k : 128 * k + 128], own_mixed)
    m_send[...] = own_mixed
    g_send[...] = to_row(jnp.sum(mixed_z * mixed_z, axis=1, keepdims=True), 8)

    def m_copy(slot, to):
        return pltpu.make_async_remote_copy(
            src_ref=m_send, dst_ref=m_recv.at[slot], send_sem=m_ss, recv_sem=m_rs,
            device_id=(kv, to), device_id_type=MESH,
        )

    place = x * 8 + tp

    def g_copy(at_x, at_tp):
        return pltpu.make_async_remote_copy(
            src_ref=g_send, dst_ref=g_recv.at[place], send_sem=g_ss, recv_sem=g_rs,
            device_id=(z * 4 + at_x, at_tp), device_id_type=MESH,
        )

    for dx in (2, 1, 3, 0):
        for dt in (4, 5, 3, 2, 6, 7, 1, 0):
            if (dx, dt) != (0, 0):
                g_copy(lax.rem(x + dx, 4), lax.rem(tp + dt, 8)).start()
    for d in (4, 5, 3, 2, 6, 7, 1):
        m_copy(tp, (tp + d) % 8).start()
    m_recv[tp] = m_send[...]
    g_recv[place] = g_send[...]
    loads[11].wait()

    for copy in a1 + a2 + c1 + c2 + value_sends + value_forwards:
        copy.wait_send()
    for d in range(4):
        out_twin(d, core).wait_send()
    for d in range(1, 4):
        out_y(d, y).wait_send()
        out_z(d, z).wait_send()
    all_of(b_recv, 7, b_ss, b_rs).wait_send()
    all_of(lat_recv, 15, lat_ss, lat_rs).wait_send()
    all_of(l_recv, 3, lx_ss, lx_rs).wait_send()
    all_of(l_recv, 12, lo_ss, lo_rs).wait_send()

    all_of(m_recv, 7, m_ss, m_rs).wait_recv()
    all_of(g_recv, 31, g_ss, g_rs).wait_recv()
    mixed = m_recv[...].reshape(64, 128)
    squares = []
    for j in range(8):
        total = g_recv[j]
        for k in range(1, 4):
            total = total + g_recv[8 * k + j]
        squares.append(jnp.broadcast_to(total, (8, 128)))
    inverse = lax.rsqrt(jnp.concatenate(squares, axis=0) / 2048.0 + EPSILON)
    picked = iota((64, 128), 0) % 8 == iota((64, 128), 1)
    inverse = jnp.sum(jnp.where(picked, inverse, 0.0), axis=1, keepdims=True)
    out_ref[...] = (mixed * inverse * ogain[...]).astype(BF16)

    all_of(m_recv, 7, m_ss, m_rs).wait_send()
    all_of(g_recv, 31, g_ss, g_rs).wait_send()


def on_device(
    tokens, token_gain, w_query, w_down_kv, w_rope_key, latent_gain, w_key_up, w_value_up, w_out, out_gain,
    cache_latent, cache_rope, lengths,
):
    freq = 1.0 / 10000.0 ** (np.arange(0, 64, 2, dtype=np.float32) / np.float32(64.0))
    freq = jnp.asarray(np.tile(freq.astype(np.float32), 4)[None, :])
    operands = (
        tokens, token_gain.reshape(1, 128), w_query.T, w_down_kv, w_rope_key.T, latent_gain.reshape(1, 512),
        w_key_up.reshape(512, 128), w_value_up.reshape(512, 128), w_out, out_gain.reshape(1, 128),
        cache_latent, cache_rope.transpose(0, 2, 1), lengths.reshape(1, 64), freq,
    )
    shapes = [(a.shape, a.dtype) for a in operands]
    shapes[7] = ((8, 512, 128), BF16)
    shapes[8] = ((4, 2, 4, 128, 128), BF16)
    local = [pltpu.VMEM(*a) for a in shapes]
    operands = tuple(pltpu.with_memory_space_constraint(v, pltpu.HBM) for v in operands)
    dma = pltpu.SemaphoreType.DMA
    scratch = local + [
        pltpu.VMEM((64, 128), F32), pltpu.VMEM((64, 64), F32), pltpu.VMEM((64, 64), F32),
        pltpu.VMEM((96, 128), BF16), pltpu.VMEM((3, 96, 128), BF16),
        pltpu.VMEM((96, 128), BF16), pltpu.VMEM((3, 96, 128), BF16),
        pltpu.VMEM((64, 640), F32), pltpu.VMEM((8, 1, 640), F32), pltpu.VMEM((16, 1, 640), F32),
        pltpu.VMEM((8, 512, 512), BF16),
        pltpu.VMEM((8, 8, 640), BF16), pltpu.VMEM((8, 8, 640), BF16),
        pltpu.VMEM((5, 64, 128), F32), pltpu.VMEM((64, 128), F32),
        pltpu.VMEM((64, 128), BF16), pltpu.VMEM((3, 64, 128), BF16),
        pltpu.VMEM((64, 128), BF16), pltpu.VMEM((3, 64, 128), BF16),
        pltpu.VMEM((1, 128), F32), pltpu.VMEM((16, 1, 128), F32),
        pltpu.VMEM((8, 128), F32), pltpu.VMEM((8, 8, 128), F32),
        pltpu.VMEM((1, 128), F32), pltpu.VMEM((32, 1, 128), F32),
        dma((12,)), dma((16,)),
        dma((6,)), dma((6,)), dma((6,)), dma((6,)), dma, dma,
        dma, dma, dma((8,)), dma((8,)),
        dma((4,)), dma((4,)), dma((4,)), dma((4,)), dma((4,)), dma((4,)),
        dma((3,)), dma((3,)), dma((3,)), dma((3,)), dma, dma, dma, dma,
        dma, dma, dma, dma,
    ]
    return pl.pallas_call(
        kernel,
        out_shape=pltpu.VMEM((64, 128), BF16),
        in_specs=[pl.BlockSpec(memory_space=pltpu.HBM)] * len(operands),
        out_specs=pl.BlockSpec(memory_space=pltpu.VMEM),
        scratch_shapes=scratch,
        compiler_params=pltpu.CompilerParams(
            collective_id=0, has_side_effects=True, vmem_limit_bytes=48 * 1024 * 1024
        ),
    )(*operands)


def solution(mesh):
    return jax.shard_map(
        on_device,
        mesh=mesh,
        in_specs=(
            P(None, "kv"), P("kv"), P("kv", "tp"), P("kv", None), P("kv", None), P(),
            P("tp", None, None), P("tp", None, None), P("tp", "kv"), P("kv"),
            P("tp", "kv", None), P("tp", "kv", None), P(),
        ),
        out_specs=P(None, "kv"),
        check_vma=False,
    )
```

```python
import functools

import jax
import jax.numpy as jnp
import numpy as np
from jax import lax
from jax.experimental import pallas as pl
from jax.experimental.pallas import tpu as pltpu
from jax.sharding import PartitionSpec as P

MESH = pl.DeviceIdType.MESH
EPSILON = 1e-06
NEGATIVE = -1e30
BF16 = jnp.bfloat16
F32 = jnp.float32


def dot(a, b):
    return jnp.dot(a, b, preferred_element_type=F32)


def dot_nt(a, b):
    return lax.dot_general(a, b, (((1,), (1,)), ((), ())), preferred_element_type=F32)


def iota(shape, axis):
    return lax.broadcasted_iota(jnp.int32, shape, axis)


def to_column(row, rows):
    picked = iota((rows, rows), 0) == iota((rows, rows), 1)
    return jnp.sum(jnp.where(picked, row[:, :rows], 0.0), axis=1, keepdims=True)


def to_row(column, rows):
    picked = iota((rows, 128), 0) == iota((rows, 128), 1)
    return jnp.sum(jnp.where(picked, column, 0.0), axis=0, keepdims=True)


def kernel(
    tok_h, tgain_h, wq_h, wd_h, wr_h, lgain_h, wk_h, wv_h, wo_h, ogain_h, cl_h, cr_h, len_h, freq_h,
    out_ref,
    tok, tgain, wq, wd, wr, lgain, wk, wv, wo, ogain, cl, cr, lens, freq,
    len_tab, cos_tab, sin_tab,
    a1_send, a1_recv, a2_send, a2_recv,
    lat_all, lat_send, lat_recv,
    keys, b_send, b_recv, q_tab, o_tab,
    c_send, c_recv, l_send, l_recv,
    m_send, m_recv, g_send, g_recv,
    load_sem, cache_sem,
    a1_ss, a1_rs, a2_ss, a2_rs, lat_ss, lat_rs, b_ss, b_rs, gv_ss, gv_rs, oy_ss, oy_rs, oz_ss, oz_rs, ot_ss, ot_rs,
    c_ss, c_rs, l_ss, l_rs, m_ss, m_rs, g_ss, g_rs,
):
    kv = lax.axis_index("kv")
    tp = lax.axis_index("tp")
    z = kv // 4
    x = kv % 4
    y = tp // 2
    core = tp % 2

    pairs = [
        (tok_h, tok), (tgain_h, tgain), (wq_h, wq), (len_h, lens), (freq_h, freq), (wd_h, wd), (wr_h, wr),
        (wk_h, wk), (lgain_h, lgain), (wv_h, wv.at[tp]), (wo_h, wo.at[z, core, y]), (ogain_h, ogain),
    ]
    loads = [pltpu.make_async_copy(s, d, load_sem.at[i]) for i, (s, d) in enumerate(pairs)]
    cache_loads = []
    for s in range(8):
        cache_loads.append(pltpu.make_async_copy(cl_h.at[s], cl.at[s], cache_sem.at[s]))
        cache_loads.append(pltpu.make_async_copy(cr_h.at[s], cr.at[s], cache_sem.at[8 + s]))
    for copy in loads[:3]:
        copy.start()
    barrier = pltpu.get_barrier_semaphore()

    def greet(to_kv, to_tp):
        pl.semaphore_signal(barrier, inc=1, device_id=(to_kv, to_tp), device_id_type=MESH)

    for d in (2, 1, 3):
        greet(z * 4 + lax.rem(x + d, 4), tp)
    for d in (2, 1, 3):
        greet(lax.rem(z + d, 4) * 4 + x, tp)
    for d in (4, 5, 3, 2, 6, 7, 1):
        greet(kv, lax.rem(tp + d, 8))

    for i in range(3):
        loads[i].wait()
    scaled = (tok[...].astype(F32) * tgain[...]).astype(BF16)
    q_part = dot_nt(scaled, wq[...])
    rope_part = q_part[:, 128:192]
    q_nope_part = q_part[:, :128]
    q_rope_part = jnp.concatenate([rope_part[:32], rope_part[32:]], axis=1)
    a1_send[0:64, :] = q_nope_part.astype(BF16)
    a1_send[64:96, :] = q_rope_part.astype(BF16)

    for copy in loads[3:] + cache_loads:
        copy.start()
    pl.semaphore_wait(barrier, 13)

    def x_dev(d):
        return (z * 4 + (x + d) % 4, tp)

    def z_dev(d):
        return (((z + d) % 4) * 4 + x, tp)

    def line(src, dst, ss, rs, first, second):
        half = src.shape[0] // 2
        copies = []
        for d in (2, 1, 3):
            for k, dev in enumerate((first, second)):
                rows = pl.ds(k * half, half)
                copies.append(
                    pltpu.make_async_remote_copy(
                        src_ref=src.at[rows], dst_ref=dst.at[d - 1, rows],
                        send_sem=ss.at[3 * k + d - 1], recv_sem=rs.at[3 * k + d - 1],
                        device_id=dev(d), device_id_type=MESH,
                    )
                )
        return copies

    def line1(src, dst, ss, rs, dev):
        return [
            pltpu.make_async_remote_copy(
                src_ref=src, dst_ref=dst.at[d - 1], send_sem=ss.at[d - 1], recv_sem=rs.at[d - 1],
                device_id=dev(d), device_id_type=MESH,
            )
            for d in (1, 2, 3)
        ]

    a1 = line(a1_send, a1_recv, a1_ss, a1_rs, x_dev, z_dev)
    for copy in a1:
        copy.start()

    twin = tp + 1 - 2 * core

    def gather_copy(buf, ss, rs, i, slot, to):
        return pltpu.make_async_remote_copy(
            src_ref=buf.at[slot], dst_ref=buf.at[slot], send_sem=ss.at[i], recv_sem=rs.at[slot],
            device_id=(kv, to), device_id_type=MESH,
        )

    def gather_first(buf, ss, rs):
        copies = [gather_copy(buf, ss, rs, i, tp, (tp + 2 * d) % 8) for i, d in enumerate((1, 3, 2))]
        return copies + [gather_copy(buf, ss, rs, 3, tp, twin)]

    def gather_forward(buf, ss, rs):
        slots = [(tp + 2 * d) % 8 for d in (1, 3, 2)]
        return [gather_copy(buf, ss, rs, 4 + i, slot, twin) for i, slot in enumerate(slots)]

    loads[9].wait()
    loads[10].wait()
    value_sends = gather_first(wv, gv_ss, gv_rs)
    value_forwards = gather_forward(wv, gv_ss, gv_rs)

    def out_y(d, at):
        return pltpu.make_async_remote_copy(
            src_ref=wo.at[z, core, y], dst_ref=wo.at[z, core, at], send_sem=oy_ss.at[d], recv_sem=oy_rs.at[at],
            device_id=(kv, (tp + 2 * d) % 8), device_id_type=MESH,
        )

    def out_z(d, at):
        return pltpu.make_async_remote_copy(
            src_ref=wo.at[z, core], dst_ref=wo.at[at, core], send_sem=oz_ss.at[d], recv_sem=oz_rs.at[at],
            device_id=((z + d) % 4 * 4 + x, tp), device_id_type=MESH,
        )

    def out_twin(d, half):
        at = (z + d) % 4
        return pltpu.make_async_remote_copy(
            src_ref=wo.at[at, core], dst_ref=wo.at[at, half], send_sem=ot_ss.at[d], recv_sem=ot_rs.at[at],
            device_id=(kv, twin), device_id_type=MESH,
        )

    for d in (1, 3, 2):
        out_y(d, y).start()
    for copy in value_sends:
        copy.start()

    for i in range(3, 7):
        loads[i].wait()
    lat_all[:, 0:512] = dot(scaled, wd[...])
    lat_all[:, 512:576] = dot_nt(scaled, wr[...])
    lat_all[:, 576:640] = jnp.zeros((64, 64), F32)
    mine = lat_all[pl.ds(pl.multiple_of(tp * 8, 8), 8), :]
    for r in range(8):
        lat_send[r] = mine[r : r + 1, :]
    lat_recv[kv] = lat_send[kv // 2]

    def lat_copy(dz, dx):
        at_z = lax.rem(z + dz, 4)
        at_x = lax.rem(x + dx, 4)
        return pltpu.make_async_remote_copy(
            src_ref=lat_send.at[at_z * 2 + at_x // 2], dst_ref=lat_recv.at[kv], send_sem=lat_ss, recv_sem=lat_rs,
            device_id=(at_z * 4 + at_x, tp), device_id_type=MESH,
        )

    len_col = to_column(lens[...].astype(F32), 64)
    len_tab[...] = jnp.broadcast_to(len_col, (64, 128))
    lane = iota((32, 128), 1)
    packed_len = jnp.where(lane < 64, len_col[:32], len_col[32:])
    angle = packed_len * freq[...]
    cosine = jnp.cos(angle)
    sine = jnp.sin(angle)
    sine = jnp.where(lane % 64 < 32, -sine, sine)
    cos_tab[0:32, :] = cosine[:, :64]
    cos_tab[32:64, :] = cosine[:, 64:]
    sin_tab[0:32, :] = sine[:, :64]
    sin_tab[32:64, :] = sine[:, 64:]

    def added(own, recv, rows):
        total = own
        for d in range(3):
            total = total + recv[d, rows, :].astype(F32)
        return total

    for copy in a1:
        copy.wait_recv()
    q_nope_sum = added(q_nope_part, a1_recv, slice(0, 64))
    q_rope_sum = added(q_rope_part, a1_recv, slice(64, 96))
    a2_send[0:64, :] = q_nope_sum.astype(BF16)
    a2_send[64:96, :] = q_rope_sum.astype(BF16)
    a2 = line(a2_send, a2_recv, a2_ss, a2_rs, z_dev, x_dev)
    for copy in a2:
        copy.start()
    for dz in (2, 1, 3, 0):
        for dx in (2, 1, 3, 0):
            if (dz, dx) != (0, 0):
                lat_copy(dz, dx).start()
    for s in range(4):
        cache_loads[2 * s].wait()
        keys[s] = cl[s].T
    for copy in a2:
        copy.wait_recv()
    q_nope = added(q_nope_sum, a2_recv, slice(0, 64)).astype(BF16)
    q_rope = added(q_rope_sum, a2_recv, slice(64, 96)).astype(BF16).astype(F32)
    swapped = jnp.where(lane % 64 < 32, pltpu.roll(q_rope, 96, 1), pltpu.roll(q_rope, 32, 1))
    q_rope = q_rope * cosine + swapped * sine
    q_rope = jnp.concatenate([q_rope[:, :64], q_rope[:, 64:]], axis=0)


    for d in (1, 3, 2):
        out_y(d, (y + d) % 4).wait_recv()
    for d in (1, 3, 2):
        out_z(d, z).start()
    out_twin(0, core).start()
    loads[7].wait()
    q_lat = dot_nt(q_nope, wk[...])
    pad = jnp.zeros((8, 64), F32)
    for j in range(8):
        block = jnp.concatenate([q_lat[8 * j : 8 * j + 8], q_rope[8 * j : 8 * j + 8], pad], axis=1)
        b_send[j] = block.astype(BF16)

    def b_copy(d):
        to = (tp + d) % 8
        return pltpu.make_async_remote_copy(
            src_ref=b_send.at[to], dst_ref=b_recv.at[tp], send_sem=b_ss, recv_sem=b_rs,
            device_id=(kv, to), device_id_type=MESH,
        )

    def all_of(ref, count, ss, rs):
        part = ref.at[pl.ds(0, count)]
        return pltpu.make_async_remote_copy(
            src_ref=part, dst_ref=part, send_sem=ss, recv_sem=rs, device_id=(kv, twin), device_id_type=MESH
        )

    for d in (4, 5, 3, 2, 6, 7, 1):
        b_copy(d).start()
    b_recv[tp] = b_send[tp]
    all_of(lat_recv, 15, lat_ss, lat_rs).wait_recv()
    lat_sum = lat_recv[0]
    for k in range(1, 16):
        lat_sum = lat_sum + lat_recv[k]
    loads[8].wait()
    lat_raw = lat_sum[:, :512]
    latent = (
        lat_raw * lax.rsqrt(jnp.mean(lat_raw * lat_raw, axis=1, keepdims=True) + EPSILON) * lgain[...]
    ).astype(BF16).astype(F32)
    key_raw = lat_sum[:, 512:576]
    new_seq = kv // 2
    new_row = tp * 8 + new_seq
    key_swapped = jnp.concatenate([key_raw[:, 32:], key_raw[:, :32]], axis=1)
    new_rope = key_raw * cos_tab[pl.ds(new_row, 1), :] + key_swapped * sin_tab[pl.ds(new_row, 1), :]
    new_rope = new_rope.astype(BF16).astype(F32)
    for s in range(4, 8):
        cache_loads[2 * s].wait()
        keys[s] = cl[s].T
    all_of(b_recv, 7, b_ss, b_rs).wait_recv()

    for copy in value_forwards:
        copy.wait_recv()
        copy.start()

    for h in range(8):
        rows = b_recv[h].astype(F32)
        for i in range(5):
            q_tab[i, 8 * h : 8 * h + 8, :] = rows[:, 128 * i : 128 * i + 128]

    def query_of(s):
        return jnp.concatenate([q_tab[i, pl.ds(s, 8, stride=8), :] for i in range(5)], axis=1)

    for copy in cache_loads[1::2]:
        copy.wait()
    factor = 192.0 ** (-0.5)

    def scores_of(s):
        q = query_of(s).astype(BF16)
        return dot(q[:, :512], keys[s]) + dot(q[:, 512:576], cr[s])

    scores = jnp.concatenate([scores_of(s) for s in range(8)], axis=0) * factor

    q_new = query_of(new_seq)
    new_score = (
        jnp.sum(q_new[:, :512] * latent, axis=1, keepdims=True)
        + jnp.sum(q_new[:, 512:576] * new_rope, axis=1, keepdims=True)
    ) * factor

    row_seq = iota((64, 1), 0) // 8
    row_length = jnp.concatenate(
        [jnp.broadcast_to(len_tab[pl.ds(tp * 8 + s, 1), 0:1], (8, 1)) for s in range(8)], axis=0
    )
    positions = (kv * 512 + iota((64, 512), 1)).astype(F32)
    visible = positions < row_length
    is_new = jnp.logical_and(row_seq == new_seq, kv % 2 == 0)
    own_new = jnp.where(is_new, jnp.concatenate([new_score] * 8, axis=0), NEGATIVE)
    top = jnp.maximum(jnp.max(jnp.where(visible, scores, NEGATIVE), axis=1, keepdims=True), own_new)
    weights = jnp.where(visible, jnp.exp(scores - top), 0.0)
    new_weight = jnp.where(is_new, jnp.exp(own_new - top), 0.0)
    total = jnp.sum(weights, axis=1, keepdims=True) + new_weight
    some = total > 0.0
    safe = jnp.where(some, total, 1.0)
    lse = jnp.where(some, top + jnp.log(safe), NEGATIVE)
    heads = [dot(weights[8 * s : 8 * s + 8].astype(BF16), cl[s]) for s in range(4)]
    def kv_at(dz, dx):
        return lax.rem(z + dz, 4) * 4 + lax.rem(x + dx, 4)

    others = [(dz, dx) for dz in (2, 1, 3, 0) for dx in (2, 1, 3, 0) if (dz, dx) != (0, 0)]
    l_send[...] = to_row(lse, 64)
    for dz, dx in others:
        pltpu.make_async_remote_copy(
            src_ref=l_send, dst_ref=l_recv.at[kv], send_sem=l_ss, recv_sem=l_rs,
            device_id=(kv_at(dz, dx), tp), device_id_type=MESH,
        ).start()
    l_recv[kv] = l_send[...]
    heads += [dot(weights[8 * s : 8 * s + 8].astype(BF16), cl[s]) for s in range(4, 8)]
    acc = jnp.concatenate(heads, axis=0) + new_weight.astype(BF16).astype(F32) * latent

    def gather_wait(buf, ss, rs):
        for d in range(4):
            slot = (twin + 2 * d) % 8
            gather_copy(buf, ss, rs, 0, slot, twin).wait_recv()

    gather_wait(wv, gv_ss, gv_rs)
    by_head = dot(acc.astype(BF16), jnp.concatenate([wv[h] for h in range(8)], axis=1))
    value = by_head[:, 0:128]
    row_head = iota((64, 128), 0) % 8
    for h in range(1, 8):
        value = jnp.where(row_head == h, by_head[:, 128 * h : 128 * h + 128], value)
    value = value / safe

    c_send[...] = value.astype(BF16)

    def c_rows(at_z):
        return c_send.at[pl.ds(pl.multiple_of(at_z * 16, 16), 16)]

    for dz, dx in others:
        pltpu.make_async_remote_copy(
            src_ref=c_rows(lax.rem(z + dz, 4)), dst_ref=c_recv.at[kv], send_sem=c_ss, recv_sem=c_rs,
            device_id=(kv_at(dz, dx), tp), device_id_type=MESH,
        ).start()
    c_recv[kv] = c_send[pl.ds(pl.multiple_of(z * 16, 16), 16), :]

    for d in (1, 3, 2):
        out_z(d, (z + d) % 4).wait_recv()
        out_twin(d, core).start()

    all_of(l_recv, 15, l_ss, l_rs).wait_recv()
    rows = [l_recv[k] for k in range(16)]
    top_row = functools.reduce(jnp.maximum, rows)
    masses = [jnp.exp(row - top_row) for row in rows]
    whole = functools.reduce(jnp.add, masses)
    own_lane = iota((16, 128), 1) == iota((16, 128), 0) + z * 16
    shares = [
        jnp.sum(jnp.where(own_lane, mass / whole, 0.0), axis=1, keepdims=True) for mass in masses
    ]

    all_of(c_recv, 15, c_ss, c_rs).wait_recv()
    merged = c_recv[0].astype(F32) * shares[0]
    for k in range(1, 16):
        merged = merged + c_recv[k].astype(F32) * shares[k]

    o_tab[...] = merged
    for d in range(4):
        out_twin(d, 1 - core).wait_recv()
    head_out = jnp.concatenate(
        [o_tab[pl.ds(2 * r + c, 2, stride=8), :] for c in range(2) for r in range(4)], axis=1
    ).astype(BF16)
    mixed_z = dot(head_out, jnp.concatenate([wo[k].reshape(1024, 128) for k in range(4)], axis=1))
    for k in range(4):
        m_send[k, :, 0:128] = mixed_z[0:1, 128 * k : 128 * k + 128]
        m_send[k, :, 128:256] = mixed_z[1:2, 128 * k : 128 * k + 128]
    g_send[...] = to_row(jnp.sum(mixed_z * mixed_z, axis=1, keepdims=True), 2)

    pair = tp * 4 + z

    def m_start(dz, dt):
        at_z = lax.rem(z + dz, 4)
        pltpu.make_async_remote_copy(
            src_ref=m_send.at[at_z], dst_ref=m_recv.at[pair], send_sem=m_ss, recv_sem=m_rs,
            device_id=(at_z * 4 + x, lax.rem(tp + dt, 8)), device_id_type=MESH,
        ).start()

    def g_start(dz, dx, dt):
        pltpu.make_async_remote_copy(
            src_ref=g_send, dst_ref=g_recv.at[x * 32 + pair], send_sem=g_ss, recv_sem=g_rs,
            device_id=(kv_at(dz, dx), lax.rem(tp + dt, 8)), device_id_type=MESH,
        ).start()

    steps = [(dz, dx, dt) for dz in (2, 1, 3, 0) for dx in (2, 1, 3, 0) for dt in (4, 5, 3, 2, 6, 7, 1, 0)][:-1]
    hops = [min(dz, 4 - dz) + min(dx, 4 - dx) + min(dt // 2, 4 - dt // 2) for dz, dx, dt in steps]
    for away in (6, 5, 4):
        for step, hop in zip(steps, hops):
            if hop == away:
                g_start(*step)
    for dz in (2, 1, 3, 0):
        for dt in (4, 5, 3, 2, 6, 7, 1, 0):
            if (dz, dt) != (0, 0):
                m_start(dz, dt)
    for away in (3, 2, 1, 0):
        for step, hop in zip(steps, hops):
            if hop == away:
                g_start(*step)
    m_recv[pair] = m_send[z]
    g_recv[x * 32 + pair] = g_send[...]
    loads[11].wait()

    for copy in a1 + a2 + value_sends + value_forwards:
        copy.wait_send()
    for d in range(4):
        out_twin(d, core).wait_send()
    for d in range(1, 4):
        out_y(d, y).wait_send()
        out_z(d, z).wait_send()
    all_of(b_recv, 7, b_ss, b_rs).wait_send()
    all_of(lat_recv, 15, lat_ss, lat_rs).wait_send()
    all_of(l_recv, 15, l_ss, l_rs).wait_send()
    all_of(c_recv, 15, c_ss, c_rs).wait_send()

    all_of(m_recv, 31, m_ss, m_rs).wait_recv()
    all_of(g_recv, 127, g_ss, g_rs).wait_recv()
    octet = iota((8, 128), 0)

    def eight(of):
        row = jnp.broadcast_to(of(0), (8, 128))
        for i in range(1, 8):
            row = jnp.where(octet == i, of(i), row)
        return row

    mixed = jnp.concatenate(
        [
            eight(lambda i: m_recv[4 * v + i // 2, :, 128 * (i % 2) : 128 * (i % 2) + 128])
            for v in range(8)
        ],
        axis=0,
    )
    totals = [g_recv[j] + g_recv[32 + j] + g_recv[64 + j] + g_recv[96 + j] for j in range(32)]
    squares = jnp.concatenate([eight(lambda i: totals[4 * v + i // 2]) for v in range(8)], axis=0)
    picked = iota((64, 128), 0) % 2 == iota((64, 128), 1)
    squares = jnp.sum(jnp.where(picked, squares, 0.0), axis=1, keepdims=True)
    inverse = lax.rsqrt(squares / 2048.0 + EPSILON)
    out_ref[...] = (mixed * inverse * ogain[...]).astype(BF16)

    all_of(m_recv, 31, m_ss, m_rs).wait_send()
    all_of(g_recv, 127, g_ss, g_rs).wait_send()


def on_device(
    tokens, token_gain, w_query, w_down_kv, w_rope_key, latent_gain, w_key_up, w_value_up, w_out, out_gain,
    cache_latent, cache_rope, lengths,
):
    freq = 1.0 / 10000.0 ** (np.arange(0, 64, 2, dtype=np.float32) / np.float32(64.0))
    freq = jnp.asarray(np.tile(freq.astype(np.float32), 4)[None, :])
    operands = (
        tokens, token_gain.reshape(1, 128), w_query.T, w_down_kv, w_rope_key.T, latent_gain.reshape(1, 512),
        w_key_up.reshape(512, 128), w_value_up.reshape(512, 128), w_out, out_gain.reshape(1, 128),
        cache_latent, cache_rope.transpose(0, 2, 1), lengths.reshape(1, 64), freq,
    )
    shapes = [(a.shape, a.dtype) for a in operands]
    shapes[7] = ((8, 512, 128), BF16)
    shapes[8] = ((4, 2, 4, 128, 128), BF16)
    local = [pltpu.VMEM(*a) for a in shapes]
    operands = tuple(pltpu.with_memory_space_constraint(v, pltpu.HBM) for v in operands)
    dma = pltpu.SemaphoreType.DMA
    scratch = local + [
        pltpu.VMEM((64, 128), F32), pltpu.VMEM((64, 64), F32), pltpu.VMEM((64, 64), F32),
        pltpu.VMEM((96, 128), BF16), pltpu.VMEM((3, 96, 128), BF16),
        pltpu.VMEM((96, 128), BF16), pltpu.VMEM((3, 96, 128), BF16),
        pltpu.VMEM((64, 640), F32), pltpu.VMEM((8, 1, 640), F32), pltpu.VMEM((16, 1, 640), F32),
        pltpu.VMEM((8, 512, 512), BF16),
        pltpu.VMEM((8, 8, 640), BF16), pltpu.VMEM((8, 8, 640), BF16),
        pltpu.VMEM((5, 64, 128), F32), pltpu.VMEM((16, 128), F32),
        pltpu.VMEM((64, 128), BF16), pltpu.VMEM((16, 16, 128), BF16),
        pltpu.VMEM((1, 128), F32), pltpu.VMEM((16, 1, 128), F32),
        pltpu.VMEM((4, 1, 256), F32), pltpu.VMEM((32, 1, 256), F32),
        pltpu.VMEM((1, 128), F32), pltpu.VMEM((128, 1, 128), F32),
        dma((12,)), dma((16,)),
        dma((6,)), dma((6,)), dma((6,)), dma((6,)), dma, dma,
        dma, dma, dma((8,)), dma((8,)),
        dma((4,)), dma((4,)), dma((4,)), dma((4,)), dma((4,)), dma((4,)),
        dma, dma, dma, dma, dma, dma, dma, dma,
    ]
    return pl.pallas_call(
        kernel,
        out_shape=pltpu.VMEM((64, 128), BF16),
        in_specs=[pl.BlockSpec(memory_space=pltpu.HBM)] * len(operands),
        out_specs=pl.BlockSpec(memory_space=pltpu.VMEM),
        scratch_shapes=scratch,
        compiler_params=pltpu.CompilerParams(
            collective_id=0, has_side_effects=True, vmem_limit_bytes=48 * 1024 * 1024
        ),
    )(*operands)


def solution(mesh):
    return jax.shard_map(
        on_device,
        mesh=mesh,
        in_specs=(
            P(None, "kv"), P("kv"), P("kv", "tp"), P("kv", None), P("kv", None), P(),
            P("tp", None, None), P("tp", None, None), P("tp", "kv"), P("kv"),
            P("tp", "kv", None), P("tp", "kv", None), P(),
        ),
        out_specs=P(None, "kv"),
        check_vma=False,
    )
```

```python
import functools

import jax
import jax.numpy as jnp
import numpy as np
from jax import lax
from jax.experimental import pallas as pl
from jax.experimental.pallas import tpu as pltpu
from jax.sharding import PartitionSpec as P

MESH = pl.DeviceIdType.MESH
EPSILON = 1e-06
NEGATIVE = -1e30
BF16 = jnp.bfloat16
F32 = jnp.float32


def dot(a, b):
    return jnp.dot(a, b, preferred_element_type=F32)


def dot_nt(a, b):
    return lax.dot_general(a, b, (((1,), (1,)), ((), ())), preferred_element_type=F32)


def iota(shape, axis):
    return lax.broadcasted_iota(jnp.int32, shape, axis)


def to_column(row, rows):
    picked = iota((rows, rows), 0) == iota((rows, rows), 1)
    return jnp.sum(jnp.where(picked, row[:, :rows], 0.0), axis=1, keepdims=True)


def to_row(column, rows):
    picked = iota((rows, 128), 0) == iota((rows, 128), 1)
    return jnp.sum(jnp.where(picked, column, 0.0), axis=0, keepdims=True)


def kernel(
    tok_h, tgain_h, wq_h, wd_h, wr_h, lgain_h, wk_h, wv_h, wo_h, ogain_h, cl_h, cr_h, len_h, freq_h,
    out_ref,
    tok, tgain, wq, wd, wr, lgain, wk, wv, wo, ogain, cl, cr, lens, freq,
    len_tab, cos_tab, sin_tab,
    a1_send, a1_recv, a2_send, a2_recv,
    lat_all, lat_send, lat_recv,
    wk_turned, keys, b_send, b_recv, q_tab, o_tab,
    c_send, c_recv, l_send, l_recv,
    m_send, m_recv, g_send, g_recv,
    load_sem, cache_sem,
    a1_ss, a1_rs, a2_ss, a2_rs, lat_ss, lat_rs, b_ss, b_rs, gv_ss, gv_rs, oy_ss, oy_rs, oz_ss, oz_rs, ot_ss, ot_rs,
    c_ss, c_rs, l_ss, l_rs, m_ss, m_rs, g_ss, g_rs,
):
    kv = lax.axis_index("kv")
    tp = lax.axis_index("tp")
    z = kv // 4
    x = kv % 4
    y = tp // 2
    core = tp % 2

    pairs = [
        (tok_h, tok), (tgain_h, tgain), (wq_h, wq), (len_h, lens), (freq_h, freq), (wd_h, wd), (wr_h, wr),
        (wk_h, wk), (lgain_h, lgain), (wv_h, wv.at[tp]), (wo_h, wo.at[z, core, y]), (ogain_h, ogain),
    ]
    loads = [pltpu.make_async_copy(s, d, load_sem.at[i]) for i, (s, d) in enumerate(pairs)]
    cache_loads = []
    for s in range(8):
        cache_loads.append(pltpu.make_async_copy(cl_h.at[s], cl.at[s], cache_sem.at[s]))
        cache_loads.append(pltpu.make_async_copy(cr_h.at[s], cr.at[s], cache_sem.at[8 + s]))
    for copy in loads[:3] + loads[9:11]:
        copy.start()
    barrier = pltpu.get_barrier_semaphore()

    def greet(to_kv, to_tp):
        pl.semaphore_signal(barrier, inc=1, device_id=(to_kv, to_tp), device_id_type=MESH)

    for d in (2, 1, 3):
        greet(z * 4 + lax.rem(x + d, 4), tp)
    for d in (2, 1, 3):
        greet(lax.rem(z + d, 4) * 4 + x, tp)
    for d in (4, 5, 3, 2, 6, 7, 1):
        greet(kv, lax.rem(tp + d, 8))

    for i in range(3):
        loads[i].wait()
    scaled = (tok[...].astype(F32) * tgain[...]).astype(BF16)
    q_part = dot_nt(scaled, wq[...])
    rope_part = q_part[:, 128:192]
    q_nope_part = q_part[:, :128]
    q_rope_part = jnp.concatenate([rope_part[:32], rope_part[32:]], axis=1)
    a1_send[0:64, :] = q_nope_part.astype(BF16)
    a1_send[64:96, :] = q_rope_part.astype(BF16)

    for copy in loads[3:9] + loads[11:] + cache_loads:
        copy.start()
    pl.semaphore_wait(barrier, 13)

    def x_dev(d):
        return (z * 4 + (x + d) % 4, tp)

    def z_dev(d):
        return (((z + d) % 4) * 4 + x, tp)

    def line(src, dst, ss, rs, first, second):
        half = src.shape[0] // 2
        copies = []
        for d in (2, 1, 3):
            for k, dev in enumerate((first, second)):
                rows = pl.ds(k * half, half)
                copies.append(
                    pltpu.make_async_remote_copy(
                        src_ref=src.at[rows], dst_ref=dst.at[d - 1, rows],
                        send_sem=ss.at[3 * k + d - 1], recv_sem=rs.at[3 * k + d - 1],
                        device_id=dev(d), device_id_type=MESH,
                    )
                )
        return copies

    def line1(src, dst, ss, rs, dev):
        return [
            pltpu.make_async_remote_copy(
                src_ref=src, dst_ref=dst.at[d - 1], send_sem=ss.at[d - 1], recv_sem=rs.at[d - 1],
                device_id=dev(d), device_id_type=MESH,
            )
            for d in (1, 2, 3)
        ]

    a1 = line(a1_send, a1_recv, a1_ss, a1_rs, x_dev, z_dev)
    for copy in a1:
        copy.start()

    twin = tp + 1 - 2 * core

    def gather_copy(buf, ss, rs, i, slot, to):
        return pltpu.make_async_remote_copy(
            src_ref=buf.at[slot], dst_ref=buf.at[slot], send_sem=ss.at[i], recv_sem=rs.at[slot],
            device_id=(kv, to), device_id_type=MESH,
        )

    def gather_first(buf, ss, rs):
        copies = [gather_copy(buf, ss, rs, i, tp, (tp + 2 * d) % 8) for i, d in enumerate((1, 3, 2))]
        return copies + [gather_copy(buf, ss, rs, 3, tp, twin)]

    def gather_forward(buf, ss, rs):
        slots = [(tp + 2 * d) % 8 for d in (1, 3, 2)]
        return [gather_copy(buf, ss, rs, 4 + i, slot, twin) for i, slot in enumerate(slots)]

    loads[9].wait()
    loads[10].wait()
    value_sends = gather_first(wv, gv_ss, gv_rs)
    value_forwards = gather_forward(wv, gv_ss, gv_rs)

    def out_y(d, at):
        return pltpu.make_async_remote_copy(
            src_ref=wo.at[z, core, y], dst_ref=wo.at[z, core, at], send_sem=oy_ss.at[d], recv_sem=oy_rs.at[at],
            device_id=(kv, (tp + 2 * d) % 8), device_id_type=MESH,
        )

    def out_z(d, at):
        return pltpu.make_async_remote_copy(
            src_ref=wo.at[z, core], dst_ref=wo.at[at, core], send_sem=oz_ss.at[d], recv_sem=oz_rs.at[at],
            device_id=((z + d) % 4 * 4 + x, tp), device_id_type=MESH,
        )

    def out_twin(d, half):
        at = (z + d) % 4
        return pltpu.make_async_remote_copy(
            src_ref=wo.at[at, core], dst_ref=wo.at[at, half], send_sem=ot_ss.at[d], recv_sem=ot_rs.at[at],
            device_id=(kv, twin), device_id_type=MESH,
        )

    for d in (1, 3, 2):
        out_y(d, y).start()
    for copy in value_sends:
        copy.start()

    for i in range(3, 7):
        loads[i].wait()
    lat_all[:, 0:512] = dot(scaled, wd[...])
    lat_all[:, 512:576] = dot_nt(scaled, wr[...])
    lat_all[:, 576:640] = jnp.zeros((64, 64), F32)
    mine = lat_all[pl.ds(pl.multiple_of(tp * 8, 8), 8), :]
    for r in range(8):
        lat_send[r] = mine[r : r + 1, :]
    lat_recv[kv] = lat_send[kv // 2]

    def lat_copy(dz, dx):
        at_z = lax.rem(z + dz, 4)
        at_x = lax.rem(x + dx, 4)
        return pltpu.make_async_remote_copy(
            src_ref=lat_send.at[at_z * 2 + at_x // 2], dst_ref=lat_recv.at[kv], send_sem=lat_ss, recv_sem=lat_rs,
            device_id=(at_z * 4 + at_x, tp), device_id_type=MESH,
        )

    len_col = to_column(lens[...].astype(F32), 64)
    len_tab[...] = jnp.broadcast_to(len_col, (64, 128))
    lane = iota((32, 128), 1)
    packed_len = jnp.where(lane < 64, len_col[:32], len_col[32:])
    angle = packed_len * freq[...]
    cosine = jnp.cos(angle)
    sine = jnp.sin(angle)
    sine = jnp.where(lane % 64 < 32, -sine, sine)
    cos_tab[0:32, :] = cosine[:, :64]
    cos_tab[32:64, :] = cosine[:, 64:]
    sin_tab[0:32, :] = sine[:, :64]
    sin_tab[32:64, :] = sine[:, 64:]

    def added(own, recv, rows):
        total = own
        for d in range(3):
            total = total + recv[d, rows, :].astype(F32)
        return total

    for copy in a1:
        copy.wait_recv()
    q_nope_sum = added(q_nope_part, a1_recv, slice(0, 64))
    q_rope_sum = added(q_rope_part, a1_recv, slice(64, 96))
    a2_send[0:64, :] = q_nope_sum.astype(BF16)
    a2_send[64:96, :] = q_rope_sum.astype(BF16)
    a2 = line(a2_send, a2_recv, a2_ss, a2_rs, z_dev, x_dev)
    for copy in a2:
        copy.start()
    for dz in (2, 1, 3, 0):
        for dx in (2, 1, 3, 0):
            if (dz, dx) != (0, 0):
                lat_copy(dz, dx).start()
    loads[7].wait()
    wk_turned[...] = wk[...].T
    for s in range(4):
        cache_loads[2 * s].wait()
        keys[s] = cl[s].T
    for copy in a2:
        copy.wait_recv()
    q_nope = added(q_nope_sum, a2_recv, slice(0, 64)).astype(BF16)
    q_rope = added(q_rope_sum, a2_recv, slice(64, 96)).astype(BF16).astype(F32)
    swapped = jnp.where(lane % 64 < 32, pltpu.roll(q_rope, 96, 1), pltpu.roll(q_rope, 32, 1))
    q_rope = q_rope * cosine + swapped * sine
    q_rope = jnp.concatenate([q_rope[:, :64], q_rope[:, 64:]], axis=0)


    for d in (1, 3, 2):
        out_y(d, (y + d) % 4).wait_recv()
    for d in (1, 3, 2):
        out_z(d, z).start()
    out_twin(0, core).start()
    q_lat = dot(q_nope, wk_turned[...])
    pad = jnp.zeros((8, 64), F32)
    for j in range(8):
        block = jnp.concatenate([q_lat[8 * j : 8 * j + 8], q_rope[8 * j : 8 * j + 8], pad], axis=1)
        b_send[j] = block.astype(BF16)

    def b_copy(d):
        to = (tp + d) % 8
        return pltpu.make_async_remote_copy(
            src_ref=b_send.at[to], dst_ref=b_recv.at[tp], send_sem=b_ss, recv_sem=b_rs,
            device_id=(kv, to), device_id_type=MESH,
        )

    def all_of(ref, count, ss, rs):
        part = ref.at[pl.ds(0, count)]
        return pltpu.make_async_remote_copy(
            src_ref=part, dst_ref=part, send_sem=ss, recv_sem=rs, device_id=(kv, twin), device_id_type=MESH
        )

    for d in (4, 5, 3, 2, 6, 7, 1):
        b_copy(d).start()
    b_recv[tp] = b_send[tp]
    all_of(lat_recv, 15, lat_ss, lat_rs).wait_recv()
    lat_sum = lat_recv[0]
    for k in range(1, 16):
        lat_sum = lat_sum + lat_recv[k]
    loads[8].wait()
    lat_raw = lat_sum[:, :512]
    latent = (
        lat_raw * lax.rsqrt(jnp.mean(lat_raw * lat_raw, axis=1, keepdims=True) + EPSILON) * lgain[...]
    ).astype(BF16).astype(F32)
    key_raw = lat_sum[:, 512:576]
    new_seq = kv // 2
    new_row = tp * 8 + new_seq
    key_swapped = jnp.concatenate([key_raw[:, 32:], key_raw[:, :32]], axis=1)
    new_rope = key_raw * cos_tab[pl.ds(new_row, 1), :] + key_swapped * sin_tab[pl.ds(new_row, 1), :]
    new_rope = new_rope.astype(BF16).astype(F32)
    for s in range(4, 8):
        cache_loads[2 * s].wait()
        keys[s] = cl[s].T
    all_of(b_recv, 7, b_ss, b_rs).wait_recv()

    for copy in value_forwards:
        copy.wait_recv()
        copy.start()

    for h in range(8):
        rows = b_recv[h].astype(F32)
        for i in range(5):
            q_tab[i, 8 * h : 8 * h + 8, :] = rows[:, 128 * i : 128 * i + 128]

    def query_of(s):
        return jnp.concatenate([q_tab[i, pl.ds(s, 8, stride=8), :] for i in range(5)], axis=1)

    for copy in cache_loads[1::2]:
        copy.wait()
    factor = 192.0 ** (-0.5)

    def scores_of(s):
        q = query_of(s).astype(BF16)
        return dot(q[:, :512], keys[s]) + dot(q[:, 512:576], cr[s])

    scores = jnp.concatenate([scores_of(s) for s in range(8)], axis=0) * factor

    q_new = query_of(new_seq)
    new_score = (
        jnp.sum(q_new[:, :512] * latent, axis=1, keepdims=True)
        + jnp.sum(q_new[:, 512:576] * new_rope, axis=1, keepdims=True)
    ) * factor

    row_seq = iota((64, 1), 0) // 8
    row_length = jnp.concatenate(
        [jnp.broadcast_to(len_tab[pl.ds(tp * 8 + s, 1), 0:1], (8, 1)) for s in range(8)], axis=0
    )
    positions = (kv * 512 + iota((64, 512), 1)).astype(F32)
    visible = positions < row_length
    is_new = jnp.logical_and(row_seq == new_seq, kv % 2 == 0)
    own_new = jnp.where(is_new, jnp.concatenate([new_score] * 8, axis=0), NEGATIVE)
    top = jnp.maximum(jnp.max(jnp.where(visible, scores, NEGATIVE), axis=1, keepdims=True), own_new)
    weights = jnp.where(visible, jnp.exp(scores - top), 0.0)
    new_weight = jnp.where(is_new, jnp.exp(own_new - top), 0.0)
    total = jnp.sum(weights, axis=1, keepdims=True) + new_weight
    some = total > 0.0
    safe = jnp.where(some, total, 1.0)
    lse = jnp.where(some, top + jnp.log(safe), NEGATIVE)
    heads = [dot(weights[8 * s : 8 * s + 8].astype(BF16), cl[s]) for s in range(4)]
    heads += [dot(weights[8 * s : 8 * s + 8].astype(BF16), cl[s]) for s in range(4, 8)]
    acc = jnp.concatenate(heads, axis=0) + new_weight.astype(BF16).astype(F32) * latent

    def kv_at(dz, dx):
        return lax.rem(z + dz, 4) * 4 + lax.rem(x + dx, 4)

    others = [(dz, dx) for dz in (2, 1, 3, 0) for dx in (2, 1, 3, 0) if (dz, dx) != (0, 0)]
    l_send[...] = to_row(lse, 64)
    for dz, dx in others:
        pltpu.make_async_remote_copy(
            src_ref=l_send, dst_ref=l_recv.at[kv], send_sem=l_ss, recv_sem=l_rs,
            device_id=(kv_at(dz, dx), tp), device_id_type=MESH,
        ).start()
    l_recv[kv] = l_send[...]

    def gather_wait(buf, ss, rs):
        for d in range(4):
            slot = (twin + 2 * d) % 8
            gather_copy(buf, ss, rs, 0, slot, twin).wait_recv()

    gather_wait(wv, gv_ss, gv_rs)
    by_head = dot(acc.astype(BF16), jnp.concatenate([wv[h] for h in range(8)], axis=1))
    value = by_head[:, 0:128]
    row_head = iota((64, 128), 0) % 8
    for h in range(1, 8):
        value = jnp.where(row_head == h, by_head[:, 128 * h : 128 * h + 128], value)
    value = value / safe

    c_send[...] = value.astype(BF16)

    def c_rows(at_z):
        return c_send.at[pl.ds(pl.multiple_of(at_z * 16, 16), 16)]

    for dz, dx in others:
        pltpu.make_async_remote_copy(
            src_ref=c_rows(lax.rem(z + dz, 4)), dst_ref=c_recv.at[kv], send_sem=c_ss, recv_sem=c_rs,
            device_id=(kv_at(dz, dx), tp), device_id_type=MESH,
        ).start()
    c_recv[kv] = c_send[pl.ds(pl.multiple_of(z * 16, 16), 16), :]

    for d in (1, 3, 2):
        out_z(d, (z + d) % 4).wait_recv()
        out_twin(d, core).start()

    all_of(l_recv, 15, l_ss, l_rs).wait_recv()
    rows = [l_recv[k] for k in range(16)]
    top_row = functools.reduce(jnp.maximum, rows)
    masses = [jnp.exp(row - top_row) for row in rows]
    whole = functools.reduce(jnp.add, masses)
    own_lane = iota((16, 128), 1) == iota((16, 128), 0) + z * 16
    shares = [
        jnp.sum(jnp.where(own_lane, mass / whole, 0.0), axis=1, keepdims=True) for mass in masses
    ]

    all_of(c_recv, 15, c_ss, c_rs).wait_recv()
    terms = [c_recv[k].astype(F32) * shares[k] for k in range(16)]
    while len(terms) > 1:
        terms = [terms[i] + terms[i + 1] for i in range(0, len(terms), 2)]
    merged = terms[0]

    o_tab[...] = merged
    for d in range(4):
        out_twin(d, 1 - core).wait_recv()
    head_out = jnp.concatenate(
        [o_tab[pl.ds(2 * r + c, 2, stride=8), :] for c in range(2) for r in range(4)], axis=1
    ).astype(BF16)
    mixed_z = dot(head_out, jnp.concatenate([wo[k].reshape(1024, 128) for k in range(4)], axis=1))
    for k in range(4):
        m_send[k, :, 0:128] = mixed_z[0:1, 128 * k : 128 * k + 128]
        m_send[k, :, 128:256] = mixed_z[1:2, 128 * k : 128 * k + 128]
    g_send[...] = to_row(jnp.sum(mixed_z * mixed_z, axis=1, keepdims=True), 2)

    pair = tp * 4 + z

    def m_start(dz, dt):
        at_z = lax.rem(z + dz, 4)
        pltpu.make_async_remote_copy(
            src_ref=m_send.at[at_z], dst_ref=m_recv.at[pair], send_sem=m_ss, recv_sem=m_rs,
            device_id=(at_z * 4 + x, lax.rem(tp + dt, 8)), device_id_type=MESH,
        ).start()

    def g_start(dz, dx, dt):
        pltpu.make_async_remote_copy(
            src_ref=g_send, dst_ref=g_recv.at[x * 32 + pair], send_sem=g_ss, recv_sem=g_rs,
            device_id=(kv_at(dz, dx), lax.rem(tp + dt, 8)), device_id_type=MESH,
        ).start()

    steps = [(dz, dx, dt) for dz in (2, 1, 3, 0) for dx in (2, 1, 3, 0) for dt in (4, 5, 3, 2, 6, 7, 1, 0)][:-1]
    hops = [min(dz, 4 - dz) + min(dx, 4 - dx) + min(dt // 2, 4 - dt // 2) for dz, dx, dt in steps]
    for away in (6, 5, 4):
        for step, hop in zip(steps, hops):
            if hop == away:
                g_start(*step)
    for dz in (2, 1, 3, 0):
        for dt in (4, 5, 3, 2, 6, 7, 1, 0):
            if (dz, dt) != (0, 0):
                m_start(dz, dt)
    for away in (3, 2, 1, 0):
        for step, hop in zip(steps, hops):
            if hop == away:
                g_start(*step)
    m_recv[pair] = m_send[z]
    g_recv[x * 32 + pair] = g_send[...]
    loads[11].wait()

    for copy in a1 + a2 + value_sends + value_forwards:
        copy.wait_send()
    for d in range(4):
        out_twin(d, core).wait_send()
    for d in range(1, 4):
        out_y(d, y).wait_send()
        out_z(d, z).wait_send()
    all_of(b_recv, 7, b_ss, b_rs).wait_send()
    all_of(lat_recv, 15, lat_ss, lat_rs).wait_send()
    all_of(l_recv, 15, l_ss, l_rs).wait_send()
    all_of(c_recv, 15, c_ss, c_rs).wait_send()

    all_of(m_recv, 31, m_ss, m_rs).wait_recv()
    all_of(g_recv, 127, g_ss, g_rs).wait_recv()
    octet = iota((8, 128), 0)

    def eight(of):
        row = jnp.broadcast_to(of(0), (8, 128))
        for i in range(1, 8):
            row = jnp.where(octet == i, of(i), row)
        return row

    mixed = jnp.concatenate(
        [
            eight(lambda i: m_recv[4 * v + i // 2, :, 128 * (i % 2) : 128 * (i % 2) + 128])
            for v in range(8)
        ],
        axis=0,
    )
    totals = [g_recv[j] + g_recv[32 + j] + g_recv[64 + j] + g_recv[96 + j] for j in range(32)]
    squares = jnp.concatenate([eight(lambda i: totals[4 * v + i // 2]) for v in range(8)], axis=0)
    picked = iota((64, 128), 0) % 2 == iota((64, 128), 1)
    squares = jnp.sum(jnp.where(picked, squares, 0.0), axis=1, keepdims=True)
    inverse = lax.rsqrt(squares / 2048.0 + EPSILON)
    out_ref[...] = (mixed * inverse * ogain[...]).astype(BF16)

    all_of(m_recv, 31, m_ss, m_rs).wait_send()
    all_of(g_recv, 127, g_ss, g_rs).wait_send()


def on_device(
    tokens, token_gain, w_query, w_down_kv, w_rope_key, latent_gain, w_key_up, w_value_up, w_out, out_gain,
    cache_latent, cache_rope, lengths,
):
    freq = 1.0 / 10000.0 ** (np.arange(0, 64, 2, dtype=np.float32) / np.float32(64.0))
    freq = jnp.asarray(np.tile(freq.astype(np.float32), 4)[None, :])
    operands = (
        tokens, token_gain.reshape(1, 128), w_query.T, w_down_kv, w_rope_key.T, latent_gain.reshape(1, 512),
        w_key_up.reshape(512, 128), w_value_up.reshape(512, 128), w_out, out_gain.reshape(1, 128),
        cache_latent, cache_rope.transpose(0, 2, 1), lengths.reshape(1, 64), freq,
    )
    shapes = [(a.shape, a.dtype) for a in operands]
    shapes[7] = ((8, 512, 128), BF16)
    shapes[8] = ((4, 2, 4, 128, 128), BF16)
    local = [pltpu.VMEM(*a) for a in shapes]
    operands = tuple(pltpu.with_memory_space_constraint(v, pltpu.HBM) for v in operands)
    dma = pltpu.SemaphoreType.DMA
    scratch = local + [
        pltpu.VMEM((64, 128), F32), pltpu.VMEM((64, 64), F32), pltpu.VMEM((64, 64), F32),
        pltpu.VMEM((96, 128), BF16), pltpu.VMEM((3, 96, 128), BF16),
        pltpu.VMEM((96, 128), BF16), pltpu.VMEM((3, 96, 128), BF16),
        pltpu.VMEM((64, 640), F32), pltpu.VMEM((8, 1, 640), F32), pltpu.VMEM((16, 1, 640), F32),
        pltpu.VMEM((128, 512), BF16), pltpu.VMEM((8, 512, 512), BF16),
        pltpu.VMEM((8, 8, 640), BF16), pltpu.VMEM((8, 8, 640), BF16),
        pltpu.VMEM((5, 64, 128), F32), pltpu.VMEM((16, 128), F32),
        pltpu.VMEM((64, 128), BF16), pltpu.VMEM((16, 16, 128), BF16),
        pltpu.VMEM((1, 128), F32), pltpu.VMEM((16, 1, 128), F32),
        pltpu.VMEM((4, 1, 256), F32), pltpu.VMEM((32, 1, 256), F32),
        pltpu.VMEM((1, 128), F32), pltpu.VMEM((128, 1, 128), F32),
        dma((12,)), dma((16,)),
        dma((6,)), dma((6,)), dma((6,)), dma((6,)), dma, dma,
        dma, dma, dma((8,)), dma((8,)),
        dma((4,)), dma((4,)), dma((4,)), dma((4,)), dma((4,)), dma((4,)),
        dma, dma, dma, dma, dma, dma, dma, dma,
    ]
    return pl.pallas_call(
        kernel,
        out_shape=pltpu.VMEM((64, 128), BF16),
        in_specs=[pl.BlockSpec(memory_space=pltpu.HBM)] * len(operands),
        out_specs=pl.BlockSpec(memory_space=pltpu.VMEM),
        scratch_shapes=scratch,
        compiler_params=pltpu.CompilerParams(
            collective_id=0, has_side_effects=True, vmem_limit_bytes=48 * 1024 * 1024
        ),
    )(*operands)


def solution(mesh):
    return jax.shard_map(
        on_device,
        mesh=mesh,
        in_specs=(
            P(None, "kv"), P("kv"), P("kv", "tp"), P("kv", None), P("kv", None), P(),
            P("tp", None, None), P("tp", None, None), P("tp", "kv"), P("kv"),
            P("tp", "kv", None), P("tp", "kv", None), P(),
        ),
        out_specs=P(None, "kv"),
        check_vma=False,
    )
```

```python
import functools

import jax
import jax.numpy as jnp
import numpy as np
from jax import lax
from jax.experimental import pallas as pl
from jax.experimental.pallas import tpu as pltpu
from jax.sharding import PartitionSpec as P

MESH = pl.DeviceIdType.MESH
EPSILON = 1e-06
NEGATIVE = -1e30
BF16 = jnp.bfloat16
F32 = jnp.float32


def dot(a, b):
    return jnp.dot(a, b, preferred_element_type=F32)


def dot_nt(a, b):
    return lax.dot_general(a, b, (((1,), (1,)), ((), ())), preferred_element_type=F32)


def iota(shape, axis):
    return lax.broadcasted_iota(jnp.int32, shape, axis)


def to_column(row, rows):
    picked = iota((rows, rows), 0) == iota((rows, rows), 1)
    return jnp.sum(jnp.where(picked, row[:, :rows], 0.0), axis=1, keepdims=True)


def to_row(column, rows):
    picked = iota((rows, 128), 0) == iota((rows, 128), 1)
    return jnp.sum(jnp.where(picked, column, 0.0), axis=0, keepdims=True)


def kernel(
    tok_h, tgain_h, wq_h, wd_h, wr_h, lgain_h, wk_h, wv_h, wo_h, ogain_h, cl_h, cr_h, len_h, freq_h,
    out_ref,
    tok, tgain, wq, wd, wr, lgain, wk, wv, wo, ogain, cl, cr, lens, freq,
    len_tab, cos_tab, sin_tab,
    a1_send, a1_recv, a2_send, a2_recv,
    lat_all, lat_send, lat_recv,
    wk_turned, keys, b_send, b_recv, q_tab, o_tab,
    c_send, c_recv, l_send, l_recv,
    m_send, m_recv, g_send, g_recv,
    load_sem, cache_sem,
    a1_ss, a1_rs, a2_ss, a2_rs, lat_ss, lat_rs, b_ss, b_rs, gv_ss, gv_rs, oy_ss, oy_rs, oz_ss, oz_rs, ot_ss, ot_rs,
    c_ss, c_rs, l_ss, l_rs, m_ss, m_rs, g_ss, g_rs,
):
    kv = lax.axis_index("kv")
    tp = lax.axis_index("tp")
    z = kv // 4
    x = kv % 4
    y = tp // 2
    core = tp % 2

    pairs = [
        (tok_h, tok), (tgain_h, tgain), (wq_h, wq), (len_h, lens), (freq_h, freq), (wd_h, wd), (wr_h, wr),
        (wk_h, wk), (lgain_h, lgain), (wv_h, wv.at[tp]), (wo_h, wo.at[z, core, y]), (ogain_h, ogain),
    ]
    loads = [pltpu.make_async_copy(s, d, load_sem.at[i]) for i, (s, d) in enumerate(pairs)]
    cache_loads = []
    for s in range(8):
        cache_loads.append(pltpu.make_async_copy(cl_h.at[s], cl.at[s], cache_sem.at[s]))
        cache_loads.append(pltpu.make_async_copy(cr_h.at[s], cr.at[s], cache_sem.at[8 + s]))
    for copy in loads[:3] + loads[9:11]:
        copy.start()
    barrier = pltpu.get_barrier_semaphore()

    def greet(to_kv, to_tp):
        pl.semaphore_signal(barrier, inc=1, device_id=(to_kv, to_tp), device_id_type=MESH)

    for d in (2, 1, 3):
        greet(z * 4 + lax.rem(x + d, 4), tp)
    for d in (2, 1, 3):
        greet(lax.rem(z + d, 4) * 4 + x, tp)
    for d in (4, 5, 3, 2, 6, 7, 1):
        greet(kv, lax.rem(tp + d, 8))

    for i in range(3):
        loads[i].wait()
    scaled = (tok[...].astype(F32) * tgain[...]).astype(BF16)
    q_part = dot_nt(scaled, wq[...])
    rope_part = q_part[:, 128:192]
    q_nope_part = q_part[:, :128]
    q_rope_part = jnp.concatenate([rope_part[:32], rope_part[32:]], axis=1)
    a1_send[0:64, :] = q_nope_part.astype(BF16)
    a1_send[64:96, :] = q_rope_part.astype(BF16)

    for copy in loads[3:9] + loads[11:] + cache_loads:
        copy.start()
    pl.semaphore_wait(barrier, 13)

    def x_dev(d):
        return (z * 4 + (x + d) % 4, tp)

    def z_dev(d):
        return (((z + d) % 4) * 4 + x, tp)

    def line(src, dst, ss, rs, first, second):
        half = src.shape[0] // 2
        copies = []
        for d in (2, 1, 3):
            for k, dev in enumerate((first, second)):
                rows = pl.ds(k * half, half)
                copies.append(
                    pltpu.make_async_remote_copy(
                        src_ref=src.at[rows], dst_ref=dst.at[d - 1, rows],
                        send_sem=ss.at[3 * k + d - 1], recv_sem=rs.at[3 * k + d - 1],
                        device_id=dev(d), device_id_type=MESH,
                    )
                )
        return copies

    def line1(src, dst, ss, rs, dev):
        return [
            pltpu.make_async_remote_copy(
                src_ref=src, dst_ref=dst.at[d - 1], send_sem=ss.at[d - 1], recv_sem=rs.at[d - 1],
                device_id=dev(d), device_id_type=MESH,
            )
            for d in (1, 2, 3)
        ]

    a1 = line(a1_send, a1_recv, a1_ss, a1_rs, x_dev, z_dev)
    for copy in a1:
        copy.start()

    twin = tp + 1 - 2 * core

    def gather_copy(buf, ss, rs, i, slot, to):
        return pltpu.make_async_remote_copy(
            src_ref=buf.at[slot], dst_ref=buf.at[slot], send_sem=ss.at[i], recv_sem=rs.at[slot],
            device_id=(kv, to), device_id_type=MESH,
        )

    def gather_first(buf, ss, rs):
        copies = [gather_copy(buf, ss, rs, i, tp, (tp + 2 * d) % 8) for i, d in enumerate((2, 1, 3))]
        return copies + [gather_copy(buf, ss, rs, 3, tp, twin)]

    def gather_forward(buf, ss, rs):
        slots = [(tp + 2 * d) % 8 for d in (1, 3, 2)]
        return [gather_copy(buf, ss, rs, 4 + i, slot, twin) for i, slot in enumerate(slots)]

    loads[9].wait()
    loads[10].wait()
    value_sends = gather_first(wv, gv_ss, gv_rs)
    value_forwards = gather_forward(wv, gv_ss, gv_rs)

    def out_y(d, at):
        return pltpu.make_async_remote_copy(
            src_ref=wo.at[z, core, y], dst_ref=wo.at[z, core, at], send_sem=oy_ss.at[d], recv_sem=oy_rs.at[at],
            device_id=(kv, (tp + 2 * d) % 8), device_id_type=MESH,
        )

    def out_z(d, at):
        return pltpu.make_async_remote_copy(
            src_ref=wo.at[z, core], dst_ref=wo.at[at, core], send_sem=oz_ss.at[d], recv_sem=oz_rs.at[at],
            device_id=((z + d) % 4 * 4 + x, tp), device_id_type=MESH,
        )

    def out_twin(d, half):
        at = (z + d) % 4
        return pltpu.make_async_remote_copy(
            src_ref=wo.at[at, core], dst_ref=wo.at[at, half], send_sem=ot_ss.at[d], recv_sem=ot_rs.at[at],
            device_id=(kv, twin), device_id_type=MESH,
        )

    for d in (2, 1, 3):
        out_y(d, y).start()
    for copy in value_sends:
        copy.start()

    for i in range(3, 7):
        loads[i].wait()
    lat_all[:, 0:512] = dot(scaled, wd[...])
    lat_all[:, 512:576] = dot_nt(scaled, wr[...])
    lat_all[:, 576:640] = jnp.zeros((64, 64), F32)
    mine = lat_all[pl.ds(pl.multiple_of(tp * 8, 8), 8), :]
    for r in range(8):
        lat_send[r] = mine[r : r + 1, :]
    lat_recv[kv] = lat_send[kv // 2]

    def lat_copy(dz, dx):
        at_z = lax.rem(z + dz, 4)
        at_x = lax.rem(x + dx, 4)
        return pltpu.make_async_remote_copy(
            src_ref=lat_send.at[at_z * 2 + at_x // 2], dst_ref=lat_recv.at[kv], send_sem=lat_ss, recv_sem=lat_rs,
            device_id=(at_z * 4 + at_x, tp), device_id_type=MESH,
        )

    len_col = to_column(lens[...].astype(F32), 64)
    len_tab[...] = jnp.broadcast_to(len_col, (64, 128))
    lane = iota((32, 128), 1)
    packed_len = jnp.where(lane < 64, len_col[:32], len_col[32:])
    angle = packed_len * freq[...]
    cosine = jnp.cos(angle)
    sine = jnp.sin(angle)
    sine = jnp.where(lane % 64 < 32, -sine, sine)
    cos_tab[0:32, :] = cosine[:, :64]
    cos_tab[32:64, :] = cosine[:, 64:]
    sin_tab[0:32, :] = sine[:, :64]
    sin_tab[32:64, :] = sine[:, 64:]

    def added(own, recv, rows):
        total = own
        for d in range(3):
            total = total + recv[d, rows, :].astype(F32)
        return total

    for copy in a1:
        copy.wait_recv()
    q_nope_sum = added(q_nope_part, a1_recv, slice(0, 64))
    q_rope_sum = added(q_rope_part, a1_recv, slice(64, 96))
    a2_send[0:64, :] = q_nope_sum.astype(BF16)
    a2_send[64:96, :] = q_rope_sum.astype(BF16)
    a2 = line(a2_send, a2_recv, a2_ss, a2_rs, z_dev, x_dev)
    for copy in a2:
        copy.start()
    for dz in (2, 1, 3, 0):
        for dx in (2, 1, 3, 0):
            if (dz, dx) != (0, 0):
                lat_copy(dz, dx).start()
    loads[7].wait()
    wk_turned[...] = wk[...].T
    for s in range(4):
        cache_loads[2 * s].wait()
        keys[s] = cl[s].T
    for copy in a2:
        copy.wait_recv()
    q_nope = added(q_nope_sum, a2_recv, slice(0, 64)).astype(BF16)
    q_rope = added(q_rope_sum, a2_recv, slice(64, 96)).astype(BF16).astype(F32)
    swapped = jnp.where(lane % 64 < 32, pltpu.roll(q_rope, 96, 1), pltpu.roll(q_rope, 32, 1))
    q_rope = q_rope * cosine + swapped * sine
    q_rope = jnp.concatenate([q_rope[:, :64], q_rope[:, 64:]], axis=0)


    for d in (1, 3, 2):
        out_y(d, (y + d) % 4).wait_recv()
    for d in (2, 1, 3):
        out_z(d, z).start()
    out_twin(0, core).start()
    q_lat = dot(q_nope, wk_turned[...])
    pad = jnp.zeros((8, 64), F32)
    for j in range(8):
        block = jnp.concatenate([q_lat[8 * j : 8 * j + 8], q_rope[8 * j : 8 * j + 8], pad], axis=1)
        b_send[j] = block.astype(BF16)

    def b_copy(d):
        to = (tp + d) % 8
        return pltpu.make_async_remote_copy(
            src_ref=b_send.at[to], dst_ref=b_recv.at[tp], send_sem=b_ss, recv_sem=b_rs,
            device_id=(kv, to), device_id_type=MESH,
        )

    def all_of(ref, count, ss, rs):
        part = ref.at[pl.ds(0, count)]
        return pltpu.make_async_remote_copy(
            src_ref=part, dst_ref=part, send_sem=ss, recv_sem=rs, device_id=(kv, twin), device_id_type=MESH
        )

    for d in (4, 5, 3, 2, 6, 7, 1):
        b_copy(d).start()
    b_recv[tp] = b_send[tp]
    all_of(lat_recv, 15, lat_ss, lat_rs).wait_recv()
    lat_sum = lat_recv[0]
    for k in range(1, 16):
        lat_sum = lat_sum + lat_recv[k]
    loads[8].wait()
    lat_raw = lat_sum[:, :512]
    latent = (
        lat_raw * lax.rsqrt(jnp.mean(lat_raw * lat_raw, axis=1, keepdims=True) + EPSILON) * lgain[...]
    ).astype(BF16).astype(F32)
    key_raw = lat_sum[:, 512:576]
    new_seq = kv // 2
    new_row = tp * 8 + new_seq
    key_swapped = jnp.concatenate([key_raw[:, 32:], key_raw[:, :32]], axis=1)
    new_rope = key_raw * cos_tab[pl.ds(new_row, 1), :] + key_swapped * sin_tab[pl.ds(new_row, 1), :]
    new_rope = new_rope.astype(BF16).astype(F32)
    for s in range(4, 8):
        cache_loads[2 * s].wait()
        keys[s] = cl[s].T
    all_of(b_recv, 7, b_ss, b_rs).wait_recv()

    for copy in value_forwards:
        copy.wait_recv()
        copy.start()

    for h in range(8):
        rows = b_recv[h].astype(F32)
        for i in range(5):
            q_tab[i, 8 * h : 8 * h + 8, :] = rows[:, 128 * i : 128 * i + 128]

    def query_of(s):
        return jnp.concatenate([q_tab[i, pl.ds(s, 8, stride=8), :] for i in range(5)], axis=1)

    for copy in cache_loads[1::2]:
        copy.wait()
    factor = 192.0 ** (-0.5)

    def scores_of(s):
        q = query_of(s).astype(BF16)
        return dot(q[:, :512], keys[s]) + dot(q[:, 512:576], cr[s])

    scores = jnp.concatenate([scores_of(s) for s in range(8)], axis=0) * factor

    q_new = query_of(new_seq)
    new_score = (
        jnp.sum(q_new[:, :512] * latent, axis=1, keepdims=True)
        + jnp.sum(q_new[:, 512:576] * new_rope, axis=1, keepdims=True)
    ) * factor

    row_seq = iota((64, 1), 0) // 8
    row_length = jnp.concatenate(
        [jnp.broadcast_to(len_tab[pl.ds(tp * 8 + s, 1), 0:1], (8, 1)) for s in range(8)], axis=0
    )
    positions = (kv * 512 + iota((64, 512), 1)).astype(F32)
    visible = positions < row_length
    is_new = jnp.logical_and(row_seq == new_seq, kv % 2 == 0)
    own_new = jnp.where(is_new, jnp.concatenate([new_score] * 8, axis=0), NEGATIVE)
    top = jnp.maximum(jnp.max(jnp.where(visible, scores, NEGATIVE), axis=1, keepdims=True), own_new)
    weights = jnp.where(visible, jnp.exp(scores - top), 0.0)
    new_weight = jnp.where(is_new, jnp.exp(own_new - top), 0.0)
    total = jnp.sum(weights, axis=1, keepdims=True) + new_weight
    some = total > 0.0
    safe = jnp.where(some, total, 1.0)
    lse = jnp.where(some, top + jnp.log(safe), NEGATIVE)
    heads = [dot(weights[8 * s : 8 * s + 8].astype(BF16), cl[s]) for s in range(4)]
    heads += [dot(weights[8 * s : 8 * s + 8].astype(BF16), cl[s]) for s in range(4, 8)]
    acc = jnp.concatenate(heads, axis=0) + new_weight.astype(BF16).astype(F32) * latent

    def kv_at(dz, dx):
        return lax.rem(z + dz, 4) * 4 + lax.rem(x + dx, 4)

    others = [(dz, dx) for dz in (2, 1, 3, 0) for dx in (2, 1, 3, 0) if (dz, dx) != (0, 0)]
    l_send[...] = to_row(lse, 64)
    for dz, dx in others:
        pltpu.make_async_remote_copy(
            src_ref=l_send, dst_ref=l_recv.at[kv], send_sem=l_ss, recv_sem=l_rs,
            device_id=(kv_at(dz, dx), tp), device_id_type=MESH,
        ).start()
    l_recv[kv] = l_send[...]

    def gather_wait(buf, ss, rs):
        for d in range(4):
            slot = (twin + 2 * d) % 8
            gather_copy(buf, ss, rs, 0, slot, twin).wait_recv()

    gather_wait(wv, gv_ss, gv_rs)
    by_head = dot(acc.astype(BF16), jnp.concatenate([wv[h] for h in range(8)], axis=1))
    value = by_head[:, 0:128]
    row_head = iota((64, 128), 0) % 8
    for h in range(1, 8):
        value = jnp.where(row_head == h, by_head[:, 128 * h : 128 * h + 128], value)
    value = value / safe

    c_send[...] = value.astype(BF16)

    def c_rows(at_z):
        return c_send.at[pl.ds(pl.multiple_of(at_z * 16, 16), 16)]

    for dz, dx in others:
        pltpu.make_async_remote_copy(
            src_ref=c_rows(lax.rem(z + dz, 4)), dst_ref=c_recv.at[kv], send_sem=c_ss, recv_sem=c_rs,
            device_id=(kv_at(dz, dx), tp), device_id_type=MESH,
        ).start()
    c_recv[kv] = c_send[pl.ds(pl.multiple_of(z * 16, 16), 16), :]

    for d in (1, 3, 2):
        out_z(d, (z + d) % 4).wait_recv()
        out_twin(d, core).start()

    all_of(l_recv, 15, l_ss, l_rs).wait_recv()
    rows = [l_recv[k] for k in range(16)]
    top_row = functools.reduce(jnp.maximum, rows)
    masses = [jnp.exp(row - top_row) for row in rows]
    whole = functools.reduce(jnp.add, masses)
    own_lane = iota((16, 128), 1) == iota((16, 128), 0) + z * 16
    shares = [
        jnp.sum(jnp.where(own_lane, mass / whole, 0.0), axis=1, keepdims=True) for mass in masses
    ]

    all_of(c_recv, 15, c_ss, c_rs).wait_recv()
    terms = [c_recv[k].astype(F32) * shares[k] for k in range(16)]
    while len(terms) > 1:
        terms = [terms[i] + terms[i + 1] for i in range(0, len(terms), 2)]
    merged = terms[0]

    o_tab[...] = merged
    for d in range(4):
        out_twin(d, 1 - core).wait_recv()
    head_out = jnp.concatenate(
        [o_tab[pl.ds(2 * r + c, 2, stride=8), :] for c in range(2) for r in range(4)], axis=1
    ).astype(BF16)
    mixed_z = dot(head_out, jnp.concatenate([wo[k].reshape(1024, 128) for k in range(4)], axis=1))
    for k in range(4):
        m_send[k, :, 0:128] = mixed_z[0:1, 128 * k : 128 * k + 128]
        m_send[k, :, 128:256] = mixed_z[1:2, 128 * k : 128 * k + 128]
    g_send[...] = to_row(jnp.sum(mixed_z * mixed_z, axis=1, keepdims=True), 2)

    pair = tp * 4 + z

    def m_start(dz, dt):
        at_z = lax.rem(z + dz, 4)
        pltpu.make_async_remote_copy(
            src_ref=m_send.at[at_z], dst_ref=m_recv.at[pair], send_sem=m_ss, recv_sem=m_rs,
            device_id=(at_z * 4 + x, lax.rem(tp + dt, 8)), device_id_type=MESH,
        ).start()

    def g_start(dz, dx, dt):
        pltpu.make_async_remote_copy(
            src_ref=g_send, dst_ref=g_recv.at[x * 32 + pair], send_sem=g_ss, recv_sem=g_rs,
            device_id=(kv_at(dz, dx), lax.rem(tp + dt, 8)), device_id_type=MESH,
        ).start()

    steps = [(dz, dx, dt) for dz in (2, 1, 3, 0) for dx in (2, 1, 3, 0) for dt in (4, 5, 3, 2, 6, 7, 1, 0)][:-1]
    hops = [min(dz, 4 - dz) + min(dx, 4 - dx) + min(dt // 2, 4 - dt // 2) for dz, dx, dt in steps]
    for away in (6, 5, 4):
        for step, hop in zip(steps, hops):
            if hop == away:
                g_start(*step)
    for dz in (2, 1, 3, 0):
        for dt in (4, 5, 3, 2, 6, 7, 1, 0):
            if (dz, dt) != (0, 0):
                m_start(dz, dt)
    for away in (3, 2, 1, 0):
        for step, hop in zip(steps, hops):
            if hop == away:
                g_start(*step)
    m_recv[pair] = m_send[z]
    g_recv[x * 32 + pair] = g_send[...]
    loads[11].wait()

    for copy in a1 + a2 + value_sends + value_forwards:
        copy.wait_send()
    for d in range(4):
        out_twin(d, core).wait_send()
    for d in range(1, 4):
        out_y(d, y).wait_send()
        out_z(d, z).wait_send()
    all_of(b_recv, 7, b_ss, b_rs).wait_send()
    all_of(lat_recv, 15, lat_ss, lat_rs).wait_send()
    all_of(l_recv, 15, l_ss, l_rs).wait_send()
    all_of(c_recv, 15, c_ss, c_rs).wait_send()

    all_of(m_recv, 31, m_ss, m_rs).wait_recv()
    all_of(g_recv, 127, g_ss, g_rs).wait_recv()
    octet = iota((8, 128), 0)

    def eight(of):
        row = jnp.broadcast_to(of(0), (8, 128))
        for i in range(1, 8):
            row = jnp.where(octet == i, of(i), row)
        return row

    mixed = jnp.concatenate(
        [
            eight(lambda i: m_recv[4 * v + i // 2, :, 128 * (i % 2) : 128 * (i % 2) + 128])
            for v in range(8)
        ],
        axis=0,
    )
    totals = [g_recv[j] + g_recv[32 + j] + g_recv[64 + j] + g_recv[96 + j] for j in range(32)]
    squares = jnp.concatenate([eight(lambda i: totals[4 * v + i // 2]) for v in range(8)], axis=0)
    picked = iota((64, 128), 0) % 2 == iota((64, 128), 1)
    squares = jnp.sum(jnp.where(picked, squares, 0.0), axis=1, keepdims=True)
    inverse = lax.rsqrt(squares / 2048.0 + EPSILON)
    out_ref[...] = (mixed * inverse * ogain[...]).astype(BF16)

    all_of(m_recv, 31, m_ss, m_rs).wait_send()
    all_of(g_recv, 127, g_ss, g_rs).wait_send()


def on_device(
    tokens, token_gain, w_query, w_down_kv, w_rope_key, latent_gain, w_key_up, w_value_up, w_out, out_gain,
    cache_latent, cache_rope, lengths,
):
    freq = 1.0 / 10000.0 ** (np.arange(0, 64, 2, dtype=np.float32) / np.float32(64.0))
    freq = jnp.asarray(np.tile(freq.astype(np.float32), 4)[None, :])
    operands = (
        tokens, token_gain.reshape(1, 128), w_query.T, w_down_kv, w_rope_key.T, latent_gain.reshape(1, 512),
        w_key_up.reshape(512, 128), w_value_up.reshape(512, 128), w_out, out_gain.reshape(1, 128),
        cache_latent, cache_rope.transpose(0, 2, 1), lengths.reshape(1, 64), freq,
    )
    shapes = [(a.shape, a.dtype) for a in operands]
    shapes[7] = ((8, 512, 128), BF16)
    shapes[8] = ((4, 2, 4, 128, 128), BF16)
    local = [pltpu.VMEM(*a) for a in shapes]
    operands = tuple(pltpu.with_memory_space_constraint(v, pltpu.HBM) for v in operands)
    dma = pltpu.SemaphoreType.DMA
    scratch = local + [
        pltpu.VMEM((64, 128), F32), pltpu.VMEM((64, 64), F32), pltpu.VMEM((64, 64), F32),
        pltpu.VMEM((96, 128), BF16), pltpu.VMEM((3, 96, 128), BF16),
        pltpu.VMEM((96, 128), BF16), pltpu.VMEM((3, 96, 128), BF16),
        pltpu.VMEM((64, 640), F32), pltpu.VMEM((8, 1, 640), F32), pltpu.VMEM((16, 1, 640), F32),
        pltpu.VMEM((128, 512), BF16), pltpu.VMEM((8, 512, 512), BF16),
        pltpu.VMEM((8, 8, 640), BF16), pltpu.VMEM((8, 8, 640), BF16),
        pltpu.VMEM((5, 64, 128), F32), pltpu.VMEM((16, 128), F32),
        pltpu.VMEM((64, 128), BF16), pltpu.VMEM((16, 16, 128), BF16),
        pltpu.VMEM((1, 128), F32), pltpu.VMEM((16, 1, 128), F32),
        pltpu.VMEM((4, 1, 256), F32), pltpu.VMEM((32, 1, 256), F32),
        pltpu.VMEM((1, 128), F32), pltpu.VMEM((128, 1, 128), F32),
        dma((12,)), dma((16,)),
        dma((6,)), dma((6,)), dma((6,)), dma((6,)), dma, dma,
        dma, dma, dma((8,)), dma((8,)),
        dma((4,)), dma((4,)), dma((4,)), dma((4,)), dma((4,)), dma((4,)),
        dma, dma, dma, dma, dma, dma, dma, dma,
    ]
    return pl.pallas_call(
        kernel,
        out_shape=pltpu.VMEM((64, 128), BF16),
        in_specs=[pl.BlockSpec(memory_space=pltpu.HBM)] * len(operands),
        out_specs=pl.BlockSpec(memory_space=pltpu.VMEM),
        scratch_shapes=scratch,
        compiler_params=pltpu.CompilerParams(
            collective_id=0, has_side_effects=True, vmem_limit_bytes=48 * 1024 * 1024
        ),
    )(*operands)


def solution(mesh):
    return jax.shard_map(
        on_device,
        mesh=mesh,
        in_specs=(
            P(None, "kv"), P("kv"), P("kv", "tp"), P("kv", None), P("kv", None), P(),
            P("tp", None, None), P("tp", None, None), P("tp", "kv"), P("kv"),
            P("tp", "kv", None), P("tp", "kv", None), P(),
        ),
        out_specs=P(None, "kv"),
        check_vma=False,
    )
```

```python
import functools

import jax
import jax.numpy as jnp
import numpy as np
from jax import lax
from jax.experimental import pallas as pl
from jax.experimental.pallas import tpu as pltpu
from jax.sharding import PartitionSpec as P

MESH = pl.DeviceIdType.MESH
EPSILON = 1e-06
NEGATIVE = -1e30
BF16 = jnp.bfloat16
F32 = jnp.float32


def dot(a, b):
    return jnp.dot(a, b, preferred_element_type=F32)


def dot_nt(a, b):
    return lax.dot_general(a, b, (((1,), (1,)), ((), ())), preferred_element_type=F32)


def iota(shape, axis):
    return lax.broadcasted_iota(jnp.int32, shape, axis)


def to_column(row, rows):
    picked = iota((rows, rows), 0) == iota((rows, rows), 1)
    return jnp.sum(jnp.where(picked, row[:, :rows], 0.0), axis=1, keepdims=True)


def to_row(column, rows):
    picked = iota((rows, 128), 0) == iota((rows, 128), 1)
    return jnp.sum(jnp.where(picked, column, 0.0), axis=0, keepdims=True)


def kernel(
    tok_h, tgain_h, wq_h, wd_h, wr_h, lgain_h, wk_h, wv_h, wo_h, ogain_h, cl_h, cr_h, len_h, freq_h,
    out_ref,
    tok, tgain, wq, wd, wr, lgain, wk, wv, wo, ogain, cl, cr, lens, freq,
    len_tab, cos_tab, sin_tab,
    a1_send, a1_recv, a2_send, a2_recv,
    lat_all, lat_send, lat_recv,
    wk_turned, keys, b_send, b_recv, q_tab, o_tab,
    c_send, c_recv, l_send, l_recv,
    m_send, m_recv, g_send, g_recv,
    load_sem, cache_sem,
    a1_ss, a1_rs, a2_ss, a2_rs, lat_ss, lat_rs, b_ss, b_rs, gv_ss, gv_rs, oy_ss, oy_rs, oz_ss, oz_rs, ot_ss, ot_rs,
    c_ss, c_rs, l_ss, l_rs, m_ss, m_rs, g_ss, g_rs,
):
    kv = lax.axis_index("kv")
    tp = lax.axis_index("tp")
    z = kv // 4
    x = kv % 4
    y = tp // 2
    core = tp % 2

    pairs = [
        (tok_h, tok), (tgain_h, tgain), (wq_h, wq), (len_h, lens), (freq_h, freq), (wd_h, wd), (wr_h, wr),
        (wk_h, wk), (lgain_h, lgain), (wv_h, wv.at[tp]), (wo_h, wo.at[z, core, y]), (ogain_h, ogain),
    ]
    loads = [pltpu.make_async_copy(s, d, load_sem.at[i]) for i, (s, d) in enumerate(pairs)]
    cache_loads = []
    for s in range(8):
        cache_loads.append(pltpu.make_async_copy(cl_h.at[s], cl.at[s], cache_sem.at[s]))
        cache_loads.append(pltpu.make_async_copy(cr_h.at[s], cr.at[s], cache_sem.at[8 + s]))
    barrier = pltpu.get_barrier_semaphore()

    def greet(to_kv, to_tp):
        pl.semaphore_signal(barrier, inc=1, device_id=(to_kv, to_tp), device_id_type=MESH)

    for d in (2, 1, 3):
        greet(z * 4 + lax.rem(x + d, 4), tp)
        greet(lax.rem(z + d, 4) * 4 + x, tp)
    for d in (4, 5, 3, 2, 6, 7, 1):
        greet(kv, lax.rem(tp + d, 8))
    for copy in loads[:3] + loads[9:11]:
        copy.start()

    for i in range(3):
        loads[i].wait()
    scaled = (tok[...].astype(F32) * tgain[...]).astype(BF16)
    q_part = dot_nt(scaled, wq[...])
    rope_part = q_part[:, 128:192]
    q_nope_part = q_part[:, :128]
    q_rope_part = jnp.concatenate([rope_part[:32], rope_part[32:]], axis=1)
    a1_send[0:64, :] = q_nope_part.astype(BF16)
    a1_send[64:96, :] = q_rope_part.astype(BF16)

    for copy in loads[3:9] + loads[11:] + cache_loads:
        copy.start()
    pl.semaphore_wait(barrier, 13)

    def x_dev(d):
        return (z * 4 + (x + d) % 4, tp)

    def z_dev(d):
        return (((z + d) % 4) * 4 + x, tp)

    def line(src, dst, ss, rs, first, second):
        half = src.shape[0] // 2
        copies = []
        for d in (2, 1, 3):
            for k, dev in enumerate((first, second)):
                rows = pl.ds(k * half, half)
                copies.append(
                    pltpu.make_async_remote_copy(
                        src_ref=src.at[rows], dst_ref=dst.at[d - 1, rows],
                        send_sem=ss.at[3 * k + d - 1], recv_sem=rs.at[3 * k + d - 1],
                        device_id=dev(d), device_id_type=MESH,
                    )
                )
        return copies

    def line1(src, dst, ss, rs, dev):
        return [
            pltpu.make_async_remote_copy(
                src_ref=src, dst_ref=dst.at[d - 1], send_sem=ss.at[d - 1], recv_sem=rs.at[d - 1],
                device_id=dev(d), device_id_type=MESH,
            )
            for d in (1, 2, 3)
        ]

    a1 = line(a1_send, a1_recv, a1_ss, a1_rs, x_dev, z_dev)
    for copy in a1:
        copy.start()

    twin = tp + 1 - 2 * core

    def gather_copy(buf, ss, rs, i, slot, to):
        return pltpu.make_async_remote_copy(
            src_ref=buf.at[slot], dst_ref=buf.at[slot], send_sem=ss.at[i], recv_sem=rs.at[slot],
            device_id=(kv, to), device_id_type=MESH,
        )

    def gather_first(buf, ss, rs):
        copies = [gather_copy(buf, ss, rs, i, tp, (tp + 2 * d) % 8) for i, d in enumerate((2, 1, 3))]
        return copies + [gather_copy(buf, ss, rs, 3, tp, twin)]

    def gather_forward(buf, ss, rs):
        slots = [(tp + 2 * d) % 8 for d in (1, 3, 2)]
        return [gather_copy(buf, ss, rs, 4 + i, slot, twin) for i, slot in enumerate(slots)]

    loads[9].wait()
    loads[10].wait()
    value_sends = gather_first(wv, gv_ss, gv_rs)
    value_forwards = gather_forward(wv, gv_ss, gv_rs)

    def out_y(d, at):
        return pltpu.make_async_remote_copy(
            src_ref=wo.at[z, core, y], dst_ref=wo.at[z, core, at], send_sem=oy_ss.at[d], recv_sem=oy_rs.at[at],
            device_id=(kv, (tp + 2 * d) % 8), device_id_type=MESH,
        )

    def out_z(d, at):
        return pltpu.make_async_remote_copy(
            src_ref=wo.at[z, core], dst_ref=wo.at[at, core], send_sem=oz_ss.at[d], recv_sem=oz_rs.at[at],
            device_id=((z + d) % 4 * 4 + x, tp), device_id_type=MESH,
        )

    def out_twin(d, half):
        at = (z + d) % 4
        return pltpu.make_async_remote_copy(
            src_ref=wo.at[at, core], dst_ref=wo.at[at, half], send_sem=ot_ss.at[d], recv_sem=ot_rs.at[at],
            device_id=(kv, twin), device_id_type=MESH,
        )

    for d in (2, 1, 3):
        out_y(d, y).start()
    for copy in value_sends:
        copy.start()

    for i in range(3, 7):
        loads[i].wait()
    lat_all[:, 0:512] = dot(scaled, wd[...])
    lat_all[:, 512:576] = dot_nt(scaled, wr[...])
    lat_all[:, 576:640] = jnp.zeros((64, 64), F32)
    mine = lat_all[pl.ds(pl.multiple_of(tp * 8, 8), 8), :]
    for r in range(8):
        lat_send[r] = mine[r : r + 1, :]
    lat_recv[kv] = lat_send[kv // 2]

    def lat_copy(dz, dx):
        at_z = lax.rem(z + dz, 4)
        at_x = lax.rem(x + dx, 4)
        return pltpu.make_async_remote_copy(
            src_ref=lat_send.at[at_z * 2 + at_x // 2], dst_ref=lat_recv.at[kv], send_sem=lat_ss, recv_sem=lat_rs,
            device_id=(at_z * 4 + at_x, tp), device_id_type=MESH,
        )

    len_col = to_column(lens[...].astype(F32), 64)
    len_tab[...] = jnp.broadcast_to(len_col, (64, 128))
    lane = iota((32, 128), 1)
    packed_len = jnp.where(lane < 64, len_col[:32], len_col[32:])
    angle = packed_len * freq[...]
    cosine = jnp.cos(angle)
    sine = jnp.sin(angle)
    sine = jnp.where(lane % 64 < 32, -sine, sine)
    cos_tab[0:32, :] = cosine[:, :64]
    cos_tab[32:64, :] = cosine[:, 64:]
    sin_tab[0:32, :] = sine[:, :64]
    sin_tab[32:64, :] = sine[:, 64:]

    def added(own, recv, rows):
        total = own
        for d in range(3):
            total = total + recv[d, rows, :].astype(F32)
        return total

    for copy in a1:
        copy.wait_recv()
    q_nope_sum = added(q_nope_part, a1_recv, slice(0, 64))
    q_rope_sum = added(q_rope_part, a1_recv, slice(64, 96))
    a2_send[0:64, :] = q_nope_sum.astype(BF16)
    a2_send[64:96, :] = q_rope_sum.astype(BF16)
    a2 = line(a2_send, a2_recv, a2_ss, a2_rs, z_dev, x_dev)
    for copy in a2:
        copy.start()
    for dz in (2, 1, 3, 0):
        for dx in (2, 1, 3, 0):
            if (dz, dx) != (0, 0):
                lat_copy(dz, dx).start()
    loads[7].wait()
    wk_turned[...] = wk[...].T
    for s in range(4):
        cache_loads[2 * s].wait()
        keys[s] = cl[s].T
    for copy in a2:
        copy.wait_recv()
    q_nope = added(q_nope_sum, a2_recv, slice(0, 64)).astype(BF16)
    q_rope = added(q_rope_sum, a2_recv, slice(64, 96)).astype(BF16).astype(F32)
    swapped = jnp.where(lane % 64 < 32, pltpu.roll(q_rope, 96, 1), pltpu.roll(q_rope, 32, 1))
    q_rope = q_rope * cosine + swapped * sine
    q_rope = jnp.concatenate([q_rope[:, :64], q_rope[:, 64:]], axis=0)


    for d in (1, 3, 2):
        out_y(d, (y + d) % 4).wait_recv()
    for d in (2, 1, 3):
        out_z(d, z).start()
    out_twin(0, core).start()
    q_lat = dot(q_nope, wk_turned[...])
    pad = jnp.zeros((8, 64), F32)
    for j in range(8):
        block = jnp.concatenate([q_lat[8 * j : 8 * j + 8], q_rope[8 * j : 8 * j + 8], pad], axis=1)
        b_send[j] = block.astype(BF16)

    def b_copy(d):
        to = (tp + d) % 8
        return pltpu.make_async_remote_copy(
            src_ref=b_send.at[to], dst_ref=b_recv.at[tp], send_sem=b_ss, recv_sem=b_rs,
            device_id=(kv, to), device_id_type=MESH,
        )

    def all_of(ref, count, ss, rs):
        part = ref.at[pl.ds(0, count)]
        return pltpu.make_async_remote_copy(
            src_ref=part, dst_ref=part, send_sem=ss, recv_sem=rs, device_id=(kv, twin), device_id_type=MESH
        )

    for d in (4, 5, 3, 2, 6, 7, 1):
        b_copy(d).start()
    b_recv[tp] = b_send[tp]
    all_of(lat_recv, 15, lat_ss, lat_rs).wait_recv()
    lat_sum = lat_recv[0]
    for k in range(1, 16):
        lat_sum = lat_sum + lat_recv[k]
    loads[8].wait()
    lat_raw = lat_sum[:, :512]
    latent = (
        lat_raw * lax.rsqrt(jnp.mean(lat_raw * lat_raw, axis=1, keepdims=True) + EPSILON) * lgain[...]
    ).astype(BF16).astype(F32)
    key_raw = lat_sum[:, 512:576]
    new_seq = kv // 2
    new_row = tp * 8 + new_seq
    key_swapped = jnp.concatenate([key_raw[:, 32:], key_raw[:, :32]], axis=1)
    new_rope = key_raw * cos_tab[pl.ds(new_row, 1), :] + key_swapped * sin_tab[pl.ds(new_row, 1), :]
    new_rope = new_rope.astype(BF16).astype(F32)
    for s in range(4, 8):
        cache_loads[2 * s].wait()
        keys[s] = cl[s].T
    all_of(b_recv, 7, b_ss, b_rs).wait_recv()

    for copy in value_forwards:
        copy.wait_recv()
        copy.start()

    for h in range(8):
        rows = b_recv[h].astype(F32)
        for i in range(5):
            q_tab[i, 8 * h : 8 * h + 8, :] = rows[:, 128 * i : 128 * i + 128]

    def query_of(s):
        return jnp.concatenate([q_tab[i, pl.ds(s, 8, stride=8), :] for i in range(5)], axis=1)

    for copy in cache_loads[1::2]:
        copy.wait()
    factor = 192.0 ** (-0.5)

    def scores_of(s):
        q = query_of(s).astype(BF16)
        return dot(q[:, :512], keys[s]) + dot(q[:, 512:576], cr[s])

    scores = jnp.concatenate([scores_of(s) for s in range(8)], axis=0) * factor

    q_new = query_of(new_seq)
    new_score = (
        jnp.sum(q_new[:, :512] * latent, axis=1, keepdims=True)
        + jnp.sum(q_new[:, 512:576] * new_rope, axis=1, keepdims=True)
    ) * factor

    row_seq = iota((64, 1), 0) // 8
    row_length = jnp.concatenate(
        [jnp.broadcast_to(len_tab[pl.ds(tp * 8 + s, 1), 0:1], (8, 1)) for s in range(8)], axis=0
    )
    positions = (kv * 512 + iota((64, 512), 1)).astype(F32)
    visible = positions < row_length
    is_new = jnp.logical_and(row_seq == new_seq, kv % 2 == 0)
    own_new = jnp.where(is_new, jnp.concatenate([new_score] * 8, axis=0), NEGATIVE)
    top = jnp.maximum(jnp.max(jnp.where(visible, scores, NEGATIVE), axis=1, keepdims=True), own_new)
    weights = jnp.where(visible, jnp.exp(scores - top), 0.0)
    new_weight = jnp.where(is_new, jnp.exp(own_new - top), 0.0)
    total = jnp.sum(weights, axis=1, keepdims=True) + new_weight
    some = total > 0.0
    safe = jnp.where(some, total, 1.0)
    lse = jnp.where(some, top + jnp.log(safe), NEGATIVE)
    heads = [dot(weights[8 * s : 8 * s + 8].astype(BF16), cl[s]) for s in range(4)]
    heads += [dot(weights[8 * s : 8 * s + 8].astype(BF16), cl[s]) for s in range(4, 8)]
    acc = jnp.concatenate(heads, axis=0) + new_weight.astype(BF16).astype(F32) * latent

    def kv_at(dz, dx):
        return lax.rem(z + dz, 4) * 4 + lax.rem(x + dx, 4)

    others = [(dz, dx) for dz in (2, 1, 3, 0) for dx in (2, 1, 3, 0) if (dz, dx) != (0, 0)]
    l_send[...] = to_row(lse, 64)
    for dz, dx in others:
        pltpu.make_async_remote_copy(
            src_ref=l_send, dst_ref=l_recv.at[kv], send_sem=l_ss, recv_sem=l_rs,
            device_id=(kv_at(dz, dx), tp), device_id_type=MESH,
        ).start()
    l_recv[kv] = l_send[...]

    def gather_wait(buf, ss, rs):
        for d in range(4):
            slot = (twin + 2 * d) % 8
            gather_copy(buf, ss, rs, 0, slot, twin).wait_recv()

    gather_wait(wv, gv_ss, gv_rs)
    by_head = dot(acc.astype(BF16), jnp.concatenate([wv[h] for h in range(8)], axis=1))
    value = by_head[:, 0:128]
    row_head = iota((64, 128), 0) % 8
    for h in range(1, 8):
        value = jnp.where(row_head == h, by_head[:, 128 * h : 128 * h + 128], value)
    value = value / safe

    c_send[...] = value.astype(BF16)

    def c_rows(at_z):
        return c_send.at[pl.ds(pl.multiple_of(at_z * 16, 16), 16)]

    for dz, dx in others:
        pltpu.make_async_remote_copy(
            src_ref=c_rows(lax.rem(z + dz, 4)), dst_ref=c_recv.at[kv], send_sem=c_ss, recv_sem=c_rs,
            device_id=(kv_at(dz, dx), tp), device_id_type=MESH,
        ).start()
    c_recv[kv] = c_send[pl.ds(pl.multiple_of(z * 16, 16), 16), :]

    for d in (1, 3, 2):
        out_z(d, (z + d) % 4).wait_recv()
        out_twin(d, core).start()

    all_of(l_recv, 15, l_ss, l_rs).wait_recv()
    rows = [l_recv[k] for k in range(16)]
    top_row = functools.reduce(jnp.maximum, rows)
    masses = [jnp.exp(row - top_row) for row in rows]
    whole = functools.reduce(jnp.add, masses)
    own_lane = iota((16, 128), 1) == iota((16, 128), 0) + z * 16
    shares = [
        jnp.sum(jnp.where(own_lane, mass / whole, 0.0), axis=1, keepdims=True) for mass in masses
    ]

    all_of(c_recv, 15, c_ss, c_rs).wait_recv()
    terms = [c_recv[k].astype(F32) * shares[k] for k in range(16)]
    while len(terms) > 1:
        terms = [terms[i] + terms[i + 1] for i in range(0, len(terms), 2)]
    merged = terms[0]

    o_tab[...] = merged
    for d in range(4):
        out_twin(d, 1 - core).wait_recv()
    head_out = jnp.concatenate(
        [o_tab[pl.ds(2 * r + c, 2, stride=8), :] for c in range(2) for r in range(4)], axis=1
    ).astype(BF16)
    mixed_z = dot(head_out, jnp.concatenate([wo[k].reshape(1024, 128) for k in range(4)], axis=1))
    for k in range(4):
        m_send[k, :, 0:128] = mixed_z[0:1, 128 * k : 128 * k + 128]
        m_send[k, :, 128:256] = mixed_z[1:2, 128 * k : 128 * k + 128]
    g_send[...] = to_row(jnp.sum(mixed_z * mixed_z, axis=1, keepdims=True), 2)

    pair = tp * 4 + z

    def m_start(dz, dt):
        at_z = lax.rem(z + dz, 4)
        pltpu.make_async_remote_copy(
            src_ref=m_send.at[at_z], dst_ref=m_recv.at[pair], send_sem=m_ss, recv_sem=m_rs,
            device_id=(at_z * 4 + x, lax.rem(tp + dt, 8)), device_id_type=MESH,
        ).start()

    def g_start(dz, dx, dt):
        pltpu.make_async_remote_copy(
            src_ref=g_send, dst_ref=g_recv.at[x * 32 + pair], send_sem=g_ss, recv_sem=g_rs,
            device_id=(kv_at(dz, dx), lax.rem(tp + dt, 8)), device_id_type=MESH,
        ).start()

    steps = [(dz, dx, dt) for dz in (2, 1, 3, 0) for dx in (2, 1, 3, 0) for dt in (4, 5, 3, 2, 6, 7, 1, 0)][:-1]
    hops = [min(dz, 4 - dz) + min(dx, 4 - dx) + min(dt // 2, 4 - dt // 2) for dz, dx, dt in steps]
    for away in (6, 5, 4):
        for step, hop in zip(steps, hops):
            if hop == away:
                g_start(*step)
    for dz in (2, 1, 3, 0):
        for dt in (4, 5, 3, 2, 6, 7, 1, 0):
            if (dz, dt) != (0, 0):
                m_start(dz, dt)
    for away in (3, 2, 1, 0):
        for step, hop in zip(steps, hops):
            if hop == away:
                g_start(*step)
    m_recv[pair] = m_send[z]
    g_recv[x * 32 + pair] = g_send[...]
    loads[11].wait()

    for copy in a1 + a2 + value_sends + value_forwards:
        copy.wait_send()
    for d in range(4):
        out_twin(d, core).wait_send()
    for d in range(1, 4):
        out_y(d, y).wait_send()
        out_z(d, z).wait_send()
    all_of(b_recv, 7, b_ss, b_rs).wait_send()
    all_of(lat_recv, 15, lat_ss, lat_rs).wait_send()
    all_of(l_recv, 15, l_ss, l_rs).wait_send()
    all_of(c_recv, 15, c_ss, c_rs).wait_send()

    all_of(m_recv, 31, m_ss, m_rs).wait_recv()
    all_of(g_recv, 127, g_ss, g_rs).wait_recv()
    octet = iota((8, 128), 0)

    def eight(of):
        row = jnp.broadcast_to(of(0), (8, 128))
        for i in range(1, 8):
            row = jnp.where(octet == i, of(i), row)
        return row

    mixed = jnp.concatenate(
        [
            eight(lambda i: m_recv[4 * v + i // 2, :, 128 * (i % 2) : 128 * (i % 2) + 128])
            for v in range(8)
        ],
        axis=0,
    )
    totals = [g_recv[j] + g_recv[32 + j] + g_recv[64 + j] + g_recv[96 + j] for j in range(32)]
    squares = jnp.concatenate([eight(lambda i: totals[4 * v + i // 2]) for v in range(8)], axis=0)
    picked = iota((64, 128), 0) % 2 == iota((64, 128), 1)
    squares = jnp.sum(jnp.where(picked, squares, 0.0), axis=1, keepdims=True)
    inverse = lax.rsqrt(squares / 2048.0 + EPSILON)
    out_ref[...] = (mixed * inverse * ogain[...]).astype(BF16)

    all_of(m_recv, 31, m_ss, m_rs).wait_send()
    all_of(g_recv, 127, g_ss, g_rs).wait_send()


def on_device(
    tokens, token_gain, w_query, w_down_kv, w_rope_key, latent_gain, w_key_up, w_value_up, w_out, out_gain,
    cache_latent, cache_rope, lengths,
):
    freq = 1.0 / 10000.0 ** (np.arange(0, 64, 2, dtype=np.float32) / np.float32(64.0))
    freq = jnp.asarray(np.tile(freq.astype(np.float32), 4)[None, :])
    operands = (
        tokens, token_gain.reshape(1, 128), w_query.T, w_down_kv, w_rope_key.T, latent_gain.reshape(1, 512),
        w_key_up.reshape(512, 128), w_value_up.reshape(512, 128), w_out, out_gain.reshape(1, 128),
        cache_latent, cache_rope.transpose(0, 2, 1), lengths.reshape(1, 64), freq,
    )
    shapes = [(a.shape, a.dtype) for a in operands]
    shapes[7] = ((8, 512, 128), BF16)
    shapes[8] = ((4, 2, 4, 128, 128), BF16)
    local = [pltpu.VMEM(*a) for a in shapes]
    operands = tuple(pltpu.with_memory_space_constraint(v, pltpu.HBM) for v in operands)
    dma = pltpu.SemaphoreType.DMA
    scratch = local + [
        pltpu.VMEM((64, 128), F32), pltpu.VMEM((64, 64), F32), pltpu.VMEM((64, 64), F32),
        pltpu.VMEM((96, 128), BF16), pltpu.VMEM((3, 96, 128), BF16),
        pltpu.VMEM((96, 128), BF16), pltpu.VMEM((3, 96, 128), BF16),
        pltpu.VMEM((64, 640), F32), pltpu.VMEM((8, 1, 640), F32), pltpu.VMEM((16, 1, 640), F32),
        pltpu.VMEM((128, 512), BF16), pltpu.VMEM((8, 512, 512), BF16),
        pltpu.VMEM((8, 8, 640), BF16), pltpu.VMEM((8, 8, 640), BF16),
        pltpu.VMEM((5, 64, 128), F32), pltpu.VMEM((16, 128), F32),
        pltpu.VMEM((64, 128), BF16), pltpu.VMEM((16, 16, 128), BF16),
        pltpu.VMEM((1, 128), F32), pltpu.VMEM((16, 1, 128), F32),
        pltpu.VMEM((4, 1, 256), F32), pltpu.VMEM((32, 1, 256), F32),
        pltpu.VMEM((1, 128), F32), pltpu.VMEM((128, 1, 128), F32),
        dma((12,)), dma((16,)),
        dma((6,)), dma((6,)), dma((6,)), dma((6,)), dma, dma,
        dma, dma, dma((8,)), dma((8,)),
        dma((4,)), dma((4,)), dma((4,)), dma((4,)), dma((4,)), dma((4,)),
        dma, dma, dma, dma, dma, dma, dma, dma,
    ]
    return pl.pallas_call(
        kernel,
        out_shape=pltpu.VMEM((64, 128), BF16),
        in_specs=[pl.BlockSpec(memory_space=pltpu.HBM)] * len(operands),
        out_specs=pl.BlockSpec(memory_space=pltpu.VMEM),
        scratch_shapes=scratch,
        compiler_params=pltpu.CompilerParams(
            collective_id=0, has_side_effects=True, vmem_limit_bytes=48 * 1024 * 1024
        ),
    )(*operands)


def solution(mesh):
    return jax.shard_map(
        on_device,
        mesh=mesh,
        in_specs=(
            P(None, "kv"), P("kv"), P("kv", "tp"), P("kv", None), P("kv", None), P(),
            P("tp", None, None), P("tp", None, None), P("tp", "kv"), P("kv"),
            P("tp", "kv", None), P("tp", "kv", None), P(),
        ),
        out_specs=P(None, "kv"),
        check_vma=False,
    )
```

```python
import functools

import jax
import jax.numpy as jnp
import numpy as np
from jax import lax
from jax.experimental import pallas as pl
from jax.experimental.pallas import tpu as pltpu
from jax.sharding import PartitionSpec as P

MESH = pl.DeviceIdType.MESH
EPSILON = 1e-06
NEGATIVE = -1e30
BF16 = jnp.bfloat16
F32 = jnp.float32


def dot(a, b):
    return jnp.dot(a, b, preferred_element_type=F32)


def dot_nt(a, b):
    return lax.dot_general(a, b, (((1,), (1,)), ((), ())), preferred_element_type=F32)


def iota(shape, axis):
    return lax.broadcasted_iota(jnp.int32, shape, axis)


def to_column(row, rows):
    picked = iota((rows, rows), 0) == iota((rows, rows), 1)
    return jnp.sum(jnp.where(picked, row[:, :rows], 0.0), axis=1, keepdims=True)


def to_row(column, rows):
    picked = iota((rows, 128), 0) == iota((rows, 128), 1)
    return jnp.sum(jnp.where(picked, column, 0.0), axis=0, keepdims=True)


def kernel(
    tok_h, tgain_h, wq_h, wd_h, wr_h, lgain_h, wk_h, wv_h, wo_h, ogain_h, cl_h, cr_h, len_h, freq_h,
    out_ref,
    tok, tgain, wq, wd, wr, lgain, wk, wv, wo, ogain, cl, cr, lens, freq,
    len_tab, cos_tab, sin_tab,
    a1_send, a1_recv, a2_send, a2_recv,
    lat_all, lat_send, lat_recv,
    wk_turned, keys, b_send, b_recv, q_tab, o_tab,
    bias_tab, c_send, c_recv, l_send, l_recv,
    m_send, m_recv, g_send, g_recv,
    load_sem, cache_sem,
    a1_ss, a1_rs, a2_ss, a2_rs, lat_ss, lat_rs, b_ss, b_rs, gv_ss, gv_rs, oy_ss, oy_rs, oz_ss, oz_rs, ot_ss, ot_rs,
    c_ss, c_rs, l_ss, l_rs, m_ss, m_rs, g_ss, g_rs,
):
    kv = lax.axis_index("kv")
    tp = lax.axis_index("tp")
    z = kv // 4
    x = kv % 4
    y = tp // 2
    core = tp % 2

    pairs = [
        (tok_h, tok), (tgain_h, tgain), (wq_h, wq), (len_h, lens), (freq_h, freq), (wd_h, wd), (wr_h, wr),
        (wk_h, wk), (lgain_h, lgain), (wv_h, wv.at[tp]), (wo_h, wo.at[z, core, y]), (ogain_h, ogain),
    ]
    loads = [pltpu.make_async_copy(s, d, load_sem.at[i]) for i, (s, d) in enumerate(pairs)]
    cache_loads = []
    for s in range(8):
        cache_loads.append(pltpu.make_async_copy(cl_h.at[s], cl.at[s], cache_sem.at[s]))
        cache_loads.append(pltpu.make_async_copy(cr_h.at[s], cr.at[s], cache_sem.at[8 + s]))
    for copy in loads[:3] + loads[9:11]:
        copy.start()
    barrier = pltpu.get_barrier_semaphore()

    def greet(to_kv, to_tp):
        pl.semaphore_signal(barrier, inc=1, device_id=(to_kv, to_tp), device_id_type=MESH)

    for d in (2, 1, 3):
        greet(z * 4 + lax.rem(x + d, 4), tp)
    for d in (2, 1, 3):
        greet(lax.rem(z + d, 4) * 4 + x, tp)
    for d in (4, 5, 3, 2, 6, 7, 1):
        greet(kv, lax.rem(tp + d, 8))

    for i in range(3):
        loads[i].wait()
    scaled = (tok[...].astype(F32) * tgain[...]).astype(BF16)
    q_part = dot_nt(scaled, wq[...])
    rope_part = q_part[:, 128:192]
    q_nope_part = q_part[:, :128]
    q_rope_part = jnp.concatenate([rope_part[:32], rope_part[32:]], axis=1)
    a1_send[0:64, :] = q_nope_part.astype(BF16)
    a1_send[64:96, :] = q_rope_part.astype(BF16)

    for copy in loads[3:9] + loads[11:] + cache_loads:
        copy.start()
    pl.semaphore_wait(barrier, 13)

    def x_dev(d):
        return (z * 4 + (x + d) % 4, tp)

    def z_dev(d):
        return (((z + d) % 4) * 4 + x, tp)

    def line(src, dst, ss, rs, first, second):
        half = src.shape[0] // 2
        copies = []
        for d in (2, 1, 3):
            for k, dev in enumerate((first, second)):
                rows = pl.ds(k * half, half)
                copies.append(
                    pltpu.make_async_remote_copy(
                        src_ref=src.at[rows], dst_ref=dst.at[d - 1, rows],
                        send_sem=ss.at[3 * k + d - 1], recv_sem=rs.at[3 * k + d - 1],
                        device_id=dev(d), device_id_type=MESH,
                    )
                )
        return copies

    def line1(src, dst, ss, rs, dev):
        return [
            pltpu.make_async_remote_copy(
                src_ref=src, dst_ref=dst.at[d - 1], send_sem=ss.at[d - 1], recv_sem=rs.at[d - 1],
                device_id=dev(d), device_id_type=MESH,
            )
            for d in (1, 2, 3)
        ]

    a1 = line(a1_send, a1_recv, a1_ss, a1_rs, x_dev, z_dev)
    for copy in a1:
        copy.start()

    twin = tp + 1 - 2 * core

    def gather_copy(buf, ss, rs, i, slot, to):
        return pltpu.make_async_remote_copy(
            src_ref=buf.at[slot], dst_ref=buf.at[slot], send_sem=ss.at[i], recv_sem=rs.at[slot],
            device_id=(kv, to), device_id_type=MESH,
        )

    def gather_first(buf, ss, rs):
        copies = [gather_copy(buf, ss, rs, i, tp, (tp + 2 * d) % 8) for i, d in enumerate((2, 1, 3))]
        return copies + [gather_copy(buf, ss, rs, 3, tp, twin)]

    def gather_forward(buf, ss, rs):
        slots = [(tp + 2 * d) % 8 for d in (1, 3, 2)]
        return [gather_copy(buf, ss, rs, 4 + i, slot, twin) for i, slot in enumerate(slots)]

    loads[9].wait()
    loads[10].wait()
    value_sends = gather_first(wv, gv_ss, gv_rs)
    value_forwards = gather_forward(wv, gv_ss, gv_rs)

    def out_y(d, at):
        return pltpu.make_async_remote_copy(
            src_ref=wo.at[z, core, y], dst_ref=wo.at[z, core, at], send_sem=oy_ss.at[d], recv_sem=oy_rs.at[at],
            device_id=(kv, (tp + 2 * d) % 8), device_id_type=MESH,
        )

    def out_z(d, at):
        return pltpu.make_async_remote_copy(
            src_ref=wo.at[z, core], dst_ref=wo.at[at, core], send_sem=oz_ss.at[d], recv_sem=oz_rs.at[at],
            device_id=((z + d) % 4 * 4 + x, tp), device_id_type=MESH,
        )

    def out_twin(d, half):
        at = (z + d) % 4
        return pltpu.make_async_remote_copy(
            src_ref=wo.at[at, core], dst_ref=wo.at[at, half], send_sem=ot_ss.at[d], recv_sem=ot_rs.at[at],
            device_id=(kv, twin), device_id_type=MESH,
        )

    for d in (2, 1, 3):
        out_y(d, y).start()
    for copy in value_sends:
        copy.start()

    for i in range(3, 7):
        loads[i].wait()
    lat_all[:, 0:512] = dot(scaled, wd[...])
    lat_all[:, 512:576] = dot_nt(scaled, wr[...])
    lat_all[:, 576:640] = jnp.zeros((64, 64), F32)
    mine = lat_all[pl.ds(pl.multiple_of(tp * 8, 8), 8), :]
    for r in range(8):
        lat_send[r] = mine[r : r + 1, :]
    lat_recv[kv] = lat_send[kv // 2]

    def lat_copy(dz, dx):
        at_z = lax.rem(z + dz, 4)
        at_x = lax.rem(x + dx, 4)
        return pltpu.make_async_remote_copy(
            src_ref=lat_send.at[at_z * 2 + at_x // 2], dst_ref=lat_recv.at[kv], send_sem=lat_ss, recv_sem=lat_rs,
            device_id=(at_z * 4 + at_x, tp), device_id_type=MESH,
        )

    len_col = to_column(lens[...].astype(F32), 64)
    len_tab[...] = jnp.broadcast_to(len_col, (64, 128))
    lane = iota((32, 128), 1)
    packed_len = jnp.where(lane < 64, len_col[:32], len_col[32:])
    angle = packed_len * freq[...]
    cosine = jnp.cos(angle)
    sine = jnp.sin(angle)
    sine = jnp.where(lane % 64 < 32, -sine, sine)
    cos_tab[0:32, :] = cosine[:, :64]
    cos_tab[32:64, :] = cosine[:, 64:]
    sin_tab[0:32, :] = sine[:, :64]
    sin_tab[32:64, :] = sine[:, 64:]

    def added(own, recv, rows):
        total = own
        for d in range(3):
            total = total + recv[d, rows, :].astype(F32)
        return total

    for copy in a1:
        copy.wait_recv()
    q_nope_sum = added(q_nope_part, a1_recv, slice(0, 64))
    q_rope_sum = added(q_rope_part, a1_recv, slice(64, 96))
    a2_send[0:64, :] = q_nope_sum.astype(BF16)
    a2_send[64:96, :] = q_rope_sum.astype(BF16)
    a2 = line(a2_send, a2_recv, a2_ss, a2_rs, z_dev, x_dev)
    for copy in a2:
        copy.start()
    for dz in (2, 1, 3, 0):
        for dx in (2, 1, 3, 0):
            if (dz, dx) != (0, 0):
                lat_copy(dz, dx).start()
    loads[7].wait()
    wk_turned[...] = wk[...].T
    for s in range(4):
        cache_loads[2 * s].wait()
        keys[s] = cl[s].T
    for copy in a2:
        copy.wait_recv()
    q_nope = added(q_nope_sum, a2_recv, slice(0, 64)).astype(BF16)
    q_rope = added(q_rope_sum, a2_recv, slice(64, 96)).astype(BF16).astype(F32)
    swapped = jnp.where(lane % 64 < 32, pltpu.roll(q_rope, 96, 1), pltpu.roll(q_rope, 32, 1))
    q_rope = q_rope * cosine + swapped * sine
    q_rope = jnp.concatenate([q_rope[:, :64], q_rope[:, 64:]], axis=0)


    for d in (1, 3, 2):
        out_y(d, (y + d) % 4).wait_recv()
    for d in (2, 1, 3):
        out_z(d, z).start()
    out_twin(0, core).start()
    q_lat = dot(q_nope, wk_turned[...])
    pad = jnp.zeros((8, 64), F32)
    for j in range(8):
        block = jnp.concatenate([q_lat[8 * j : 8 * j + 8], q_rope[8 * j : 8 * j + 8], pad], axis=1)
        b_send[j] = block.astype(BF16)

    def b_copy(d):
        to = (tp + d) % 8
        return pltpu.make_async_remote_copy(
            src_ref=b_send.at[to], dst_ref=b_recv.at[tp], send_sem=b_ss, recv_sem=b_rs,
            device_id=(kv, to), device_id_type=MESH,
        )

    def all_of(ref, count, ss, rs):
        part = ref.at[pl.ds(0, count)]
        return pltpu.make_async_remote_copy(
            src_ref=part, dst_ref=part, send_sem=ss, recv_sem=rs, device_id=(kv, twin), device_id_type=MESH
        )

    for d in (4, 5, 3, 2, 6, 7, 1):
        b_copy(d).start()
    b_recv[tp] = b_send[tp]
    all_of(lat_recv, 15, lat_ss, lat_rs).wait_recv()
    lat_sum = lat_recv[0]
    for k in range(1, 16):
        lat_sum = lat_sum + lat_recv[k]
    loads[8].wait()
    lat_raw = lat_sum[:, :512]
    latent = (
        lat_raw * lax.rsqrt(jnp.mean(lat_raw * lat_raw, axis=1, keepdims=True) + EPSILON) * lgain[...]
    ).astype(BF16).astype(F32)
    key_raw = lat_sum[:, 512:576]
    new_seq = kv // 2
    new_row = tp * 8 + new_seq
    key_swapped = jnp.concatenate([key_raw[:, 32:], key_raw[:, :32]], axis=1)
    new_rope = key_raw * cos_tab[pl.ds(new_row, 1), :] + key_swapped * sin_tab[pl.ds(new_row, 1), :]
    new_rope = new_rope.astype(BF16).astype(F32)
    for s in range(4, 8):
        cache_loads[2 * s].wait()
        keys[s] = cl[s].T
    row_length = jnp.concatenate(
        [jnp.broadcast_to(len_tab[pl.ds(tp * 8 + s, 1), 0:1], (8, 1)) for s in range(8)], axis=0
    )
    positions = (kv * 512 + iota((64, 512), 1)).astype(F32)
    visible = positions < row_length
    bias_tab[...] = jnp.where(visible, 0.0, NEGATIVE)
    all_of(b_recv, 7, b_ss, b_rs).wait_recv()

    for copy in value_forwards:
        copy.wait_recv()
        copy.start()

    for h in range(8):
        rows = b_recv[h].astype(F32)
        for i in range(5):
            q_tab[i, 8 * h : 8 * h + 8, :] = rows[:, 128 * i : 128 * i + 128]

    def query_of(s):
        return jnp.concatenate([q_tab[i, pl.ds(s, 8, stride=8), :] for i in range(5)], axis=1)

    for copy in cache_loads[1::2]:
        copy.wait()
    factor = 192.0 ** (-0.5)

    def scores_of(s):
        q = query_of(s).astype(BF16)
        return dot(q[:, :512], keys[s]) + dot(q[:, 512:576], cr[s])

    scores = jnp.concatenate([scores_of(s) for s in range(8)], axis=0) * factor + bias_tab[...]

    q_new = query_of(new_seq)
    new_score = (
        jnp.sum(q_new[:, :512] * latent, axis=1, keepdims=True)
        + jnp.sum(q_new[:, 512:576] * new_rope, axis=1, keepdims=True)
    ) * factor

    row_seq = iota((64, 1), 0) // 8
    is_new = jnp.logical_and(row_seq == new_seq, kv % 2 == 0)
    own_new = jnp.where(is_new, jnp.concatenate([new_score] * 8, axis=0), NEGATIVE)
    top = jnp.maximum(jnp.max(scores, axis=1, keepdims=True), own_new)
    shift = jnp.where(top > 0.5 * NEGATIVE, top, 0.0)
    weights = jnp.exp(scores - shift)
    new_weight = jnp.where(is_new, jnp.exp(own_new - top), 0.0)
    total = jnp.sum(weights, axis=1, keepdims=True) + new_weight
    some = total > 0.0
    safe = jnp.where(some, total, 1.0)
    lse = jnp.where(some, top + jnp.log(safe), NEGATIVE)
    heads = [dot(weights[8 * s : 8 * s + 8].astype(BF16), cl[s]) for s in range(4)]
    heads += [dot(weights[8 * s : 8 * s + 8].astype(BF16), cl[s]) for s in range(4, 8)]
    acc = jnp.concatenate(heads, axis=0) + new_weight.astype(BF16).astype(F32) * latent

    def kv_at(dz, dx):
        return lax.rem(z + dz, 4) * 4 + lax.rem(x + dx, 4)

    others = [(dz, dx) for dz in (2, 1, 3, 0) for dx in (2, 1, 3, 0) if (dz, dx) != (0, 0)]
    l_send[...] = to_row(lse, 64)
    for dz, dx in others:
        pltpu.make_async_remote_copy(
            src_ref=l_send, dst_ref=l_recv.at[kv], send_sem=l_ss, recv_sem=l_rs,
            device_id=(kv_at(dz, dx), tp), device_id_type=MESH,
        ).start()
    l_recv[kv] = l_send[...]

    def gather_wait(buf, ss, rs):
        for d in range(4):
            slot = (twin + 2 * d) % 8
            gather_copy(buf, ss, rs, 0, slot, twin).wait_recv()

    gather_wait(wv, gv_ss, gv_rs)
    by_head = dot(acc.astype(BF16), jnp.concatenate([wv[h] for h in range(8)], axis=1))
    value = by_head[:, 0:128]
    row_head = iota((64, 128), 0) % 8
    for h in range(1, 8):
        value = jnp.where(row_head == h, by_head[:, 128 * h : 128 * h + 128], value)
    value = value / safe

    c_send[...] = value.astype(BF16)

    def c_rows(at_z):
        return c_send.at[pl.ds(pl.multiple_of(at_z * 16, 16), 16)]

    for dz, dx in others:
        pltpu.make_async_remote_copy(
            src_ref=c_rows(lax.rem(z + dz, 4)), dst_ref=c_recv.at[kv], send_sem=c_ss, recv_sem=c_rs,
            device_id=(kv_at(dz, dx), tp), device_id_type=MESH,
        ).start()
    c_recv[kv] = c_send[pl.ds(pl.multiple_of(z * 16, 16), 16), :]

    for d in (1, 3, 2):
        out_z(d, (z + d) % 4).wait_recv()
        out_twin(d, core).start()

    all_of(l_recv, 15, l_ss, l_rs).wait_recv()
    rows = [l_recv[k] for k in range(16)]
    top_row = functools.reduce(jnp.maximum, rows)
    masses = [jnp.exp(row - top_row) for row in rows]
    whole = functools.reduce(jnp.add, masses)
    own_lane = iota((16, 128), 1) == iota((16, 128), 0) + z * 16
    shares = [
        jnp.sum(jnp.where(own_lane, mass / whole, 0.0), axis=1, keepdims=True) for mass in masses
    ]

    all_of(c_recv, 15, c_ss, c_rs).wait_recv()
    terms = [c_recv[k].astype(F32) * shares[k] for k in range(16)]
    while len(terms) > 1:
        terms = [terms[i] + terms[i + 1] for i in range(0, len(terms), 2)]
    merged = terms[0]

    o_tab[...] = merged
    for d in range(4):
        out_twin(d, 1 - core).wait_recv()
    head_out = jnp.concatenate(
        [o_tab[pl.ds(2 * r + c, 2, stride=8), :] for c in range(2) for r in range(4)], axis=1
    ).astype(BF16)
    mixed_z = dot(head_out, jnp.concatenate([wo[k].reshape(1024, 128) for k in range(4)], axis=1))
    for k in range(4):
        m_send[k, :, 0:128] = mixed_z[0:1, 128 * k : 128 * k + 128]
        m_send[k, :, 128:256] = mixed_z[1:2, 128 * k : 128 * k + 128]
    g_send[...] = to_row(jnp.sum(mixed_z * mixed_z, axis=1, keepdims=True), 2)

    pair = tp * 4 + z

    def m_start(dz, dt):
        at_z = lax.rem(z + dz, 4)
        pltpu.make_async_remote_copy(
            src_ref=m_send.at[at_z], dst_ref=m_recv.at[pair], send_sem=m_ss, recv_sem=m_rs,
            device_id=(at_z * 4 + x, lax.rem(tp + dt, 8)), device_id_type=MESH,
        ).start()

    def g_start(dz, dx, dt):
        pltpu.make_async_remote_copy(
            src_ref=g_send, dst_ref=g_recv.at[x * 32 + pair], send_sem=g_ss, recv_sem=g_rs,
            device_id=(kv_at(dz, dx), lax.rem(tp + dt, 8)), device_id_type=MESH,
        ).start()

    steps = [(dz, dx, dt) for dz in (2, 1, 3, 0) for dx in (2, 1, 3, 0) for dt in (4, 5, 3, 2, 6, 7, 1, 0)][:-1]
    hops = [min(dz, 4 - dz) + min(dx, 4 - dx) + min(dt // 2, 4 - dt // 2) for dz, dx, dt in steps]
    for away in (6, 5, 4):
        for step, hop in zip(steps, hops):
            if hop == away:
                g_start(*step)
    for dz in (2, 1, 3, 0):
        for dt in (4, 5, 3, 2, 6, 7, 1, 0):
            if (dz, dt) != (0, 0):
                m_start(dz, dt)
    for away in (3, 2, 1, 0):
        for step, hop in zip(steps, hops):
            if hop == away:
                g_start(*step)
    m_recv[pair] = m_send[z]
    g_recv[x * 32 + pair] = g_send[...]
    loads[11].wait()

    for copy in a1 + a2 + value_sends + value_forwards:
        copy.wait_send()
    for d in range(4):
        out_twin(d, core).wait_send()
    for d in range(1, 4):
        out_y(d, y).wait_send()
        out_z(d, z).wait_send()
    all_of(b_recv, 7, b_ss, b_rs).wait_send()
    all_of(lat_recv, 15, lat_ss, lat_rs).wait_send()
    all_of(l_recv, 15, l_ss, l_rs).wait_send()
    all_of(c_recv, 15, c_ss, c_rs).wait_send()

    all_of(m_recv, 31, m_ss, m_rs).wait_recv()
    all_of(g_recv, 127, g_ss, g_rs).wait_recv()
    octet = iota((8, 128), 0)

    def eight(of):
        row = jnp.broadcast_to(of(0), (8, 128))
        for i in range(1, 8):
            row = jnp.where(octet == i, of(i), row)
        return row

    mixed = jnp.concatenate(
        [
            eight(lambda i: m_recv[4 * v + i // 2, :, 128 * (i % 2) : 128 * (i % 2) + 128])
            for v in range(8)
        ],
        axis=0,
    )
    totals = [g_recv[j] + g_recv[32 + j] + g_recv[64 + j] + g_recv[96 + j] for j in range(32)]
    squares = jnp.concatenate([eight(lambda i: totals[4 * v + i // 2]) for v in range(8)], axis=0)
    picked = iota((64, 128), 0) % 2 == iota((64, 128), 1)
    squares = jnp.sum(jnp.where(picked, squares, 0.0), axis=1, keepdims=True)
    inverse = lax.rsqrt(squares / 2048.0 + EPSILON)
    out_ref[...] = (mixed * inverse * ogain[...]).astype(BF16)

    all_of(m_recv, 31, m_ss, m_rs).wait_send()
    all_of(g_recv, 127, g_ss, g_rs).wait_send()


def on_device(
    tokens, token_gain, w_query, w_down_kv, w_rope_key, latent_gain, w_key_up, w_value_up, w_out, out_gain,
    cache_latent, cache_rope, lengths,
):
    freq = 1.0 / 10000.0 ** (np.arange(0, 64, 2, dtype=np.float32) / np.float32(64.0))
    freq = jnp.asarray(np.tile(freq.astype(np.float32), 4)[None, :])
    operands = (
        tokens, token_gain.reshape(1, 128), w_query.T, w_down_kv, w_rope_key.T, latent_gain.reshape(1, 512),
        w_key_up.reshape(512, 128), w_value_up.reshape(512, 128), w_out, out_gain.reshape(1, 128),
        cache_latent, cache_rope.transpose(0, 2, 1), lengths.reshape(1, 64), freq,
    )
    shapes = [(a.shape, a.dtype) for a in operands]
    shapes[7] = ((8, 512, 128), BF16)
    shapes[8] = ((4, 2, 4, 128, 128), BF16)
    local = [pltpu.VMEM(*a) for a in shapes]
    operands = tuple(pltpu.with_memory_space_constraint(v, pltpu.HBM) for v in operands)
    dma = pltpu.SemaphoreType.DMA
    scratch = local + [
        pltpu.VMEM((64, 128), F32), pltpu.VMEM((64, 64), F32), pltpu.VMEM((64, 64), F32),
        pltpu.VMEM((96, 128), BF16), pltpu.VMEM((3, 96, 128), BF16),
        pltpu.VMEM((96, 128), BF16), pltpu.VMEM((3, 96, 128), BF16),
        pltpu.VMEM((64, 640), F32), pltpu.VMEM((8, 1, 640), F32), pltpu.VMEM((16, 1, 640), F32),
        pltpu.VMEM((128, 512), BF16), pltpu.VMEM((8, 512, 512), BF16),
        pltpu.VMEM((8, 8, 640), BF16), pltpu.VMEM((8, 8, 640), BF16),
        pltpu.VMEM((5, 64, 128), F32), pltpu.VMEM((16, 128), F32),
        pltpu.VMEM((64, 512), F32), pltpu.VMEM((64, 128), BF16), pltpu.VMEM((16, 16, 128), BF16),
        pltpu.VMEM((1, 128), F32), pltpu.VMEM((16, 1, 128), F32),
        pltpu.VMEM((4, 1, 256), F32), pltpu.VMEM((32, 1, 256), F32),
        pltpu.VMEM((1, 128), F32), pltpu.VMEM((128, 1, 128), F32),
        dma((12,)), dma((16,)),
        dma((6,)), dma((6,)), dma((6,)), dma((6,)), dma, dma,
        dma, dma, dma((8,)), dma((8,)),
        dma((4,)), dma((4,)), dma((4,)), dma((4,)), dma((4,)), dma((4,)),
        dma, dma, dma, dma, dma, dma, dma, dma,
    ]
    return pl.pallas_call(
        kernel,
        out_shape=pltpu.VMEM((64, 128), BF16),
        in_specs=[pl.BlockSpec(memory_space=pltpu.HBM)] * len(operands),
        out_specs=pl.BlockSpec(memory_space=pltpu.VMEM),
        scratch_shapes=scratch,
        compiler_params=pltpu.CompilerParams(
            collective_id=0, has_side_effects=True, vmem_limit_bytes=48 * 1024 * 1024
        ),
    )(*operands)


def solution(mesh):
    return jax.shard_map(
        on_device,
        mesh=mesh,
        in_specs=(
            P(None, "kv"), P("kv"), P("kv", "tp"), P("kv", None), P("kv", None), P(),
            P("tp", None, None), P("tp", None, None), P("tp", "kv"), P("kv"),
            P("tp", "kv", None), P("tp", "kv", None), P(),
        ),
        out_specs=P(None, "kv"),
        check_vma=False,
    )
```
